512 devices in a mesh: sp: 32 (over z, x), tp: 16 (over y, core).
Axes of the slice: x: 4, y: 8, z: 8, core: 2. Of those that a mesh axis runs over, the one named last changes fastest.
Arguments:
- queries: bfloat16 [8192, 1024], P('sp', 'tp'), may hold values from -64 to 64
- keys: bfloat16 [8192, 1024], P('sp', 'tp'), may hold values from -64 to 64
- values: bfloat16 [8192, 1024], P('sp', 'tp'), may hold values from -6 to 6
- cum_gate: float32 [16, 8192], P('tp'), may hold values from -8192 to 0, as said below
- out_weight: bfloat16 [1024, 2048], P('tp'), may hold values from -0.375 to 0.375
- resid: bfloat16 [8192, 2048], P('sp'), may hold values from -6 to 6
- norm_gain: float32 [2048], replicated, may hold values from 0.1 to 1.9
- routes: int32 [8192, 2], P('sp'), may hold values from 0 to 31, all different within a row; in each aligned block of 256 rows (0 to 255, 256 to 511, ...) at most 20 rows name the same one
- route_weight: float32 [8192, 2], P('sp'), may hold values from 0.1 to 0.9
- gate_weight: bfloat16 [32, 2048, 4096], P('sp', None, 'tp'), may hold values from -0.125 to 0.125
- up_weight: bfloat16 [32, 2048, 4096], P('sp', None, 'tp'), may hold values from -0.125 to 0.125
- down_weight: bfloat16 [32, 4096, 2048], P('sp', 'tp'), may hold values from -0.09375 to 0.09375
Outputs:
- layer_out: bfloat16 [8192, 2048], P('sp', 'tp')
The draws below stay inside these ranges and needn't reach their ends.
Inputs may be any that keep to these rules, and one draw needn't show every extreme that they name: `routes`: each token names 2 different experts. Among the rows of one index of sp, no expert is named more than 20 times, a bound that some block reaches. `cum_gate`: each head's row does not rise along the positions.
All inputs are finite; a program needn't handle non-finite values.
Results may differ from the reference program's by a relative error of at most 0.015.
Values may be sent and summed in bfloat16 or wider, within the bound.
No kernel may reach another device: no remote copies, remote signals or barrier semaphores. Data moves between devices by JAX's collectives and lax.ppermute only.
A program may use at most 64 MiB of HBM per device.

```python
import math
import jax
import jax.numpy as jnp
import numpy as np
from jax import lax

D = 2048
HEADS = 16
HD = 64
FF = 4096
TOPK = 2
TOK_DEV = 256
SEQUENCE_TOKENS = 8192
EXPERTS = 32
CAP = 20
N_SP = 32
N_TP = 16


def draw_queries(key, part):
    base = jax.random.normal(jax.random.fold_in(key, 1), (SEQUENCE_TOKENS, HEADS * HD), jnp.float32)
    base = jnp.clip(base, -6.0, 6.0)
    return base.astype(jnp.bfloat16)


def draw_keys(key, part):
    base = jax.random.normal(jax.random.fold_in(key, 2), (SEQUENCE_TOKENS, HEADS * HD), jnp.float32)
    base = jnp.clip(base, -6.0, 6.0) * 2.0
    return base.astype(jnp.bfloat16)


def draw_cum_gate(key, part):
    parallel_flows = jax.random.split(jax.random.fold_in(key, 3), 6)
    order = jax.random.permutation(parallel_flows[0], HEADS)
    slow = order < HEADS // 2
    fast_rate = jnp.exp(jax.random.uniform(parallel_flows[1], (HEADS,), jnp.float32, jnp.log(1.0 / 100.0), jnp.log(1.0 / 30.0)))
    rate = jnp.where(slow, 0.8 / SEQUENCE_TOKENS, fast_rate)
    blocks = SEQUENCE_TOKENS // TOK_DEV
    block_factor = jnp.exp(jax.random.uniform(parallel_flows[2], (blocks,), jnp.float32, jnp.log(0.5), jnp.log(2.0)))
    rough = jax.random.uniform(parallel_flows[3], (HEADS, SEQUENCE_TOKENS), jnp.float32, 0.3, 1.7)
    forget_step = -rate[:, None] * jnp.repeat(block_factor, TOK_DEV)[None, :] * rough
    group_position = jax.random.randint(parallel_flows[4], (2,), 0, SEQUENCE_TOKENS)
    token_group = jnp.log(1.0 - jax.random.uniform(parallel_flows[5], (2,), jnp.float32, 0.2, 0.5))
    forget_step = forget_step.at[:, group_position].add(token_group[None, :])
    return jnp.cumsum(forget_step, axis=1)


def steps_of(stream_key, dims, pieces, smallest, largest):
    gain = 1.0
    for axis_at, blocks in pieces:
        draws = jax.random.uniform(jax.random.fold_in(jax.random.fold_in(stream_key, 6), axis_at), (blocks,), jnp.float32, smallest / len(pieces), largest / len(pieces))
        gain = gain * jnp.repeat(jnp.exp(draws), dims[axis_at] // blocks).reshape((-1,) + (1,) * (len(dims) - 1 - axis_at))
    return gain


def assign_block(rng, own, number, rows, number_of, top, bound, slope):
    ranking = jax.random.permutation(rng, number_of)
    crowded, ordinary = portions_of(number_of, rows * top, bound, slope, True), portions_of(number_of, rows * top, bound, slope, False)
    places = jnp.arange(number_of)

    def named(sizes, rotation):
        used = int((sizes > 0).sum())
        fixed = max(1, used // 4)
        shifted = fixed + (places - fixed + rotation * (used - fixed)) % max(1, number_of - fixed)
        return jnp.zeros((number_of,), jnp.int32).at[ranking[jnp.where(places < fixed, places, shifted)]].set(jnp.asarray(sizes, jnp.int32))

    sizes = jnp.where(number % 4 == 0, named(crowded, number // 4), named(ordinary, number - number // 4 - 1))
    mixed = jax.random.permutation(jax.random.fold_in(own, 3), number_of)
    giver, taker = mixed[0:number_of // 2 * 2:2], mixed[1:number_of // 2 * 2:2]
    margin = jnp.minimum(sizes[giver] - 1, bound - sizes[taker]) // 2
    margin = jnp.where((giver == ranking[0]) | (taker == ranking[0]) | (sizes[taker] == 0), 0, jnp.maximum(margin, 0))
    shifted = jax.random.randint(jax.random.fold_in(own, 4), (number_of // 2,), 0, 1 << 20) % (margin + 1)
    sizes = sizes.at[giver].add(-shifted).at[taker].add(shifted)
    items = jnp.searchsorted(jnp.cumsum(sizes), jnp.arange(rows * top), side="right").astype(jnp.int32)
    table = items.reshape(top, rows).T
    table = table[jax.random.permutation(jax.random.fold_in(own, 1), rows)]
    rotation = jax.random.randint(jax.random.fold_in(own, 2), (rows, 1), 0, top)
    return jnp.take_along_axis(table, (jnp.arange(top)[None, :] + rotation) % top, axis=1)


def portions_of(number_of, total, bound, skew, full):
    loads = [(1 << 20) // math.isqrt(standing ** skew) + 1 for standing in range(1, number_of + 1)]
    largest = bound if full else min(bound, max(-(-total // number_of), total * loads[0] // sum(loads)))
    least = 1 if total - largest >= number_of - 1 else 0
    holding, spare = [largest] + [least] * (number_of - 1), total - largest - least * (number_of - 1)
    while spare > 0:
        free = [i for i in range(1, number_of) if holding[i] < largest] or [i for i in range(1, number_of) if holding[i] < bound]
        mass, remaining = sum([loads[i] for i in free]), spare
        for i in free:
            extra = min(bound - holding[i], max(1, remaining * loads[i] // mass), spare)
            holding[i] = holding[i] + extra
            spare = spare - extra
    return np.array(holding)


def gaussian(key, extent, deviation, bound, pieces=(), kind=jnp.bfloat16):
    values = deviation * jax.random.normal(key, extent, jnp.float32)
    if pieces:
        values = values * steps_of(key, extent, pieces, -0.22, 0.18)
    return jnp.clip(values, -bound, bound).astype(kind)


def setup_inputs(seed: int = 0) -> dict:
    key_of = jax.random.split(jax.random.key(seed), 13)
    queries = draw_queries(jax.random.fold_in(key_of[12], 71), 0)
    keys = draw_keys(jax.random.fold_in(key_of[12], 71), 0)
    values = gaussian(key_of[2], (SEQUENCE_TOKENS, HEADS * HD), 1.0, 6.0, ((0, 32), (1, 16)))
    cum_gate = draw_cum_gate(jax.random.fold_in(key_of[12], 71), 0)
    out_weight = gaussian(key_of[4], (HEADS * HD, D), (2.0 / (HEADS * HD) ** 0.5), 0.375, ((0, 16),))
    resid = gaussian(key_of[5], (SEQUENCE_TOKENS, D), 1.0, 6.0, ((0, 32),))
    norm_gain = jnp.clip(1.0 + 0.18 * jax.random.normal(key_of[6], (D,), jnp.float32), 0.1, 1.9)
    routes_keys = jax.random.split(jax.random.fold_in(key_of[7], 1), SEQUENCE_TOKENS // TOK_DEV)
    routes_turns = jax.random.permutation(jax.random.fold_in(key_of[7], 3), SEQUENCE_TOKENS // TOK_DEV)
    routes = jax.vmap(lambda own, number: assign_block(jax.random.fold_in(key_of[7], 2), own, number, TOK_DEV, EXPERTS, TOPK, CAP, 2))(routes_keys, routes_turns).reshape((SEQUENCE_TOKENS, TOPK))
    route_weight = jnp.clip(0.1 + 0.79999997 * jax.random.uniform(key_of[8], (SEQUENCE_TOKENS, TOPK), jnp.float32) ** steps_of(key_of[8], (SEQUENCE_TOKENS, TOPK), ((0, 32),), -0.2, 0.2), 0.1, 0.9)
    gate_weight = gaussian(key_of[9], (EXPERTS, D, FF), D ** -0.5, 0.125, ((0, 32), (2, 16)))
    up_weight = gaussian(key_of[10], (EXPERTS, D, FF), D ** -0.5, 0.125, ((0, 32), (2, 16)))
    down_weight = gaussian(key_of[11], (EXPERTS, FF, D), FF ** -0.5, 0.09375, ((0, 32), (1, 16)))
    return dict(queries=queries, keys=keys, values=values, cum_gate=cum_gate, out_weight=out_weight, resid=resid, norm_gain=norm_gain, routes=routes, route_weight=route_weight, gate_weight=gate_weight, up_weight=up_weight, down_weight=down_weight)


epsilon = 1e-06

def attention(queries, keys, values, cum_gate):
    length = queries.shape[0]
    score_scale = HD ** (-0.5)
    query_all = queries.reshape(length, HEADS, HD).astype(jnp.float32)
    key_all = keys.reshape(length, HEADS, HD).astype(jnp.float32)
    value_all = values.reshape(length, HEADS, HD).astype(jnp.float32)
    block_rows = math.gcd(length, 256)
    key_pos = jnp.arange(length, dtype=jnp.int32)

    def one_block(block_index):
        block_first = (block_index * block_rows).astype(jnp.int32)
        query_part = lax.dynamic_slice_in_dim(query_all, block_first, block_rows, 0)
        cum_query = lax.dynamic_slice_in_dim(cum_gate, block_first, block_rows, 1)
        scores = jnp.einsum('qhd,khd->hqk', query_part, key_all) * score_scale
        scores = scores + cum_query[:, :, None] - cum_gate[:, None, :]
        query_pos = block_first + jnp.arange(block_rows, dtype=jnp.int32)
        permitted_mask = (key_pos[None, :] <= query_pos[:, None])[None]
        best_score = lax.optimization_barrier(jnp.max(jnp.where(permitted_mask, scores, -jnp.inf), axis=-1, keepdims=True))
        weights = jnp.where(permitted_mask, jnp.exp(scores - best_score), 0.0)
        weight_sum = lax.optimization_barrier(jnp.sum(weights, axis=-1))
        rounded = lax.optimization_barrier(weights.astype(jnp.bfloat16)).astype(jnp.float32)
        value_sum = jnp.einsum('hqk,khd->hqd', rounded, value_all)
        return (value_sum / weight_sum[..., None]).astype(jnp.bfloat16)
    blocks = lax.map(one_block, jnp.arange(length // block_rows, dtype=jnp.int32))
    return blocks.transpose(0, 2, 1, 3).reshape(length, HEADS * HD)

def project(attended, out_weight):
    length = attended.shape[0]
    group_cols = HEADS * HD // N_TP
    parts = attended.reshape(length, N_TP, group_cols).transpose(1, 0, 2)
    weight_parts = out_weight.reshape(N_TP, group_cols, D)

    def add_group(running, pair):
        term = jnp.dot(pair[0], pair[1], preferred_element_type=jnp.float32)
        rounded = lax.optimization_barrier(term.astype(jnp.bfloat16)).astype(jnp.float32)
        return (running + rounded, None)
    mixed_sum, ignored = lax.scan(add_group, jnp.zeros((length, D), jnp.float32), (parts, weight_parts))
    return mixed_sum

def experts_out(normed, routes, route_weight, gate_weight, up_weight, down_weight):
    length = normed.shape[0]
    capacity = N_SP * CAP
    chosen = routes.reshape(-1).astype(jnp.int32)
    row_of = jnp.arange(length * TOPK, dtype=jnp.int32) // TOPK
    weight_flat = route_weight.reshape(-1)
    group_rows = FF // N_TP

    def add_expert(running, expert_index):
        hit = (chosen == expert_index).astype(jnp.int32)
        rank_within = jnp.cumsum(hit) - hit
        slot_index = jnp.where(hit > 0, rank_within, capacity).astype(jnp.int32)
        source_row = jnp.zeros((capacity + 1,), jnp.int32).at[slot_index].set(row_of)[:capacity]
        slot_weight = jnp.zeros((capacity + 1,), jnp.float32).at[slot_index].set(weight_flat * hit.astype(jnp.float32))[:capacity]
        arrived_rows = normed[source_row]
        gate_sum = jnp.dot(arrived_rows, gate_weight[expert_index], preferred_element_type=jnp.float32)
        up_sum = jnp.dot(arrived_rows, up_weight[expert_index], preferred_element_type=jnp.float32)
        hidden = (jax.nn.silu(gate_sum) * up_sum).astype(jnp.bfloat16)
        hidden_groups = hidden.reshape(capacity, N_TP, group_rows).transpose(1, 0, 2).astype(jnp.float32)
        down_groups = down_weight[expert_index].reshape(N_TP, group_rows, D).astype(jnp.float32)
        terms = jnp.einsum('grf,gfd->grd', hidden_groups, down_groups)
        rounded = lax.optimization_barrier(terms.astype(jnp.bfloat16)).astype(jnp.float32)
        expert_rows = lax.optimization_barrier(jnp.sum(rounded, axis=0)).astype(jnp.bfloat16)
        running = running.at[source_row].add(slot_weight[:, None] * expert_rows.astype(jnp.float32))
        return (running, None)
    combined, ignored = lax.scan(add_expert, jnp.zeros((length, D), jnp.float32), jnp.arange(EXPERTS, dtype=jnp.int32))
    return combined

def reference(queries, keys, values, cum_gate, out_weight, resid, norm_gain, routes, route_weight, gate_weight, up_weight, down_weight):
    attended = attention(queries, keys, values, cum_gate)
    stream = resid.astype(jnp.float32) + project(attended, out_weight)
    square_mean = lax.optimization_barrier(jnp.mean(stream * stream, axis=1, keepdims=True))
    normed = (stream * lax.rsqrt(square_mean + epsilon) * norm_gain).astype(jnp.bfloat16)
    combined = experts_out(normed, routes, route_weight, gate_weight, up_weight, down_weight)
    return (stream + combined).astype(jnp.bfloat16)
```

```python
import jax
import jax.numpy as jnp
from jax import lax
from jax.experimental import pallas as pl
from jax.experimental.pallas import tpu as pltpu
from jax.sharding import Mesh, PartitionSpec as P

NZ, NX, NY, NC = 8, 4, 8, 2
NSP, NTP = NZ * NX, NY * NC
SP, TP = ("z", "x"), ("y", "c")
HD = 64
TOK = 256
D = 2048
COLS = D // NTP
KEYS = NX * TOK
CAP = 20
SLOT = 24
ROWS = NSP * CAP
PADROWS = NSP * SLOT
META = 16
FFL = 256
EPS = 1e-06
LOW = -1e30
bf = jnp.bfloat16
f32 = jnp.float32

INTERPRET = False


def call(body, out_shape, inputs, smem=0, scratch=()):
    specs = [pl.BlockSpec(memory_space=pltpu.SMEM)] * smem
    specs += [pl.BlockSpec(memory_space=pltpu.VMEM)] * (len(inputs) - smem)
    many = isinstance(out_shape, (tuple, list))
    vm = pl.BlockSpec(memory_space=pltpu.VMEM)
    return pl.pallas_call(
        body,
        out_shape=out_shape,
        in_specs=specs,
        out_specs=tuple([vm] * len(out_shape)) if many else vm,
        scratch_shapes=list(scratch),
        interpret=INTERPRET,
        compiler_params=pltpu.CompilerParams(vmem_limit_bytes=48 * 1024 * 1024),
    )(*inputs)


def three(v):
    hi = v.astype(bf).astype(f32)
    rest = v - hi
    mid = rest.astype(bf).astype(f32)
    return hi, mid, rest - mid


def attend(at_ref, q_ref, kv_ref, gate_ref, out_ref, keys_ref, vals_ref):
    z, x = at_ref[0], at_ref[1]
    first = gate_ref[0:1, 0:1]
    row64 = lax.broadcasted_iota(jnp.int32, (HD, TOK), 0)
    for j in range(NX):
        bias = first - gate_ref[j : j + 1, :]
        hi, mid, lo = three(bias)
        extra = jnp.where(row64 == 0, hi, jnp.where(row64 == 1, mid, jnp.where(row64 == 2, lo, 0.0)))
        both = jnp.concatenate([kv_ref[j, 0:HD, :], extra.astype(bf)], axis=0)
        keys_ref[j * TOK : (j + 1) * TOK, :] = both.T
        vals_ref[0:HD, j * TOK : (j + 1) * TOK] = kv_ref[j, HD : 2 * HD, :]
        vals_ref[HD : HD + 16, j * TOK : (j + 1) * TOK] = jnp.ones((16, TOK), bf)
    ones = jnp.where(row64 < 3, 1.0, 0.0).astype(bf)
    row16 = lax.broadcasted_iota(jnp.int32, (16, TOK), 0)

    def part(zq, masked):
        q = jnp.concatenate([q_ref[zq] * bf(HD**-0.5), ones], axis=0)
        s = jnp.dot(keys_ref[...], q, preferred_element_type=f32)
        if masked:
            ki = lax.broadcasted_iota(jnp.int32, (KEYS, TOK), 0)
            qi = lax.broadcasted_iota(jnp.int32, (KEYS, TOK), 1) + x * TOK
            s = jnp.where(ki <= qi, s, LOW)
        m = jnp.max(s, axis=0, keepdims=True)
        p = jnp.exp(s - m).astype(bf)
        o = jnp.dot(vals_ref[...], p, preferred_element_type=f32)
        total = o[HD : HD + 1, :]
        hi, mid, lo = three(m + jnp.log(total))
        stats = jnp.where(row16 == 0, hi, jnp.where(row16 == 1, mid, jnp.where(row16 == 2, lo, 0.0)))
        out_ref[zq, 0:HD, :] = (o[0:HD, :] / total).astype(bf)
        out_ref[zq, HD : HD + 16, :] = stats.astype(bf)

    part(z, True)

    def later(zq, carry):
        part(zq, False)
        return carry

    lax.fori_loop(z + 1, NZ, later, 0)

    def earlier(zq, carry):
        out_ref[zq, 0:HD, :] = jnp.zeros((HD, TOK), bf)
        out_ref[zq, HD : HD + 16, :] = jnp.where(row16 == 0, LOW, 0.0).astype(bf)
        return carry

    lax.fori_loop(0, z, earlier, 0)


def merge(part_ref, off_ref, out_ref):
    ls = []
    for i in range(NZ):
        st = part_ref[i, HD : HD + 16, :].astype(f32)
        ls.append(st[0:1] + st[1:2] + st[2:3] + off_ref[i : i + 1, :])
    m = ls[0]
    for v in ls[1:]:
        m = jnp.maximum(m, v)
    acc = jnp.zeros((HD, TOK), f32)
    total = jnp.zeros((1, TOK), f32)
    for i in range(NZ):
        w = jnp.exp(ls[i] - m)
        total = total + w
        acc = acc + w * part_ref[i, 0:HD, :].astype(f32)
    out_ref[...] = (acc / total).astype(bf)


def project(att_ref, w_ref, resid_ref, gain_ref, routes_ref, stream_ref, out_ref, slots_ref):
    mixed = lax.dot_general(att_ref[...], w_ref[...], (((0,), (0,)), ((), ())), preferred_element_type=f32)
    stream = resid_ref[...].astype(f32) + mixed
    stream_ref[...] = stream
    square = jnp.sum(stream * stream, axis=1, keepdims=True)
    hi = square.astype(bf)
    lo = (square - hi.astype(f32)).astype(bf)
    scaled = (stream * gain_ref[...]).astype(bf)
    wide = (TOK, COLS)
    rows = jnp.concatenate([scaled, jnp.broadcast_to(hi, wide), jnp.broadcast_to(lo, wide)], axis=1)
    e0, e1 = routes_ref[0:1, :], routes_ref[1:2, :]
    io = lax.broadcasted_iota(jnp.int32, (NSP, TOK), 0)
    h0, h1 = io == e0, io == e1
    hit = jnp.where(h0, 1.0, jnp.where(h1, 1.0, 0.0)).astype(bf)
    ia = lax.broadcasted_iota(jnp.int32, (TOK, TOK), 0)
    ib = lax.broadcasted_iota(jnp.int32, (TOK, TOK), 1)
    upper = jnp.where(ia < ib, 1.0, 0.0).astype(bf)
    before = jnp.dot(hit, upper, preferred_element_type=f32)
    r0 = jnp.sum(jnp.where(h0, before, 0.0), axis=0, keepdims=True).astype(jnp.int32)
    r1 = jnp.sum(jnp.where(h1, before, 0.0), axis=0, keepdims=True).astype(jnp.int32)
    s0 = e0 * SLOT + r0
    s1 = e1 * SLOT + r1
    slots_ref[...] = jnp.concatenate([s0, s1, jnp.zeros((6, TOK), jnp.int32)], axis=0)
    ir = lax.broadcasted_iota(jnp.int32, (PADROWS, TOK), 0)
    pick = jnp.where(ir == s0, 1.0, jnp.where(ir == s1, 1.0, 0.0)).astype(bf)
    sent = jnp.dot(pick, rows, preferred_element_type=f32).reshape(NSP, SLOT, 3 * COLS)
    shape = (NSP, SLOT, COLS)
    rank = lax.broadcasted_iota(jnp.int32, shape, 1)
    lane = lax.broadcasted_iota(jnp.int32, shape, 2)
    data, his, los = sent[:, :, 0:COLS], sent[:, :, COLS : 2 * COLS], sent[:, :, 2 * COLS :]
    mh = jnp.sum(jnp.where(lane == rank, his, 0.0), axis=1, keepdims=True)
    ml = jnp.sum(jnp.where(lane == rank, los, 0.0), axis=1, keepdims=True)
    data = jnp.where(rank == CAP, mh, jnp.where(rank == CAP + 1, ml, data))
    out_ref[...] = data.astype(bf)


def squeeze(in_ref, out_ref, rows_ref):
    rank = lax.broadcasted_iota(jnp.int32, (NSP, SLOT, COLS), 1)
    x = in_ref[...].astype(f32)
    part = jnp.sum(jnp.where((rank == CAP) | (rank == CAP + 1), x, 0.0), axis=1)
    lane = lax.broadcasted_iota(jnp.int32, (NSP, COLS), 1)
    part = jnp.where(lane < CAP, part, 0.0)
    packed = part[0:8]
    for g in range(1, 4):
        packed = packed + pltpu.roll(part[8 * g : 8 * g + 8], 32 * g, 1)
    hi = packed.astype(bf).astype(f32)
    for i in range(NSP):
        rows_ref[CAP * i : CAP * i + CAP, :] = in_ref[i].astype(f32)[0:CAP, :]
    rows_ref[ROWS : ROWS + 8, :] = hi
    rows_ref[ROWS + 8 : ROWS + 16, :] = packed - hi
    out_ref[...] = rows_ref[...].astype(bf)


def experts(c_ref, own_ref, other_ref, wg_ref, wu_ref, wd_ref, mine_ref, theirs_ref, g_ref, u_ref, h_ref):
    c = c_ref[0]
    total = jnp.zeros((8, COLS), f32)
    for ref in (own_ref, other_ref):
        for y in range(NY):
            meta = ref[y, ROWS : ROWS + META, :].astype(f32)
            total = total + meta[0:8] + meta[8:16]
    scale8 = lax.rsqrt(total / D + EPS)
    shape = (ROWS, COLS)
    row = lax.broadcasted_iota(jnp.int32, shape, 0).astype(f32)
    lane = lax.broadcasted_iota(jnp.int32, shape, 1).astype(f32)
    src = jnp.floor((row + 0.5) * (1.0 / CAP))
    group = jnp.floor((src + 0.5) * 0.125)
    sub = src - 8.0 * group
    target = 32.0 * group + (row - CAP * src)
    spread = jnp.zeros(shape, f32)
    for a in range(8):
        spread = jnp.where(sub == a, scale8[a : a + 1, :], spread)
    scale = jnp.sum(jnp.where(lane == target, spread, 0.0), axis=1, keepdims=True)
    for y in range(NY):
        xx = jnp.concatenate([own_ref[y, 0:ROWS, :], other_ref[y, 0:ROWS, :]], axis=1)
        first = pl.multiple_of((2 * y + c) * COLS, COLS)
        second = pl.multiple_of((2 * y + 1 - c) * COLS, COLS)
        for w_ref, acc_ref in ((wg_ref, g_ref), (wu_ref, u_ref)):
            w = jnp.concatenate([w_ref[pl.ds(first, COLS), :], w_ref[pl.ds(second, COLS), :]], axis=0)
            part = jnp.dot(xx, w, preferred_element_type=f32)
            if y == 0:
                acc_ref[...] = part
            else:
                acc_ref[...] += part
    gate = g_ref[...] * scale
    up = u_ref[...] * scale
    h_ref[...] = (gate / (1.0 + jnp.exp(-gate)) * up).astype(bf)
    even = c == 0
    for y in range(NY):
        res = jnp.dot(h_ref[...], wd_ref[:, 2 * y * COLS : (2 * y + 2) * COLS], preferred_element_type=f32)
        low, high = res[:, 0:COLS], res[:, COLS:]
        mine_ref[y] = jnp.where(even, low, high).astype(bf)
        theirs_ref[y] = jnp.where(even, high, low).astype(bf)


def gather_sum(in_ref, out_ref, rows_ref):
    acc = in_ref[0].astype(f32)
    for y in range(1, NY):
        acc = acc + in_ref[y].astype(f32)
    rows_ref[...] = acc
    pad = jnp.zeros((SLOT - CAP, COLS), f32)
    for i in range(NSP):
        out_ref[i] = jnp.concatenate([rows_ref[CAP * i : CAP * i + CAP, :], pad], axis=0).astype(bf)


def finish(ret_ref, slots_ref, rw_ref, stream_ref, out_ref):
    slots = slots_ref[...].astype(f32).T
    weight = jnp.concatenate([rw_ref[...], jnp.zeros((6, TOK), f32)], axis=0).T
    lane = lax.broadcasted_iota(jnp.int32, (TOK, PADROWS), 1).astype(f32)
    out = stream_ref[...]
    for k in range(2):
        pick = jnp.where(lane == slots[:, k : k + 1], 1.0, 0.0).astype(bf)
        got = jnp.dot(pick, ret_ref[...], preferred_element_type=f32)
        out = out + weight[:, k : k + 1] * got
    out_ref[...] = out.astype(bf)


def to_all(v, axis):
    n = lax.axis_size(axis)
    return lax.all_to_all(jnp.broadcast_to(v[None], (n, *v.shape)), axis, 0, 0, tiled=True)


def exchange(v, axis):
    return lax.all_to_all(v, axis, 0, 0, tiled=True)


def local(
    queries,
    keys,
    values,
    cum_gate,
    out_weight,
    resid,
    norm_gain,
    routes,
    route_weight,
    gate_weight,
    up_weight,
    down_weight,
):
    z, x, y, c = (lax.axis_index(a) for a in ("z", "x", "y", "c"))
    sds = jax.ShapeDtypeStruct
    col = (y * NC + c) * COLS
    w_cols = exchange(out_weight.reshape(HD, NTP, COLS).transpose(1, 0, 2), TP).reshape(NTP * HD, COLS)
    resid_cols = lax.dynamic_slice_in_dim(resid, col, COLS, 1)
    gain_cols = lax.dynamic_slice_in_dim(norm_gain, col, COLS, 0).reshape(1, COLS)
    gate_keys = lax.dynamic_slice_in_dim(cum_gate[0], z * KEYS, KEYS, 0).reshape(NX, TOK)
    firsts = cum_gate.reshape(NZ, KEYS)[:, 0:1]
    offset = lax.dynamic_slice_in_dim(cum_gate, (z * NX + x) * TOK, TOK, 1) - firsts

    kv = to_all(jnp.concatenate([keys.T, values.T], axis=0), "x")
    q = to_all(queries.T, "z")
    at = jnp.stack([z, x]).astype(jnp.int32)
    parts = call(
        attend,
        sds((NZ, HD + 16, TOK), bf),
        (at, q, kv, gate_keys),
        smem=1,
        scratch=(pltpu.VMEM((KEYS, 2 * HD), bf), pltpu.VMEM((HD + 16, KEYS), bf)),
    )
    parts = exchange(parts, "z")
    attended = call(merge, sds((HD, TOK), bf), (parts, offset))
    attended = lax.all_gather(attended, TP, axis=0, tiled=True)
    stream, outgoing, slots = call(
        project,
        (sds((TOK, COLS), f32), sds((NSP, SLOT, COLS), bf), sds((8, TOK), jnp.int32)),
        (attended, w_cols, resid_cols, gain_cols, routes.T),
    )
    arrived = exchange(outgoing, SP)
    rows = call(squeeze, sds((ROWS + META, COLS), bf), (arrived,), scratch=(pltpu.VMEM((ROWS + META, COLS), f32),))
    own = to_all(rows, "y")
    swap = [(0, 1), (1, 0)]
    other = lax.ppermute(own, "c", swap)
    big = sds((NY, ROWS, COLS), bf)
    mine, theirs = call(
        experts,
        (big, big),
        (c.reshape(1).astype(jnp.int32), own, other, gate_weight[0], up_weight[0], down_weight[0]),
        smem=1,
        scratch=(pltpu.VMEM((ROWS, FFL), f32), pltpu.VMEM((ROWS, FFL), f32), pltpu.VMEM((ROWS, FFL), bf)),
    )
    theirs = lax.ppermute(theirs, "c", swap)
    pair = (mine.astype(f32) + theirs.astype(f32)).astype(bf)
    pair = exchange(pair, "y")
    back = call(gather_sum, sds((NSP, SLOT, COLS), bf), (pair,), scratch=(pltpu.VMEM((ROWS, COLS), f32),))
    returned = exchange(back, SP).reshape(PADROWS, COLS)
    return call(finish, sds((TOK, COLS), bf), (returned, slots, route_weight.T, stream))


def solution(mesh):
    grid = Mesh(mesh.devices.reshape(NZ, NX, NY, NC), ("z", "x", "y", "c"))
    return jax.shard_map(
        local,
        mesh=grid,
        in_specs=(
            P(SP, TP),
            P(SP, TP),
            P(SP, TP),
            P(TP, None),
            P(TP, None),
            P(SP, None),
            P(),
            P(SP, None),
            P(SP, None),
            P(SP, None, TP),
            P(SP, None, TP),
            P(SP, TP, None),
        ),
        out_specs=P(SP, TP),
        check_vma=False,
    )
```

```python
import jax
import jax.numpy as jnp
from jax import lax
from jax.experimental import pallas as pl
from jax.experimental.pallas import tpu as pltpu
from jax.sharding import Mesh, PartitionSpec as P


NZ, NX, NY, NC = 8, 4, 8, 2
NSP, NTP = NZ * NX, NY * NC
SP, TP = ("z", "x"), ("y", "c")
HD = 64
TOK = 256
D = 2048
COLS = D // NTP
KEYS = NX * TOK
CAP = 20
SLOT = 24
SEND = 48
ROWS = NSP * CAP
PADROWS = NSP * SLOT
META = 16
FFL = 256
EPS = 1e-06
LOW = -1e30
bf = jnp.bfloat16
f32 = jnp.float32

INTERPRET = False


def call(body, out_shape, inputs, smem=0, scratch=(), limit=12):
    specs = [pl.BlockSpec(memory_space=pltpu.SMEM)] * smem
    specs += [pl.BlockSpec(memory_space=pltpu.VMEM)] * (len(inputs) - smem)
    many = isinstance(out_shape, (tuple, list))
    vm = pl.BlockSpec(memory_space=pltpu.VMEM)
    return pl.pallas_call(
        body,
        out_shape=out_shape,
        in_specs=specs,
        out_specs=tuple([vm] * len(out_shape)) if many else vm,
        scratch_shapes=list(scratch),
        interpret=INTERPRET,
        compiler_params=pltpu.CompilerParams(vmem_limit_bytes=limit * 1024 * 1024),
    )(*inputs)


def three(v):
    hi = v.astype(bf).astype(f32)
    rest = v - hi
    mid = rest.astype(bf).astype(f32)
    return hi, mid, rest - mid


def attend(at_ref, q_ref, kv_ref, gate_ref, out_ref, keys_ref, vals_ref):
    z, x = at_ref[0], at_ref[1]
    first = gate_ref[0:1, 0:1]
    row64 = lax.broadcasted_iota(jnp.int32, (HD, TOK), 0)
    for j in range(NX):
        bias = first - gate_ref[j : j + 1, :]
        hi, mid, lo = three(bias)
        extra = jnp.where(row64 == 0, hi, jnp.where(row64 == 1, mid, jnp.where(row64 == 2, lo, 0.0)))
        both = jnp.concatenate([kv_ref[j, 0:HD, :], extra.astype(bf)], axis=0)
        keys_ref[j * TOK : (j + 1) * TOK, :] = both.T
        vals_ref[0:HD, j * TOK : (j + 1) * TOK] = kv_ref[j, HD : 2 * HD, :]
        vals_ref[HD : HD + 16, j * TOK : (j + 1) * TOK] = jnp.ones((16, TOK), bf)
    ones = jnp.where(row64 < 3, 1.0, 0.0).astype(bf)
    row16 = lax.broadcasted_iota(jnp.int32, (16, TOK), 0)

    def part(zq, masked):
        q = jnp.concatenate([q_ref[zq] * bf(HD**-0.5), ones], axis=0)
        s = jnp.dot(keys_ref[...], q, preferred_element_type=f32)
        if masked:
            ki = lax.broadcasted_iota(jnp.int32, (KEYS, TOK), 0)
            qi = lax.broadcasted_iota(jnp.int32, (KEYS, TOK), 1) + x * TOK
            s = jnp.where(ki <= qi, s, LOW)
        m = jnp.max(s, axis=0, keepdims=True)
        p = jnp.exp(s - m).astype(bf)
        o = jnp.dot(vals_ref[...], p, preferred_element_type=f32)
        total = o[HD : HD + 1, :]
        hi, mid, lo = three(m + jnp.log(total))
        stats = jnp.where(row16 == 0, hi, jnp.where(row16 == 1, mid, jnp.where(row16 == 2, lo, 0.0)))
        out_ref[zq, 0:HD, :] = (o[0:HD, :] / total).astype(bf)
        out_ref[zq, HD : HD + 16, :] = stats.astype(bf)

    part(z, True)

    def later(zq, carry):
        part(zq, False)
        return carry

    lax.fori_loop(z + 1, NZ, later, 0)

    def earlier(zq, carry):
        out_ref[zq, 0:HD, :] = jnp.zeros((HD, TOK), bf)
        out_ref[zq, HD : HD + 16, :] = jnp.where(row16 == 0, LOW, 0.0).astype(bf)
        return carry

    lax.fori_loop(0, z, earlier, 0)


def merge(part_ref, off_ref, out_ref):
    ls = []
    for i in range(NZ):
        st = part_ref[i, HD : HD + 16, :].astype(f32)
        ls.append(st[0:1] + st[1:2] + st[2:3] + off_ref[i : i + 1, :])
    m = ls[0]
    for v in ls[1:]:
        m = jnp.maximum(m, v)
    acc = jnp.zeros((HD, TOK), f32)
    total = jnp.zeros((1, TOK), f32)
    for i in range(NZ):
        w = jnp.exp(ls[i] - m)
        total = total + w
        acc = acc + w * part_ref[i, 0:HD, :].astype(f32)
    out_ref[...] = (acc / total).astype(bf)


def project(at_ref, att_ref, w_ref, resid_ref, gain_ref, routes_ref, stream_ref, out_ref, slots_ref):
    c0 = pl.multiple_of(at_ref[0], COLS)
    c1 = pl.multiple_of(at_ref[1], COLS)
    weights = [jnp.concatenate([w_ref[t, q * HD : (q + 1) * HD, :] for t in range(NTP)], axis=0) for q in range(2)]
    w = jnp.concatenate(weights, axis=1)
    mixed = lax.dot_general(att_ref[...], w, (((0,), (0,)), ((), ())), preferred_element_type=f32)
    resid = jnp.concatenate([resid_ref[:, pl.ds(c0, COLS)], resid_ref[:, pl.ds(c1, COLS)]], axis=1)
    gain = jnp.concatenate([gain_ref[:, pl.ds(c0, COLS)], gain_ref[:, pl.ds(c1, COLS)]], axis=1)
    stream = resid.astype(f32) + mixed
    stream_ref[...] = jnp.where(at_ref[2] == 0, stream[:, 0:COLS], stream[:, COLS:])
    square = jnp.sum(stream * stream, axis=1, keepdims=True)
    hi = square.astype(bf)
    lo = (square - hi.astype(f32)).astype(bf)
    scaled = (stream * gain).astype(bf)
    wide = (TOK, COLS)
    rows = jnp.concatenate([scaled, jnp.broadcast_to(hi, wide), jnp.broadcast_to(lo, wide)], axis=1)
    e0, e1 = routes_ref[0:1, :], routes_ref[1:2, :]
    io = lax.broadcasted_iota(jnp.int32, (NSP, TOK), 0)
    h0, h1 = io == e0, io == e1
    hit = jnp.where(h0, 1.0, jnp.where(h1, 1.0, 0.0)).astype(bf)
    ia = lax.broadcasted_iota(jnp.int32, (TOK, TOK), 0)
    ib = lax.broadcasted_iota(jnp.int32, (TOK, TOK), 1)
    upper = jnp.where(ia < ib, 1.0, 0.0).astype(bf)
    before = jnp.dot(hit, upper, preferred_element_type=f32)
    r0 = jnp.sum(jnp.where(h0, before, 0.0), axis=0, keepdims=True).astype(jnp.int32)
    r1 = jnp.sum(jnp.where(h1, before, 0.0), axis=0, keepdims=True).astype(jnp.int32)
    slots_ref[...] = jnp.concatenate([e0 * SLOT + r0, e1 * SLOT + r1, jnp.zeros((6, TOK), jnp.int32)], axis=0)
    s0 = e0 * SEND + r0
    s1 = e1 * SEND + r1
    ir = lax.broadcasted_iota(jnp.int32, (NSP * SEND, TOK), 0)
    hits = (ir == s0) | (ir == s1) | (ir == s0 + CAP) | (ir == s1 + CAP)
    pick = jnp.where(hits, 1.0, 0.0).astype(bf)
    sent = jnp.dot(pick, rows, preferred_element_type=f32).reshape(NSP, SEND, 4 * COLS)
    shape = (NSP, SEND, COLS)
    rank = lax.broadcasted_iota(jnp.int32, shape, 1)
    lane = lax.broadcasted_iota(jnp.int32, shape, 2)
    data = jnp.where(rank < CAP, sent[:, :, 0:COLS], sent[:, :, COLS : 2 * COLS])
    same = (lane == rank) & (rank < CAP)
    mh = jnp.sum(jnp.where(same, sent[:, :, 2 * COLS : 3 * COLS], 0.0), axis=1, keepdims=True)
    ml = jnp.sum(jnp.where(same, sent[:, :, 3 * COLS :], 0.0), axis=1, keepdims=True)
    data = jnp.where(rank == 2 * CAP, mh, jnp.where(rank == 2 * CAP + 1, ml, data))
    out_ref[...] = data.astype(bf)


def squeeze(in_ref, all_ref, low_ref, high_ref, rows_ref):
    rank = lax.broadcasted_iota(jnp.int32, (NSP, SEND, COLS), 1)
    x = in_ref[...].astype(f32)
    part = jnp.sum(jnp.where((rank == 2 * CAP) | (rank == 2 * CAP + 1), x, 0.0), axis=1)
    lane = lax.broadcasted_iota(jnp.int32, (NSP, COLS), 1)
    part = jnp.where(lane < CAP, part, 0.0)
    packed = part[0:8]
    for g in range(1, 4):
        packed = packed + pltpu.roll(part[8 * g : 8 * g + 8], 32 * g, 1)
    hi = packed.astype(bf).astype(f32)
    for i in range(NSP):
        x = in_ref[i].astype(f32)
        rows_ref[ROWS + CAP * i : ROWS + CAP * i + CAP, :] = x[0:CAP, :]
        rows_ref[CAP * i : CAP * i + CAP, :] = x[CAP : 2 * CAP, :]
    rows_ref[2 * ROWS : 2 * ROWS + 8, :] = hi
    rows_ref[2 * ROWS + 8 : 2 * ROWS + META, :] = packed - hi
    all_ref[...] = rows_ref[...].astype(bf)
    high_ref[...] = rows_ref[0:ROWS, :].astype(bf)
    low_ref[...] = rows_ref[ROWS : 2 * ROWS + META, :].astype(bf)


PIECES = (
    (0, 0, 0, ROWS),
    (0, 1, 0, 0),
    (3, 0, 1, ROWS),
    (3, 1, 1, 0),
    (1, 0, 2, ROWS),
    (1, 1, 2, 0),
    (2, 0, 3, 0),
    (2, 1, 4, 0),
)
METAS = ((0, 2 * ROWS), (1, 2 * ROWS), (2, 2 * ROWS), (3, ROWS))


def experts(at_ref, *refs):
    owns, others = refs[0:5], refs[5:10]
    wg_ref, wu_ref, wd_ref, mine_ref, theirs_ref, g_ref, u_ref, h_ref = refs[10:]
    y, c = at_ref[0], at_ref[1]
    total = jnp.zeros((8, COLS), f32)
    for pieces in (owns, others):
        for n, at in METAS:
            meta = pieces[n][at : at + META, :].astype(f32)
            total = total + meta[0:8] + meta[8:16]
    scale8 = lax.rsqrt(total / D + EPS)
    shape = (ROWS, COLS)
    row = lax.broadcasted_iota(jnp.int32, shape, 0).astype(f32)
    lane = lax.broadcasted_iota(jnp.int32, shape, 1).astype(f32)
    src = jnp.floor((row + 0.5) * (1.0 / CAP))
    group = jnp.floor((src + 0.5) * 0.125)
    sub = src - 8.0 * group
    target = 32.0 * group + (row - CAP * src)
    spread = jnp.zeros(shape, f32)
    for a in range(8):
        spread = jnp.where(sub == a, scale8[a : a + 1, :], spread)
    scale = jnp.sum(jnp.where(lane == target, spread, 0.0), axis=1, keepdims=True)
    for step, (off, upper, n, at) in enumerate(PIECES):
        xx = jnp.concatenate([owns[n][at : at + ROWS, :], others[n][at : at + ROWS, :]], axis=1)
        block = lax.rem(y + off, NY // 2) + upper * (NY // 2)
        first = pl.multiple_of((2 * block + c) * COLS, COLS)
        second = pl.multiple_of((2 * block + 1 - c) * COLS, COLS)
        for w_ref, acc_ref in ((wg_ref, g_ref), (wu_ref, u_ref)):
            w = jnp.concatenate([w_ref[pl.ds(first, COLS), :], w_ref[pl.ds(second, COLS), :]], axis=0)
            part = jnp.dot(xx, w, preferred_element_type=f32)
            if step == 0:
                acc_ref[...] = part
            else:
                acc_ref[...] += part
    gate = g_ref[...] * scale
    up = u_ref[...] * scale
    h_ref[...] = (gate / (1.0 + jnp.exp(-gate)) * up).astype(bf)
    even = c == 0
    for y in range(NY):
        res = jnp.dot(h_ref[...], wd_ref[:, 2 * y * COLS : (2 * y + 2) * COLS], preferred_element_type=f32)
        low, high = res[:, 0:COLS], res[:, COLS:]
        mine_ref[y] = jnp.where(even, low, high).astype(bf)
        theirs_ref[y] = jnp.where(even, high, low).astype(bf)


def gather_sum(in_ref, out_ref, rows_ref):
    acc = in_ref[0].astype(f32)
    for y in range(1, NY):
        acc = acc + in_ref[y].astype(f32)
    rows_ref[...] = acc
    pad = jnp.zeros((SLOT - CAP, COLS), f32)
    for i in range(NSP):
        out_ref[i] = jnp.concatenate([rows_ref[CAP * i : CAP * i + CAP, :], pad], axis=0).astype(bf)


def finish(ret_ref, slots_ref, rw_ref, stream_ref, out_ref):
    slots = slots_ref[...].astype(f32).T
    weight = jnp.concatenate([rw_ref[...], jnp.zeros((6, TOK), f32)], axis=0).T
    lane = lax.broadcasted_iota(jnp.int32, (TOK, PADROWS), 1).astype(f32)
    out = stream_ref[...]
    for k in range(2):
        pick = jnp.where(lane == slots[:, k : k + 1], 1.0, 0.0).astype(bf)
        got = jnp.dot(pick, ret_ref[...], preferred_element_type=f32)
        out = out + weight[:, k : k + 1] * got
    out_ref[...] = out.astype(bf)


def to_all(v, axis):
    n = lax.axis_size(axis)
    return lax.all_to_all(jnp.broadcast_to(v[None], (n, *v.shape)), axis, 0, 0, tiled=True)


def shift(v, by):
    return lax.ppermute(v, "y", [(i, (i + by) % NY) for i in range(NY)])


def exchange(v, axis):
    return lax.all_to_all(v, axis, 0, 0, tiled=True)


def layer(
    queries,
    keys,
    values,
    cum_gate,
    out_weight,
    resid,
    norm_gain,
    routes,
    route_weight,
    gate_weight,
    up_weight,
    down_weight,
):
    z, x, y, c = (lax.axis_index(a) for a in ("z", "x", "y", "c"))
    sds = jax.ShapeDtypeStruct
    half = NY // 2
    w = out_weight.reshape(HD, 2, half, NC, COLS).transpose(2, 3, 1, 0, 4).reshape(NTP // 2, 2 * HD, COLS)
    w_cols = exchange(jnp.concatenate([w, w], axis=0), TP)
    low = (lax.rem(y, half) * NC + c) * COLS
    at_cols = jnp.stack([low, low + half * NC * COLS, y // half]).astype(jnp.int32)
    gate_keys = lax.dynamic_slice_in_dim(cum_gate[0], z * KEYS, KEYS, 0).reshape(NX, TOK)
    firsts = cum_gate.reshape(NZ, KEYS)[:, 0:1]
    offset = lax.dynamic_slice_in_dim(cum_gate, (z * NX + x) * TOK, TOK, 1) - firsts

    kv = to_all(jnp.concatenate([keys.T, values.T], axis=0), "x")
    at = jnp.stack([z, x]).astype(jnp.int32)
    q_send, kv, gate_keys, at, offset, at_cols = lax.optimization_barrier(
        (jnp.broadcast_to(queries.T[None], (NZ, HD, TOK)), kv, gate_keys, at, offset, at_cols)
    )
    q = exchange(q_send, "z")
    parts = call(
        attend,
        sds((NZ, HD + 16, TOK), bf),
        (at, q, kv, gate_keys),
        smem=1,
        scratch=(pltpu.VMEM((KEYS, 2 * HD), bf), pltpu.VMEM((HD + 16, KEYS), bf)),
    )
    parts = exchange(parts, "z")
    attended = call(merge, sds((HD, TOK), bf), (parts, offset))
    attended = lax.all_gather(attended, TP, axis=0, tiled=True)
    stream, outgoing, slots = call(
        project,
        (sds((TOK, COLS), f32), sds((NSP, SEND, COLS), bf), sds((8, TOK), jnp.int32)),
        (at_cols, attended, w_cols, resid, norm_gain.reshape(1, D), routes.T),
        smem=1,
    )
    arrived = exchange(outgoing, SP)
    rows = 2 * ROWS + META
    every, lower, higher = call(
        squeeze,
        (sds((rows, COLS), bf), sds((ROWS + META, COLS), bf), sds((ROWS, COLS), bf)),
        (arrived,),
        scratch=(pltpu.VMEM((rows, COLS), f32),),
    )
    swap = [(0, 1), (1, 0)]
    owns = [every]
    for v, by in ((every, 1), (every, -1), (lower, 2), (higher, -2)):
        owns.append(shift(v, by))
    others = []
    for v in owns:
        others.append(lax.ppermute(v, "c", swap))
    big = sds((NY, ROWS, COLS), bf)
    mine, theirs = call(
        experts,
        (big, big),
        (jnp.stack([y, c]).astype(jnp.int32), *owns, *others, gate_weight[0], up_weight[0], down_weight[0]),
        smem=1,
        scratch=(pltpu.VMEM((ROWS, FFL), f32), pltpu.VMEM((ROWS, FFL), f32), pltpu.VMEM((ROWS, FFL), bf)),
        limit=24,
    )
    theirs = lax.ppermute(theirs, "c", swap)
    pair = (mine.astype(f32) + theirs.astype(f32)).astype(bf)
    pair = exchange(pair, "y")
    back = call(gather_sum, sds((NSP, SLOT, COLS), bf), (pair,), scratch=(pltpu.VMEM((ROWS, COLS), f32),))
    returned = exchange(back, SP).reshape(PADROWS, COLS)
    return call(finish, sds((TOK, COLS), bf), (returned, slots, route_weight.T, stream))


def solution(mesh):
    grid = Mesh(mesh.devices.reshape(NZ, NX, NY, NC), ("z", "x", "y", "c"))
    return jax.shard_map(
        layer,
        mesh=grid,
        in_specs=(
            P(SP, TP),
            P(SP, TP),
            P(SP, TP),
            P(TP, None),
            P(TP, None),
            P(SP, None),
            P(),
            P(SP, None),
            P(SP, None),
            P(SP, None, TP),
            P(SP, None, TP),
            P(SP, TP, None),
        ),
        out_specs=P(SP, TP),
        check_vma=False,
    )
```

```python
import jax
import jax.numpy as jnp
from jax import lax
from jax.experimental import pallas as pl
from jax.experimental.pallas import tpu as pltpu
from jax.sharding import Mesh, PartitionSpec as P


NZ, NX, NY, NC = 8, 4, 8, 2
NSP, NTP = NZ * NX, NY * NC
SP, TP = ("z", "x"), ("y", "c")
HD = 64
TOK = 256
D = 2048
COLS = D // NTP
KEYS = NX * TOK
CAP = 20
SLOT = 24
SEND = 48
ROWS = NSP * CAP
PADROWS = NSP * SLOT
META = 16
FFL = 256
EPS = 1e-06
LOW = -1e30
bf = jnp.bfloat16
f32 = jnp.float32

INTERPRET = False


def call(body, out_shape, inputs, smem=0, scratch=(), limit=12):
    specs = [pl.BlockSpec(memory_space=pltpu.SMEM)] * smem
    specs += [pl.BlockSpec(memory_space=pltpu.VMEM)] * (len(inputs) - smem)
    many = isinstance(out_shape, (tuple, list))
    vm = pl.BlockSpec(memory_space=pltpu.VMEM)
    return pl.pallas_call(
        body,
        out_shape=out_shape,
        in_specs=specs,
        out_specs=tuple([vm] * len(out_shape)) if many else vm,
        scratch_shapes=list(scratch),
        interpret=INTERPRET,
        compiler_params=pltpu.CompilerParams(vmem_limit_bytes=limit * 1024 * 1024),
    )(*inputs)


def three(v):
    hi = v.astype(bf).astype(f32)
    rest = v - hi
    mid = rest.astype(bf).astype(f32)
    return hi, mid, rest - mid


def attend(at_ref, q_ref, kv0_ref, kv1_ref, kv2_ref, kv3_ref, gate_ref, out_ref, keys_ref, vals_ref):
    z, x = at_ref[0], at_ref[1]
    first = gate_ref[:, pl.ds(pl.multiple_of(z * KEYS, KEYS), TOK)][:, 0:1]
    row64 = lax.broadcasted_iota(jnp.int32, (HD, TOK), 0)
    for j, kv_ref in enumerate((kv0_ref, kv1_ref, kv2_ref, kv3_ref)):
        where = lax.rem(x + NX - j, NX)
        place = pl.multiple_of(where * TOK, TOK)
        bias = first - gate_ref[:, pl.ds(pl.multiple_of(z * KEYS + where * TOK, TOK), TOK)]
        hi, mid, lo = three(bias)
        extra = jnp.where(row64 == 0, hi, jnp.where(row64 == 1, mid, jnp.where(row64 == 2, lo, 0.0)))
        both = jnp.concatenate([kv_ref[0:HD, :], extra.astype(bf)], axis=0)
        keys_ref[pl.ds(place, TOK), :] = both.T
        vals_ref[0:HD, pl.ds(place, TOK)] = kv_ref[HD : 2 * HD, :]
        vals_ref[HD : HD + 16, pl.ds(place, TOK)] = jnp.ones((16, TOK), bf)
    ones = jnp.where(row64 < 3, 1.0, 0.0).astype(bf)
    row16 = lax.broadcasted_iota(jnp.int32, (16, TOK), 0)

    def part(zq, masked):
        q = jnp.concatenate([q_ref[zq] * bf(HD**-0.5), ones], axis=0)
        s = jnp.dot(keys_ref[...], q, preferred_element_type=f32)
        if masked:
            ki = lax.broadcasted_iota(jnp.int32, (KEYS, TOK), 0)
            qi = lax.broadcasted_iota(jnp.int32, (KEYS, TOK), 1) + x * TOK
            s = jnp.where(ki <= qi, s, LOW)
        m = jnp.max(s, axis=0, keepdims=True)
        p = jnp.exp(s - m).astype(bf)
        o = jnp.dot(vals_ref[...], p, preferred_element_type=f32)
        total = o[HD : HD + 1, :]
        hi, mid, lo = three(m + jnp.log(total))
        stats = jnp.where(row16 == 0, hi, jnp.where(row16 == 1, mid, jnp.where(row16 == 2, lo, 0.0)))
        out_ref[zq, 0:HD, :] = (o[0:HD, :] / total).astype(bf)
        out_ref[zq, HD : HD + 16, :] = stats.astype(bf)

    part(z, True)

    def later(zq, carry):
        part(zq, False)
        return carry

    lax.fori_loop(z + 1, NZ, later, 0)

    def earlier(zq, carry):
        out_ref[zq, 0:HD, :] = jnp.zeros((HD, TOK), bf)
        out_ref[zq, HD : HD + 16, :] = jnp.where(row16 == 0, LOW, 0.0).astype(bf)
        return carry

    lax.fori_loop(0, z, earlier, 0)


def merge(at_ref, part_ref, gate_ref, out_ref):
    ls = []
    place = pl.multiple_of(at_ref[0] * KEYS + at_ref[1] * TOK, TOK)
    mine = gate_ref[:, pl.ds(place, TOK)]
    for i in range(NZ):
        st = part_ref[i, HD : HD + 16, :].astype(f32)
        ls.append(st[0:1] + st[1:2] + st[2:3] + (mine - gate_ref[:, i * KEYS : i * KEYS + 1]))
    m = ls[0]
    for v in ls[1:]:
        m = jnp.maximum(m, v)
    acc = jnp.zeros((HD, TOK), f32)
    total = jnp.zeros((1, TOK), f32)
    for i in range(NZ):
        w = jnp.exp(ls[i] - m)
        total = total + w
        acc = acc + w * part_ref[i, 0:HD, :].astype(f32)
    out_ref[...] = (acc / total).astype(bf)


def spread_weight(w_ref, out_ref):
    for y in range(NY):
        for c in range(NC):
            for q in range(2):
                block = (y % (NY // 2) + q * (NY // 2)) * NC + c
                out_ref[y * NC + c, q * HD : (q + 1) * HD, :] = w_ref[:, block * COLS : (block + 1) * COLS]


def project(at_ref, att_ref, w_ref, resid_ref, gain_ref, routes_ref, stream_ref, out_ref, slots_ref):
    c0 = pl.multiple_of(at_ref[0], COLS)
    c1 = pl.multiple_of(at_ref[1], COLS)
    weights = [jnp.concatenate([w_ref[t, q * HD : (q + 1) * HD, :] for t in range(NTP)], axis=0) for q in range(2)]
    w = jnp.concatenate(weights, axis=1)
    mixed = lax.dot_general(att_ref[...], w, (((0,), (0,)), ((), ())), preferred_element_type=f32)
    resid = jnp.concatenate([resid_ref[:, pl.ds(c0, COLS)], resid_ref[:, pl.ds(c1, COLS)]], axis=1)
    gain = jnp.concatenate([gain_ref[:, pl.ds(c0, COLS)], gain_ref[:, pl.ds(c1, COLS)]], axis=1)
    stream = resid.astype(f32) + mixed
    stream_ref[...] = jnp.where(at_ref[2] == 0, stream[:, 0:COLS], stream[:, COLS:])
    square = jnp.sum(stream * stream, axis=1, keepdims=True)
    hi = square.astype(bf)
    lo = (square - hi.astype(f32)).astype(bf)
    scaled = (stream * gain).astype(bf)
    wide = (TOK, COLS)
    rows = jnp.concatenate([scaled, jnp.broadcast_to(hi, wide), jnp.broadcast_to(lo, wide)], axis=1)
    e0, e1 = routes_ref[0:1, :], routes_ref[1:2, :]
    io = lax.broadcasted_iota(jnp.int32, (NSP, TOK), 0)
    h0, h1 = io == e0, io == e1
    hit = jnp.where(h0, 1.0, jnp.where(h1, 1.0, 0.0)).astype(bf)
    ia = lax.broadcasted_iota(jnp.int32, (TOK, TOK), 0)
    ib = lax.broadcasted_iota(jnp.int32, (TOK, TOK), 1)
    upper = jnp.where(ia < ib, 1.0, 0.0).astype(bf)
    before = jnp.dot(hit, upper, preferred_element_type=f32)
    r0 = jnp.sum(jnp.where(h0, before, 0.0), axis=0, keepdims=True).astype(jnp.int32)
    r1 = jnp.sum(jnp.where(h1, before, 0.0), axis=0, keepdims=True).astype(jnp.int32)
    slots_ref[...] = jnp.concatenate([e0 * SLOT + r0, e1 * SLOT + r1, jnp.zeros((6, TOK), jnp.int32)], axis=0)
    s0 = e0 * SEND + r0
    s1 = e1 * SEND + r1
    ir = lax.broadcasted_iota(jnp.int32, (NSP * SEND, TOK), 0)
    hits = (ir == s0) | (ir == s1) | (ir == s0 + CAP) | (ir == s1 + CAP)
    pick = jnp.where(hits, 1.0, 0.0).astype(bf)
    sent = jnp.dot(pick, rows, preferred_element_type=f32).reshape(NSP, SEND, 4 * COLS)
    shape = (NSP, SEND, COLS)
    rank = lax.broadcasted_iota(jnp.int32, shape, 1)
    lane = lax.broadcasted_iota(jnp.int32, shape, 2)
    data = jnp.where(rank < CAP, sent[:, :, 0:COLS], sent[:, :, COLS : 2 * COLS])
    same = (lane == rank) & (rank < CAP)
    mh = jnp.sum(jnp.where(same, sent[:, :, 2 * COLS : 3 * COLS], 0.0), axis=1, keepdims=True)
    ml = jnp.sum(jnp.where(same, sent[:, :, 3 * COLS :], 0.0), axis=1, keepdims=True)
    data = jnp.where(rank == 2 * CAP, mh, jnp.where(rank == 2 * CAP + 1, ml, data))
    out_ref[...] = data.astype(bf)


def squeeze(in_ref, all_ref, low_ref, high_ref, rows_ref):
    rank = lax.broadcasted_iota(jnp.int32, (NSP, SEND, COLS), 1)
    x = in_ref[...].astype(f32)
    part = jnp.sum(jnp.where((rank == 2 * CAP) | (rank == 2 * CAP + 1), x, 0.0), axis=1)
    lane = lax.broadcasted_iota(jnp.int32, (NSP, COLS), 1)
    part = jnp.where(lane < CAP, part, 0.0)
    packed = part[0:8]
    for g in range(1, 4):
        packed = packed + pltpu.roll(part[8 * g : 8 * g + 8], 32 * g, 1)
    hi = packed.astype(bf).astype(f32)
    for i in range(NSP):
        x = in_ref[i].astype(f32)
        rows_ref[ROWS + CAP * i : ROWS + CAP * i + CAP, :] = x[0:CAP, :]
        rows_ref[CAP * i : CAP * i + CAP, :] = x[CAP : 2 * CAP, :]
    rows_ref[2 * ROWS : 2 * ROWS + 8, :] = hi
    rows_ref[2 * ROWS + 8 : 2 * ROWS + META, :] = packed - hi
    all_ref[...] = rows_ref[...].astype(bf)
    high_ref[...] = rows_ref[0:ROWS, :].astype(bf)
    low_ref[...] = rows_ref[ROWS : 2 * ROWS + META, :].astype(bf)


PIECES = (
    (0, 0, 0, ROWS),
    (0, 1, 0, 0),
    (3, 0, 1, ROWS),
    (3, 1, 1, 0),
    (1, 0, 2, ROWS),
    (1, 1, 2, 0),
    (2, 0, 3, 0),
    (2, 1, 4, 0),
)
METAS = ((0, 2 * ROWS), (1, 2 * ROWS), (2, 2 * ROWS), (3, ROWS))


def experts(at_ref, *refs):
    every, near, far = refs[5:8]
    rows = 2 * ROWS + META
    owns = refs[0:5]
    others = (every, near.at[0:rows], near.at[rows:], far.at[0 : ROWS + META], far.at[ROWS + META :])
    wg_ref, wu_ref, wd_ref, mine_ref, theirs_ref, g_ref, u_ref, h_ref = refs[8:]
    y, c = at_ref[0], at_ref[1]
    total = jnp.zeros((8, COLS), f32)
    for pieces in (owns, others):
        for n, at in METAS:
            meta = pieces[n][at : at + META, :].astype(f32)
            total = total + meta[0:8] + meta[8:16]
    scale8 = lax.rsqrt(total / D + EPS)
    shape = (ROWS, COLS)
    row = lax.broadcasted_iota(jnp.int32, shape, 0).astype(f32)
    lane = lax.broadcasted_iota(jnp.int32, shape, 1).astype(f32)
    src = jnp.floor((row + 0.5) * (1.0 / CAP))
    group = jnp.floor((src + 0.5) * 0.125)
    sub = src - 8.0 * group
    target = 32.0 * group + (row - CAP * src)
    spread = jnp.zeros(shape, f32)
    for a in range(8):
        spread = jnp.where(sub == a, scale8[a : a + 1, :], spread)
    scale = jnp.sum(jnp.where(lane == target, spread, 0.0), axis=1, keepdims=True)
    for step, (off, upper, n, at) in enumerate(PIECES):
        xx = jnp.concatenate([owns[n][at : at + ROWS, :], others[n][at : at + ROWS, :]], axis=1)
        block = lax.rem(y + off, NY // 2) + upper * (NY // 2)
        first = pl.multiple_of((2 * block + c) * COLS, COLS)
        second = pl.multiple_of((2 * block + 1 - c) * COLS, COLS)
        for w_ref, acc_ref in ((wg_ref, g_ref), (wu_ref, u_ref)):
            w = jnp.concatenate([w_ref[pl.ds(first, COLS), :], w_ref[pl.ds(second, COLS), :]], axis=0)
            part = jnp.dot(xx, w, preferred_element_type=f32)
            if step == 0:
                acc_ref[...] = part
            else:
                acc_ref[...] += part
    gate = g_ref[...] * scale
    up = u_ref[...] * scale
    h_ref[...] = (gate / (1.0 + jnp.exp(-gate)) * up).astype(bf)
    even = c == 0
    for y in range(NY):
        res = jnp.dot(h_ref[...], wd_ref[:, 2 * y * COLS : (2 * y + 2) * COLS], preferred_element_type=f32)
        low, high = res[:, 0:COLS], res[:, COLS:]
        mine_ref[y] = jnp.where(even, low, high).astype(bf)
        theirs_ref[y] = jnp.where(even, high, low).astype(bf)


def gather_sum(in_ref, out_ref, rows_ref):
    acc = in_ref[0].astype(f32)
    for y in range(1, NY):
        acc = acc + in_ref[y].astype(f32)
    rows_ref[...] = acc
    pad = jnp.zeros((SLOT - CAP, COLS), f32)
    for i in range(NSP):
        out_ref[i] = jnp.concatenate([rows_ref[CAP * i : CAP * i + CAP, :], pad], axis=0).astype(bf)


def finish(ret_ref, slots_ref, rw_ref, stream_ref, out_ref):
    slots = slots_ref[...].astype(f32).T
    weight = jnp.concatenate([rw_ref[...], jnp.zeros((6, TOK), f32)], axis=0).T
    lane = lax.broadcasted_iota(jnp.int32, (TOK, PADROWS), 1).astype(f32)
    out = stream_ref[...]
    for k in range(2):
        pick = jnp.where(lane == slots[:, k : k + 1], 1.0, 0.0).astype(bf)
        got = jnp.dot(pick, ret_ref[...], preferred_element_type=f32)
        out = out + weight[:, k : k + 1] * got
    out_ref[...] = out.astype(bf)


def to_all(v, axis):
    n = lax.axis_size(axis)
    return lax.all_to_all(jnp.broadcast_to(v[None], (n, *v.shape)), axis, 0, 0, tiled=True)


def shift(v, by):
    return lax.ppermute(v, "y", [(i, (i + by) % NY) for i in range(NY)])


def exchange(v, axis):
    return lax.all_to_all(v, axis, 0, 0, tiled=True)


def layer(
    queries,
    keys,
    values,
    cum_gate,
    out_weight,
    resid,
    norm_gain,
    routes,
    route_weight,
    gate_weight,
    up_weight,
    down_weight,
):
    z, x, y, c = (lax.axis_index(a) for a in ("z", "x", "y", "c"))
    sds = jax.ShapeDtypeStruct
    half = NY // 2
    low = (lax.rem(y, half) * NC + c) * COLS
    at_cols = jnp.stack([low, low + half * NC * COLS, y // half]).astype(jnp.int32)
    at = jnp.stack([z, x]).astype(jnp.int32)
    q = to_all(queries.T, "z")
    w_send = call(spread_weight, sds((NTP, 2 * HD, COLS), bf), (out_weight,))
    w_cols = exchange(w_send, TP)
    kv = [jnp.concatenate([keys.T, values.T], axis=0)]
    for n in range(1, NX):
        kv.append(lax.ppermute(kv[0], "x", [(i, (i + n) % NX) for i in range(NX)]))
    parts = call(
        attend,
        sds((NZ, HD + 16, TOK), bf),
        (at, q, *kv, cum_gate),
        smem=1,
        scratch=(pltpu.VMEM((KEYS, 2 * HD), bf), pltpu.VMEM((HD + 16, KEYS), bf)),
    )
    parts, w_cols = lax.optimization_barrier((parts, w_cols))
    parts = exchange(parts, "z")
    attended = call(merge, sds((HD, TOK), bf), (at, parts, cum_gate), smem=1)
    attended = lax.all_gather(attended, TP, axis=0, tiled=True)
    stream, outgoing, slots = call(
        project,
        (sds((TOK, COLS), f32), sds((NSP, SEND, COLS), bf), sds((8, TOK), jnp.int32)),
        (at_cols, attended, w_cols, resid, norm_gain.reshape(1, D), routes.T),
        smem=1,
    )
    arrived = exchange(outgoing, SP)
    rows = 2 * ROWS + META
    every, lower, higher = call(
        squeeze,
        (sds((rows, COLS), bf), sds((ROWS + META, COLS), bf), sds((ROWS, COLS), bf)),
        (arrived,),
        scratch=(pltpu.VMEM((rows, COLS), f32),),
    )
    swap = [(0, 1), (1, 0)]
    owns = [every]
    for v, by in ((every, 1), (every, -1), (lower, 2), (higher, -2)):
        owns.append(shift(v, by))
    others = []
    for v in (every, jnp.concatenate(owns[1:3], axis=0), jnp.concatenate(owns[3:5], axis=0)):
        others.append(lax.ppermute(v, "c", swap))
    big = sds((NY, ROWS, COLS), bf)
    mine, theirs = call(
        experts,
        (big, big),
        (jnp.stack([y, c]).astype(jnp.int32), *owns, *others, gate_weight[0], up_weight[0], down_weight[0]),
        smem=1,
        scratch=(pltpu.VMEM((ROWS, FFL), f32), pltpu.VMEM((ROWS, FFL), f32), pltpu.VMEM((ROWS, FFL), bf)),
        limit=24,
    )
    theirs = lax.ppermute(theirs, "c", swap)
    pair = (mine.astype(f32) + theirs.astype(f32)).astype(bf)
    pair = exchange(pair, "y")
    back = call(gather_sum, sds((NSP, SLOT, COLS), bf), (pair,), scratch=(pltpu.VMEM((ROWS, COLS), f32),))
    returned = exchange(back, SP).reshape(PADROWS, COLS)
    return call(finish, sds((TOK, COLS), bf), (returned, slots, route_weight.T, stream))


def solution(mesh):
    grid = Mesh(mesh.devices.reshape(NZ, NX, NY, NC), ("z", "x", "y", "c"))
    return jax.shard_map(
        layer,
        mesh=grid,
        in_specs=(
            P(SP, TP),
            P(SP, TP),
            P(SP, TP),
            P(TP, None),
            P(TP, None),
            P(SP, None),
            P(),
            P(SP, None),
            P(SP, None),
            P(SP, None, TP),
            P(SP, None, TP),
            P(SP, TP, None),
        ),
        out_specs=P(SP, TP),
        check_vma=False,
    )
```

```python
import jax
import jax.numpy as jnp
from jax import lax
from jax.experimental import pallas as pl
from jax.experimental.pallas import tpu as pltpu
from jax.sharding import Mesh, PartitionSpec as P


NZ, NX, NY, NC = 8, 4, 8, 2
NSP, NTP = NZ * NX, NY * NC
SP, TP = ("z", "x"), ("y", "c")
HD = 64
TOK = 256
D = 2048
COLS = D // NTP
ROW = NX * TOK
CAP = 20
SLOT = 24
SEND = 48
ROWS = NSP * CAP
PADROWS = NSP * SLOT
META = 16
FFL = 256
EPS = 1e-06
LOW = -1e30
bf = jnp.bfloat16
f32 = jnp.float32

INTERPRET = False


def call(body, out_shape, inputs, smem=0, scratch=(), limit=12):
    specs = [pl.BlockSpec(memory_space=pltpu.SMEM)] * smem
    specs += [pl.BlockSpec(memory_space=pltpu.VMEM)] * (len(inputs) - smem)
    many = isinstance(out_shape, (tuple, list))
    vm = pl.BlockSpec(memory_space=pltpu.VMEM)
    return pl.pallas_call(
        body,
        out_shape=out_shape,
        in_specs=specs,
        out_specs=tuple([vm] * len(out_shape)) if many else vm,
        scratch_shapes=list(scratch),
        interpret=INTERPRET,
        compiler_params=pltpu.CompilerParams(vmem_limit_bytes=limit * 1024 * 1024),
    )(*inputs)


def three(v):
    hi = v.astype(bf).astype(f32)
    rest = v - hi
    mid = rest.astype(bf).astype(f32)
    return hi, mid, rest - mid


def attend(at_ref, q0_ref, q1_ref, q2_ref, q3_ref, kv_ref, gate_ref, out_ref, qs_ref, s_ref, m_ref, acc_ref):
    z, x = at_ref[0], at_ref[1]
    first = gate_ref[:, pl.ds(pl.multiple_of(z * ROW, ROW), TOK)][:, 0:1]
    row64 = lax.broadcasted_iota(jnp.int32, (HD, TOK), 0)
    ones = jnp.where(row64 < 3, 1.0, 0.0).astype(bf)
    for j, q_ref in enumerate((q0_ref, q1_ref, q2_ref, q3_ref)):
        place = pl.multiple_of(lax.rem(x + NX - j, NX) * TOK, TOK)
        qs_ref[0:HD, pl.ds(place, TOK)] = q_ref[...] * bf(HD**-0.5)
        qs_ref[HD : 2 * HD, pl.ds(place, TOK)] = ones

    def scores(zk):
        place = pl.multiple_of(zk * ROW + x * TOK, TOK)
        hi, mid, lo = three(first - gate_ref[:, pl.ds(place, TOK)])
        extra = jnp.where(row64 == 0, hi, jnp.where(row64 == 1, mid, jnp.where(row64 == 2, lo, 0.0)))
        both = jnp.concatenate([kv_ref[zk, 0:HD, :], extra.astype(bf)], axis=0)
        return jnp.dot(both.T, qs_ref[...], preferred_element_type=f32)

    s = scores(z)
    ki = lax.broadcasted_iota(jnp.int32, (TOK, ROW), 0) + x * TOK
    qi = lax.broadcasted_iota(jnp.int32, (TOK, ROW), 1)
    s = jnp.where(ki <= qi, s, LOW)
    s_ref[z] = s
    m_ref[...] = jnp.broadcast_to(jnp.max(s, axis=0, keepdims=True), (8, ROW))

    def look(zk, carry):
        s = scores(zk)
        s_ref[zk] = s
        m_ref[...] = jnp.maximum(m_ref[...], jnp.max(s, axis=0, keepdims=True))
        return carry

    lax.fori_loop(0, z, look, 0)
    m = m_ref[0:1, :]
    acc_ref[...] = jnp.zeros((HD + 16, ROW), f32)

    def weigh(zk, carry):
        p = jnp.exp(s_ref[zk] - m).astype(bf)
        v = jnp.concatenate([kv_ref[zk, HD : 2 * HD, :], jnp.ones((16, TOK), bf)], axis=0)
        acc_ref[...] += jnp.dot(v, p, preferred_element_type=f32)
        return carry

    lax.fori_loop(0, z + 1, weigh, 0)
    row16 = lax.broadcasted_iota(jnp.int32, (16, ROW), 0)
    total = acc_ref[HD : HD + 1, :]
    hi, mid, lo = three(m + jnp.log(total))
    stats = jnp.where(row16 == 0, hi, jnp.where(row16 == 1, mid, jnp.where(row16 == 2, lo, 0.0))).astype(bf)
    o = (acc_ref[0:HD, :] / total).astype(bf)
    for j in range(NX):
        out_ref[j, 0:HD, :] = o[:, j * TOK : (j + 1) * TOK]
        out_ref[j, HD : HD + 16, :] = stats[:, j * TOK : (j + 1) * TOK]


def merge(part_ref, out_ref):
    ls = []
    for i in range(NX):
        st = part_ref[i, HD : HD + 16, :].astype(f32)
        ls.append(st[0:1] + st[1:2] + st[2:3])
    m = ls[0]
    for v in ls[1:]:
        m = jnp.maximum(m, v)
    acc = jnp.zeros((HD, TOK), f32)
    total = jnp.zeros((1, TOK), f32)
    for i in range(NX):
        w = jnp.exp(ls[i] - m)
        total = total + w
        acc = acc + w * part_ref[i, 0:HD, :].astype(f32)
    out_ref[...] = (acc / total).astype(bf)


def spread_weight(w_ref, out_ref):
    for y in range(NY):
        for c in range(NC):
            for q in range(2):
                block = (y % (NY // 2) + q * (NY // 2)) * NC + c
                out_ref[y * NC + c, q * HD : (q + 1) * HD, :] = w_ref[:, block * COLS : (block + 1) * COLS]


def project(at_ref, att_ref, w_ref, resid_ref, gain_ref, routes_ref, stream_ref, out_ref, slots_ref):
    c0 = pl.multiple_of(at_ref[0], COLS)
    c1 = pl.multiple_of(at_ref[1], COLS)
    weights = [jnp.concatenate([w_ref[t, q * HD : (q + 1) * HD, :] for t in range(NTP)], axis=0) for q in range(2)]
    w = jnp.concatenate(weights, axis=1)
    mixed = lax.dot_general(att_ref[...], w, (((0,), (0,)), ((), ())), preferred_element_type=f32)
    resid = jnp.concatenate([resid_ref[:, pl.ds(c0, COLS)], resid_ref[:, pl.ds(c1, COLS)]], axis=1)
    gain = jnp.concatenate([gain_ref[:, pl.ds(c0, COLS)], gain_ref[:, pl.ds(c1, COLS)]], axis=1)
    stream = resid.astype(f32) + mixed
    stream_ref[...] = jnp.where(at_ref[2] == 0, stream[:, 0:COLS], stream[:, COLS:])
    square = jnp.sum(stream * stream, axis=1, keepdims=True)
    hi = square.astype(bf)
    lo = (square - hi.astype(f32)).astype(bf)
    scaled = (stream * gain).astype(bf)
    wide = (TOK, COLS)
    rows = jnp.concatenate([scaled, jnp.broadcast_to(hi, wide), jnp.broadcast_to(lo, wide)], axis=1)
    e0, e1 = routes_ref[0:1, :], routes_ref[1:2, :]
    io = lax.broadcasted_iota(jnp.int32, (NSP, TOK), 0)
    h0, h1 = io == e0, io == e1
    hit = jnp.where(h0, 1.0, jnp.where(h1, 1.0, 0.0)).astype(bf)
    ia = lax.broadcasted_iota(jnp.int32, (TOK, TOK), 0)
    ib = lax.broadcasted_iota(jnp.int32, (TOK, TOK), 1)
    upper = jnp.where(ia < ib, 1.0, 0.0).astype(bf)
    before = jnp.dot(hit, upper, preferred_element_type=f32)
    r0 = jnp.sum(jnp.where(h0, before, 0.0), axis=0, keepdims=True).astype(jnp.int32)
    r1 = jnp.sum(jnp.where(h1, before, 0.0), axis=0, keepdims=True).astype(jnp.int32)
    slots_ref[...] = jnp.concatenate([e0 * SLOT + r0, e1 * SLOT + r1, jnp.zeros((6, TOK), jnp.int32)], axis=0)
    s0 = e0 * SEND + r0
    s1 = e1 * SEND + r1
    ir = lax.broadcasted_iota(jnp.int32, (NSP * SEND, TOK), 0)
    hits = (ir == s0) | (ir == s1) | (ir == s0 + CAP) | (ir == s1 + CAP)
    pick = jnp.where(hits, 1.0, 0.0).astype(bf)
    sent = jnp.dot(pick, rows, preferred_element_type=f32).reshape(NSP, SEND, 4 * COLS)
    shape = (NSP, SEND, COLS)
    rank = lax.broadcasted_iota(jnp.int32, shape, 1)
    lane = lax.broadcasted_iota(jnp.int32, shape, 2)
    data = jnp.where(rank < CAP, sent[:, :, 0:COLS], sent[:, :, COLS : 2 * COLS])
    same = (lane == rank) & (rank < CAP)
    mh = jnp.sum(jnp.where(same, sent[:, :, 2 * COLS : 3 * COLS], 0.0), axis=1, keepdims=True)
    ml = jnp.sum(jnp.where(same, sent[:, :, 3 * COLS :], 0.0), axis=1, keepdims=True)
    data = jnp.where(rank == 2 * CAP, mh, jnp.where(rank == 2 * CAP + 1, ml, data))
    out_ref[...] = data.astype(bf)


def squeeze(in_ref, all_ref, low_ref, high_ref, rows_ref):
    rank = lax.broadcasted_iota(jnp.int32, (NSP, SEND, COLS), 1)
    x = in_ref[...].astype(f32)
    part = jnp.sum(jnp.where((rank == 2 * CAP) | (rank == 2 * CAP + 1), x, 0.0), axis=1)
    lane = lax.broadcasted_iota(jnp.int32, (NSP, COLS), 1)
    part = jnp.where(lane < CAP, part, 0.0)
    packed = part[0:8]
    for g in range(1, 4):
        packed = packed + pltpu.roll(part[8 * g : 8 * g + 8], 32 * g, 1)
    hi = packed.astype(bf).astype(f32)
    for i in range(NSP):
        x = in_ref[i].astype(f32)
        rows_ref[ROWS + CAP * i : ROWS + CAP * i + CAP, :] = x[0:CAP, :]
        rows_ref[CAP * i : CAP * i + CAP, :] = x[CAP : 2 * CAP, :]
    rows_ref[2 * ROWS : 2 * ROWS + 8, :] = hi
    rows_ref[2 * ROWS + 8 : 2 * ROWS + META, :] = packed - hi
    all_ref[...] = rows_ref[...].astype(bf)
    high_ref[...] = rows_ref[0:ROWS, :].astype(bf)
    low_ref[...] = rows_ref[ROWS : 2 * ROWS + META, :].astype(bf)


PIECES = (
    (0, 0, 0, ROWS),
    (0, 1, 0, 0),
    (3, 0, 1, ROWS),
    (3, 1, 1, 0),
    (1, 0, 2, ROWS),
    (1, 1, 2, 0),
    (2, 0, 3, 0),
    (2, 1, 4, 0),
)
METAS = ((0, 2 * ROWS), (1, 2 * ROWS), (2, 2 * ROWS), (3, ROWS))


def experts(at_ref, *refs):
    every, near, far = refs[5:8]
    rows = 2 * ROWS + META
    owns = refs[0:5]
    others = (every, near.at[0:rows], near.at[rows:], far.at[0 : ROWS + META], far.at[ROWS + META :])
    wg_ref, wu_ref, wd_ref, mine_ref, theirs_ref, g_ref, u_ref, h_ref = refs[8:]
    y, c = at_ref[0], at_ref[1]
    total = jnp.zeros((8, COLS), f32)
    for pieces in (owns, others):
        for n, at in METAS:
            meta = pieces[n][at : at + META, :].astype(f32)
            total = total + meta[0:8] + meta[8:16]
    scale8 = lax.rsqrt(total / D + EPS)
    shape = (ROWS, COLS)
    row = lax.broadcasted_iota(jnp.int32, shape, 0).astype(f32)
    lane = lax.broadcasted_iota(jnp.int32, shape, 1).astype(f32)
    src = jnp.floor((row + 0.5) * (1.0 / CAP))
    group = jnp.floor((src + 0.5) * 0.125)
    sub = src - 8.0 * group
    target = 32.0 * group + (row - CAP * src)
    spread = jnp.zeros(shape, f32)
    for a in range(8):
        spread = jnp.where(sub == a, scale8[a : a + 1, :], spread)
    scale = jnp.sum(jnp.where(lane == target, spread, 0.0), axis=1, keepdims=True)
    for step, (off, upper, n, at) in enumerate(PIECES):
        xx = jnp.concatenate([owns[n][at : at + ROWS, :], others[n][at : at + ROWS, :]], axis=1)
        block = lax.rem(y + off, NY // 2) + upper * (NY // 2)
        first = pl.multiple_of((2 * block + c) * COLS, COLS)
        second = pl.multiple_of((2 * block + 1 - c) * COLS, COLS)
        for w_ref, acc_ref in ((wg_ref, g_ref), (wu_ref, u_ref)):
            w = jnp.concatenate([w_ref[pl.ds(first, COLS), :], w_ref[pl.ds(second, COLS), :]], axis=0)
            part = jnp.dot(xx, w, preferred_element_type=f32)
            if step == 0:
                acc_ref[...] = part
            else:
                acc_ref[...] += part
    gate = g_ref[...] * scale
    up = u_ref[...] * scale
    h_ref[...] = (gate / (1.0 + jnp.exp(-gate)) * up).astype(bf)
    even = c == 0
    for y in range(NY):
        res = jnp.dot(h_ref[...], wd_ref[:, 2 * y * COLS : (2 * y + 2) * COLS], preferred_element_type=f32)
        low, high = res[:, 0:COLS], res[:, COLS:]
        mine_ref[y] = jnp.where(even, low, high).astype(bf)
        theirs_ref[y] = jnp.where(even, high, low).astype(bf)


def gather_sum(in_ref, out_ref, rows_ref):
    acc = in_ref[0].astype(f32)
    for y in range(1, NY):
        acc = acc + in_ref[y].astype(f32)
    rows_ref[...] = acc
    pad = jnp.zeros((SLOT - CAP, COLS), f32)
    for i in range(NSP):
        out_ref[i] = jnp.concatenate([rows_ref[CAP * i : CAP * i + CAP, :], pad], axis=0).astype(bf)


def finish(ret_ref, slots_ref, rw_ref, stream_ref, out_ref):
    slots = slots_ref[...].astype(f32).T
    weight = jnp.concatenate([rw_ref[...], jnp.zeros((6, TOK), f32)], axis=0).T
    lane = lax.broadcasted_iota(jnp.int32, (TOK, PADROWS), 1).astype(f32)
    out = stream_ref[...]
    for k in range(2):
        pick = jnp.where(lane == slots[:, k : k + 1], 1.0, 0.0).astype(bf)
        got = jnp.dot(pick, ret_ref[...], preferred_element_type=f32)
        out = out + weight[:, k : k + 1] * got
    out_ref[...] = out.astype(bf)


def shift(v, by):
    return lax.ppermute(v, "y", [(i, (i + by) % NY) for i in range(NY)])


def exchange(v, axis):
    return lax.all_to_all(v, axis, 0, 0, tiled=True)


def layer(
    queries,
    keys,
    values,
    cum_gate,
    out_weight,
    resid,
    norm_gain,
    routes,
    route_weight,
    gate_weight,
    up_weight,
    down_weight,
):
    z, x, y, c = (lax.axis_index(a) for a in ("z", "x", "y", "c"))
    sds = jax.ShapeDtypeStruct
    half = NY // 2
    low = (lax.rem(y, half) * NC + c) * COLS
    at_cols = jnp.stack([low, low + half * NC * COLS, y // half]).astype(jnp.int32)
    at = jnp.stack([z, x]).astype(jnp.int32)
    w_send = call(spread_weight, sds((NTP, 2 * HD, COLS), bf), (out_weight,))
    kv = jnp.concatenate([keys.T, values.T], axis=0)
    kv, w_send, at, at_cols = lax.optimization_barrier(
        (jnp.broadcast_to(kv[None], (NZ, 2 * HD, TOK)), w_send, at, at_cols)
    )
    kv = exchange(kv, "z")
    w_cols = exchange(w_send, TP)
    q = [queries.T]
    for n in range(1, NX):
        q.append(lax.ppermute(q[0], "x", [(i, (i + n) % NX) for i in range(NX)]))
    parts = call(
        attend,
        sds((NX, HD + 16, TOK), bf),
        (at, *q, kv, cum_gate),
        smem=1,
        scratch=(
            pltpu.VMEM((2 * HD, ROW), bf),
            pltpu.VMEM((NZ, TOK, ROW), f32),
            pltpu.VMEM((8, ROW), f32),
            pltpu.VMEM((HD + 16, ROW), f32),
        ),
        limit=24,
    )
    parts, w_cols = lax.optimization_barrier((parts, w_cols))
    parts = exchange(parts, "x")
    attended = call(merge, sds((HD, TOK), bf), (parts,))
    attended = lax.all_gather(attended, TP, axis=0, tiled=True)
    stream, outgoing, slots = call(
        project,
        (sds((TOK, COLS), f32), sds((NSP, SEND, COLS), bf), sds((8, TOK), jnp.int32)),
        (at_cols, attended, w_cols, resid, norm_gain.reshape(1, D), routes.T),
        smem=1,
    )
    arrived = exchange(outgoing, SP)
    rows = 2 * ROWS + META
    every, lower, higher = call(
        squeeze,
        (sds((rows, COLS), bf), sds((ROWS + META, COLS), bf), sds((ROWS, COLS), bf)),
        (arrived,),
        scratch=(pltpu.VMEM((rows, COLS), f32),),
    )
    swap = [(0, 1), (1, 0)]
    owns = [every]
    for v, by in ((every, 1), (every, -1), (lower, 2), (higher, -2)):
        owns.append(shift(v, by))
    others = []
    for v in (every, jnp.concatenate(owns[1:3], axis=0), jnp.concatenate(owns[3:5], axis=0)):
        others.append(lax.ppermute(v, "c", swap))
    big = sds((NY, ROWS, COLS), bf)
    mine, theirs = call(
        experts,
        (big, big),
        (jnp.stack([y, c]).astype(jnp.int32), *owns, *others, gate_weight[0], up_weight[0], down_weight[0]),
        smem=1,
        scratch=(pltpu.VMEM((ROWS, FFL), f32), pltpu.VMEM((ROWS, FFL), f32), pltpu.VMEM((ROWS, FFL), bf)),
        limit=24,
    )
    theirs = lax.ppermute(theirs, "c", swap)
    pair = (mine.astype(f32) + theirs.astype(f32)).astype(bf)
    pair = exchange(pair, "y")
    back = call(gather_sum, sds((NSP, SLOT, COLS), bf), (pair,), scratch=(pltpu.VMEM((ROWS, COLS), f32),))
    returned = exchange(back, SP).reshape(PADROWS, COLS)
    return call(finish, sds((TOK, COLS), bf), (returned, slots, route_weight.T, stream))


def solution(mesh):
    grid = Mesh(mesh.devices.reshape(NZ, NX, NY, NC), ("z", "x", "y", "c"))
    return jax.shard_map(
        layer,
        mesh=grid,
        in_specs=(
            P(SP, TP),
            P(SP, TP),
            P(SP, TP),
            P(TP, None),
            P(TP, None),
            P(SP, None),
            P(),
            P(SP, None),
            P(SP, None),
            P(SP, None, TP),
            P(SP, None, TP),
            P(SP, TP, None),
        ),
        out_specs=P(SP, TP),
        check_vma=False,
    )
```

```python
import jax
import jax.numpy as jnp
from jax import lax
from jax.experimental import pallas as pl
from jax.experimental.pallas import tpu as pltpu
from jax.sharding import Mesh, PartitionSpec as P


NZ, NX, NY, NC = 8, 4, 8, 2
NSP, NTP = NZ * NX, NY * NC
Y = ("yh", "yl")
SP, TP = ("z", "x"), ("yh", "yl", "c")
HALF = NY // 2
HD = 64
TOK = 256
D = 2048
COLS = D // NTP
ROW = NX * TOK
CAP = 20
SLOT = 24
SEND = 48
ROWS = NSP * CAP
PADROWS = NSP * SLOT
META = 16
FFL = 256
EPS = 1e-06
LOW = -1e30
bf = jnp.bfloat16
f32 = jnp.float32

INTERPRET = False


def call(body, out_shape, inputs, smem=0, scratch=(), limit=12):
    specs = [pl.BlockSpec(memory_space=pltpu.SMEM)] * smem
    specs += [pl.BlockSpec(memory_space=pltpu.VMEM)] * (len(inputs) - smem)
    many = isinstance(out_shape, (tuple, list))
    vm = pl.BlockSpec(memory_space=pltpu.VMEM)
    return pl.pallas_call(
        body,
        out_shape=out_shape,
        in_specs=specs,
        out_specs=tuple([vm] * len(out_shape)) if many else vm,
        scratch_shapes=list(scratch),
        interpret=INTERPRET,
        compiler_params=pltpu.CompilerParams(vmem_limit_bytes=limit * 1024 * 1024),
    )(*inputs)


def three(v):
    hi = v.astype(bf).astype(f32)
    rest = v - hi
    mid = rest.astype(bf).astype(f32)
    return hi, mid, rest - mid


def attend(at_ref, q0_ref, q1_ref, q2_ref, q3_ref, kv_ref, gate_ref, out_ref, qs_ref, s_ref, m_ref, acc_ref):
    z, x = at_ref[0], at_ref[1]
    first = gate_ref[:, pl.ds(pl.multiple_of(z * ROW, ROW), TOK)][:, 0:1]
    row64 = lax.broadcasted_iota(jnp.int32, (HD, TOK), 0)
    ones = jnp.where(row64 < 3, 1.0, 0.0).astype(bf)
    for j, q_ref in enumerate((q0_ref, q1_ref, q2_ref, q3_ref)):
        place = pl.multiple_of(lax.rem(x + NX - j, NX) * TOK, TOK)
        qs_ref[0:HD, pl.ds(place, TOK)] = q_ref[...] * bf(HD**-0.5)
        qs_ref[HD : 2 * HD, pl.ds(place, TOK)] = ones

    def scores(zk):
        place = pl.multiple_of(zk * ROW + x * TOK, TOK)
        hi, mid, lo = three(first - gate_ref[:, pl.ds(place, TOK)])
        extra = jnp.where(row64 == 0, hi, jnp.where(row64 == 1, mid, jnp.where(row64 == 2, lo, 0.0)))
        both = jnp.concatenate([kv_ref[zk, 0:HD, :], extra.astype(bf)], axis=0)
        return jnp.dot(both.T, qs_ref[...], preferred_element_type=f32)

    s = scores(z)
    ki = lax.broadcasted_iota(jnp.int32, (TOK, ROW), 0) + x * TOK
    qi = lax.broadcasted_iota(jnp.int32, (TOK, ROW), 1)
    s = jnp.where(ki <= qi, s, LOW)
    s_ref[z] = s
    m_ref[...] = jnp.broadcast_to(jnp.max(s, axis=0, keepdims=True), (8, ROW))

    def look(zk, carry):
        s = scores(zk)
        s_ref[zk] = s
        m_ref[...] = jnp.maximum(m_ref[...], jnp.max(s, axis=0, keepdims=True))
        return carry

    lax.fori_loop(0, z, look, 0)
    m = m_ref[0:1, :]
    acc_ref[...] = jnp.zeros((HD + 16, ROW), f32)

    def weigh(zk, carry):
        p = jnp.exp(s_ref[zk] - m).astype(bf)
        v = jnp.concatenate([kv_ref[zk, HD : 2 * HD, :], jnp.ones((16, TOK), bf)], axis=0)
        acc_ref[...] += jnp.dot(v, p, preferred_element_type=f32)
        return carry

    lax.fori_loop(0, z + 1, weigh, 0)
    row16 = lax.broadcasted_iota(jnp.int32, (16, ROW), 0)
    total = acc_ref[HD : HD + 1, :]
    hi, mid, lo = three(m + jnp.log(total))
    stats = jnp.where(row16 == 0, hi, jnp.where(row16 == 1, mid, jnp.where(row16 == 2, lo, 0.0))).astype(bf)
    o = (acc_ref[0:HD, :] / total).astype(bf)
    for j in range(NX):
        out_ref[j, 0:HD, :] = o[:, j * TOK : (j + 1) * TOK]
        out_ref[j, HD : HD + 16, :] = stats[:, j * TOK : (j + 1) * TOK]


def merge(part_ref, out_ref):
    ls = []
    for i in range(NX):
        st = part_ref[i, HD : HD + 16, :].astype(f32)
        ls.append(st[0:1] + st[1:2] + st[2:3])
    m = ls[0]
    for v in ls[1:]:
        m = jnp.maximum(m, v)
    acc = jnp.zeros((HD, TOK), f32)
    total = jnp.zeros((1, TOK), f32)
    for i in range(NX):
        w = jnp.exp(ls[i] - m)
        total = total + w
        acc = acc + w * part_ref[i, 0:HD, :].astype(f32)
    out_ref[...] = (acc / total).astype(bf)


def spread_weight(w_ref, out_ref):
    for y in range(NY):
        for c in range(NC):
            for q in range(2):
                block = (y % (NY // 2) + q * (NY // 2)) * NC + c
                out_ref[y * NC + c, q * HD : (q + 1) * HD, :] = w_ref[:, block * COLS : (block + 1) * COLS]


def project(at_ref, att_ref, w_ref, resid_ref, gain_ref, routes_ref, stream_ref, out_ref, slots_ref):
    c0 = pl.multiple_of(at_ref[0], COLS)
    c1 = pl.multiple_of(at_ref[1], COLS)
    weights = [jnp.concatenate([w_ref[t, q * HD : (q + 1) * HD, :] for t in range(NTP)], axis=0) for q in range(2)]
    w = jnp.concatenate(weights, axis=1)
    mixed = lax.dot_general(att_ref[...], w, (((0,), (0,)), ((), ())), preferred_element_type=f32)
    resid = jnp.concatenate([resid_ref[:, pl.ds(c0, COLS)], resid_ref[:, pl.ds(c1, COLS)]], axis=1)
    gain = jnp.concatenate([gain_ref[:, pl.ds(c0, COLS)], gain_ref[:, pl.ds(c1, COLS)]], axis=1)
    stream = resid.astype(f32) + mixed
    stream_ref[...] = jnp.where(at_ref[2] == 0, stream[:, 0:COLS], stream[:, COLS:])
    square = jnp.sum(stream * stream, axis=1, keepdims=True)
    hi = square.astype(bf)
    lo = (square - hi.astype(f32)).astype(bf)
    scaled = (stream * gain).astype(bf)
    wide = (TOK, COLS)
    rows = jnp.concatenate([scaled, jnp.broadcast_to(hi, wide), jnp.broadcast_to(lo, wide)], axis=1)
    e0, e1 = routes_ref[0:1, :], routes_ref[1:2, :]
    io = lax.broadcasted_iota(jnp.int32, (NSP, TOK), 0)
    h0, h1 = io == e0, io == e1
    hit = jnp.where(h0, 1.0, jnp.where(h1, 1.0, 0.0)).astype(bf)
    ia = lax.broadcasted_iota(jnp.int32, (TOK, TOK), 0)
    ib = lax.broadcasted_iota(jnp.int32, (TOK, TOK), 1)
    upper = jnp.where(ia < ib, 1.0, 0.0).astype(bf)
    before = jnp.dot(hit, upper, preferred_element_type=f32)
    r0 = jnp.sum(jnp.where(h0, before, 0.0), axis=0, keepdims=True).astype(jnp.int32)
    r1 = jnp.sum(jnp.where(h1, before, 0.0), axis=0, keepdims=True).astype(jnp.int32)
    slots_ref[...] = jnp.concatenate([2 * SLOT * e0 + r0, 2 * SLOT * e1 + r1, jnp.zeros((6, TOK), jnp.int32)], axis=0)
    s0 = e0 * SEND + r0
    s1 = e1 * SEND + r1
    ir = lax.broadcasted_iota(jnp.int32, (NSP * SEND, TOK), 0)
    hits = (ir == s0) | (ir == s1) | (ir == s0 + CAP) | (ir == s1 + CAP)
    pick = jnp.where(hits, 1.0, 0.0).astype(bf)
    sent = jnp.dot(pick, rows, preferred_element_type=f32).reshape(NSP, SEND, 4 * COLS)
    shape = (NSP, SEND, COLS)
    rank = lax.broadcasted_iota(jnp.int32, shape, 1)
    lane = lax.broadcasted_iota(jnp.int32, shape, 2)
    data = jnp.where(rank < CAP, sent[:, :, 0:COLS], sent[:, :, COLS : 2 * COLS])
    same = (lane == rank) & (rank < CAP)
    mh = jnp.sum(jnp.where(same, sent[:, :, 2 * COLS : 3 * COLS], 0.0), axis=1, keepdims=True)
    ml = jnp.sum(jnp.where(same, sent[:, :, 3 * COLS :], 0.0), axis=1, keepdims=True)
    data = jnp.where(rank == 2 * CAP, mh, jnp.where(rank == 2 * CAP + 1, ml, data))
    out_ref[...] = data.astype(bf)


def squeeze(in_ref, all_ref, low_ref, high_ref, rows_ref):
    rank = lax.broadcasted_iota(jnp.int32, (NSP, SEND, COLS), 1)
    x = in_ref[...].astype(f32)
    part = jnp.sum(jnp.where((rank == 2 * CAP) | (rank == 2 * CAP + 1), x, 0.0), axis=1)
    lane = lax.broadcasted_iota(jnp.int32, (NSP, COLS), 1)
    part = jnp.where(lane < CAP, part, 0.0)
    packed = part[0:8]
    for g in range(1, 4):
        packed = packed + pltpu.roll(part[8 * g : 8 * g + 8], 32 * g, 1)
    hi = packed.astype(bf).astype(f32)
    for i in range(NSP):
        x = in_ref[i].astype(f32)
        rows_ref[ROWS + CAP * i : ROWS + CAP * i + CAP, :] = x[0:CAP, :]
        rows_ref[CAP * i : CAP * i + CAP, :] = x[CAP : 2 * CAP, :]
    rows_ref[2 * ROWS : 2 * ROWS + 8, :] = hi
    rows_ref[2 * ROWS + 8 : 2 * ROWS + META, :] = packed - hi
    all_ref[...] = rows_ref[...].astype(bf)
    high_ref[...] = rows_ref[0:ROWS, :].astype(bf)
    low_ref[...] = rows_ref[ROWS : 2 * ROWS + META, :].astype(bf)


PIECES = (
    (0, 0, 0, ROWS),
    (0, 1, 0, 0),
    (3, 0, 1, ROWS),
    (3, 1, 1, 0),
    (1, 0, 2, ROWS),
    (1, 1, 2, 0),
    (2, 0, 3, 0),
    (2, 1, 4, 0),
)
METAS = ((0, 2 * ROWS), (1, 2 * ROWS), (2, 2 * ROWS), (3, ROWS))


SENDS = (
    (0, 0, 2, 0),
    (0, ROWS, 2, 1),
    (1, 0, 1, 0),
    (1, ROWS, 1, 1),
    (1, 2 * ROWS, 3, 0),
    (1, 3 * ROWS, 3, 1),
    (1, 4 * ROWS, 0, 0),
    (1, 5 * ROWS, 0, 1),
)


def experts(at_ref, *refs):
    every, near, far = refs[5:8]
    rows = 2 * ROWS + META
    owns = refs[0:5]
    others = (every, near.at[0:rows], near.at[rows:], far.at[0 : ROWS + META], far.at[ROWS + META :])
    wg_ref, wu_ref, wd_ref = refs[8:11]
    outs = refs[11:15]
    g_ref, u_ref, h_ref = refs[15:]
    y, c = at_ref[0], at_ref[1]
    total = jnp.zeros((8, COLS), f32)
    for pieces in (owns, others):
        for n, at in METAS:
            meta = pieces[n][at : at + META, :].astype(f32)
            total = total + meta[0:8] + meta[8:16]
    scale8 = lax.rsqrt(total / D + EPS)
    shape = (ROWS, COLS)
    row = lax.broadcasted_iota(jnp.int32, shape, 0).astype(f32)
    lane = lax.broadcasted_iota(jnp.int32, shape, 1).astype(f32)
    src = jnp.floor((row + 0.5) * (1.0 / CAP))
    group = jnp.floor((src + 0.5) * 0.125)
    sub = src - 8.0 * group
    target = 32.0 * group + (row - CAP * src)
    spread = jnp.zeros(shape, f32)
    for a in range(8):
        spread = jnp.where(sub == a, scale8[a : a + 1, :], spread)
    scale = jnp.sum(jnp.where(lane == target, spread, 0.0), axis=1, keepdims=True)
    for step, (off, upper, n, at) in enumerate(PIECES):
        xx = jnp.concatenate([owns[n][at : at + ROWS, :], others[n][at : at + ROWS, :]], axis=1)
        block = lax.rem(y + off, NY // 2) + upper * (NY // 2)
        first = pl.multiple_of((2 * block + c) * COLS, COLS)
        second = pl.multiple_of((2 * block + 1 - c) * COLS, COLS)
        for w_ref, acc_ref in ((wg_ref, g_ref), (wu_ref, u_ref)):
            w = jnp.concatenate([w_ref[pl.ds(first, COLS), :], w_ref[pl.ds(second, COLS), :]], axis=0)
            part = jnp.dot(xx, w, preferred_element_type=f32)
            if step == 0:
                acc_ref[...] = part
            else:
                acc_ref[...] += part
    gate = g_ref[...] * scale
    up = u_ref[...] * scale
    h_ref[...] = (gate / (1.0 + jnp.exp(-gate)) * up).astype(bf)
    even = c == 0
    for ref, at, off, upper in SENDS:
        block = lax.rem(y + off, HALF) + upper * HALF
        place = pl.multiple_of(2 * block * COLS, 2 * COLS)
        res = jnp.dot(h_ref[...], wd_ref[:, pl.ds(place, 2 * COLS)], preferred_element_type=f32)
        low, high = res[:, 0:COLS], res[:, COLS:]
        outs[ref][at : at + ROWS, :] = jnp.where(even, low, high).astype(bf)
        outs[ref + 2][at : at + ROWS, :] = jnp.where(even, high, low).astype(bf)


def gather_sum(mine_ref, theirs_ref, n0_ref, n1_ref, f0_ref, f1_ref, out_ref, rows_ref):
    base = 4 * ROWS
    pad = jnp.zeros((SLOT - CAP, COLS), f32)
    for q, far_ref in enumerate((f0_ref, f1_ref)):
        at = slice(q * ROWS, (q + 1) * ROWS)
        kept = slice(base + q * ROWS, base + (q + 1) * ROWS)
        acc = mine_ref[kept, :].astype(f32) + theirs_ref[kept, :].astype(f32)
        acc = acc + n0_ref[at, :].astype(f32) + n1_ref[at, :].astype(f32)
        rows_ref[...] = acc + far_ref[...].astype(f32)
        for i in range(NSP):
            out_ref[2 * i + q] = jnp.concatenate([rows_ref[CAP * i : CAP * i + CAP, :], pad], axis=0).astype(bf)


def finish(ret_ref, slots_ref, rw_ref, stream_ref, out_ref):
    slots = slots_ref[...].astype(f32).T
    weight = jnp.concatenate([rw_ref[...], jnp.zeros((6, TOK), f32)], axis=0).T
    lane = lax.broadcasted_iota(jnp.int32, (TOK, 2 * PADROWS), 1).astype(f32)
    out = stream_ref[...]
    for k in range(2):
        slot = slots[:, k : k + 1]
        pick = jnp.where((lane == slot) | (lane == slot + SLOT), 1.0, 0.0).astype(bf)
        got = jnp.dot(pick, ret_ref[...], preferred_element_type=f32)
        out = out + weight[:, k : k + 1] * got
    out_ref[...] = out.astype(bf)


def shift(v, by):
    return lax.ppermute(v, Y, [(i, (i + by) % NY) for i in range(NY)])


def exchange(v, axis):
    return lax.all_to_all(v, axis, 0, 0, tiled=True)


def layer(
    queries,
    keys,
    values,
    cum_gate,
    out_weight,
    resid,
    norm_gain,
    routes,
    route_weight,
    gate_weight,
    up_weight,
    down_weight,
):
    z, x, y, c = (lax.axis_index(a) for a in ("z", "x", Y, "c"))
    sds = jax.ShapeDtypeStruct
    half = NY // 2
    low = (lax.rem(y, half) * NC + c) * COLS
    at_cols = jnp.stack([low, low + half * NC * COLS, y // half]).astype(jnp.int32)
    at = jnp.stack([z, x]).astype(jnp.int32)
    w_send = call(spread_weight, sds((NTP, 2 * HD, COLS), bf), (out_weight,))
    kv = jnp.concatenate([keys.T, values.T], axis=0)
    kv, w_send, at, at_cols = lax.optimization_barrier(
        (jnp.broadcast_to(kv[None], (NZ, 2 * HD, TOK)), w_send, at, at_cols)
    )
    kv = exchange(kv, "z")
    w_cols = exchange(w_send, TP)
    q = [queries.T]
    for n in range(1, NX):
        q.append(lax.ppermute(q[0], "x", [(i, (i + n) % NX) for i in range(NX)]))
    parts = call(
        attend,
        sds((NX, HD + 16, TOK), bf),
        (at, *q, kv, cum_gate),
        smem=1,
        scratch=(
            pltpu.VMEM((2 * HD, ROW), bf),
            pltpu.VMEM((NZ, TOK, ROW), f32),
            pltpu.VMEM((8, ROW), f32),
            pltpu.VMEM((HD + 16, ROW), f32),
        ),
        limit=24,
    )
    parts, w_cols = lax.optimization_barrier((parts, w_cols))
    parts = exchange(parts, "x")
    attended = call(merge, sds((HD, TOK), bf), (parts,))
    attended = lax.all_gather(attended, TP, axis=0, tiled=True)
    stream, outgoing, slots = call(
        project,
        (sds((TOK, COLS), f32), sds((NSP, SEND, COLS), bf), sds((8, TOK), jnp.int32)),
        (at_cols, attended, w_cols, resid, norm_gain.reshape(1, D), routes.T),
        smem=1,
    )
    arrived = exchange(outgoing, SP)
    rows = 2 * ROWS + META
    every, lower, higher = call(
        squeeze,
        (sds((rows, COLS), bf), sds((ROWS + META, COLS), bf), sds((ROWS, COLS), bf)),
        (arrived,),
        scratch=(pltpu.VMEM((rows, COLS), f32),),
    )
    swap = [(0, 1), (1, 0)]
    owns = [every]
    for v, by in ((every, 1), (every, -1), (lower, 2), (higher, -2)):
        owns.append(shift(v, by))
    others = []
    for v in (every, jnp.concatenate(owns[1:3], axis=0), jnp.concatenate(owns[3:5], axis=0)):
        others.append(lax.ppermute(v, "c", swap))
    far_out, near_out = sds((2 * ROWS, COLS), bf), sds((6 * ROWS, COLS), bf)
    far_mine, near_mine, far_theirs, near_theirs = call(
        experts,
        (far_out, near_out, far_out, near_out),
        (jnp.stack([y, c]).astype(jnp.int32), *owns, *others, gate_weight[0], up_weight[0], down_weight[0]),
        smem=1,
        scratch=(pltpu.VMEM((ROWS, FFL), f32), pltpu.VMEM((ROWS, FFL), f32), pltpu.VMEM((ROWS, FFL), bf)),
        limit=24,
    )
    far_theirs = lax.ppermute(far_theirs, "c", swap)
    near_theirs = lax.ppermute(near_theirs, "c", swap)

    def pair(a, b, first, count):
        part = slice(first * ROWS, (first + count) * ROWS)
        return (a[part].astype(f32) + b[part].astype(f32)).astype(bf)

    got = []
    for a, b, first, count, by in (
        (far_mine, far_theirs, 0, 1, 2),
        (far_mine, far_theirs, 1, 1, -2),
        (near_mine, near_theirs, 0, 2, 1),
        (near_mine, near_theirs, 2, 2, -1),
    ):
        got.append(shift(pair(a, b, first, count), by))
    back = call(
        gather_sum,
        sds((2 * NSP, SLOT, COLS), bf),
        (near_mine, near_theirs, got[2], got[3], got[0], got[1]),
        scratch=(pltpu.VMEM((ROWS, COLS), f32),),
    )
    returned = exchange(back, ("z", "x", "yh")).reshape(2 * PADROWS, COLS)
    return call(finish, sds((TOK, COLS), bf), (returned, slots, route_weight.T, stream))


def solution(mesh):
    grid = Mesh(mesh.devices.reshape(NZ, NX, 2, HALF, NC), ("z", "x", "yh", "yl", "c"))
    return jax.shard_map(
        layer,
        mesh=grid,
        in_specs=(
            P(SP, TP),
            P(SP, TP),
            P(SP, TP),
            P(TP, None),
            P(TP, None),
            P(SP, None),
            P(),
            P(SP, None),
            P(SP, None),
            P(SP, None, TP),
            P(SP, None, TP),
            P(SP, TP, None),
        ),
        out_specs=P(SP, TP),
        check_vma=False,
    )
```

```python
import jax
import jax.numpy as jnp
from jax import lax
from jax.experimental import pallas as pl
from jax.experimental.pallas import tpu as pltpu
from jax.sharding import Mesh, PartitionSpec as P


NZ, NX, NY, NC = 8, 4, 8, 2
NSP, NTP = NZ * NX, NY * NC
Y = ("yh", "yl")
SP, TP = ("z", "x"), ("yh", "yl", "c")
HALF = NY // 2
HD = 64
TOK = 256
D = 2048
COLS = D // NTP
ROW = NX * TOK
CAP = 20
SLOT = 24
SEND = 48
ROWS = NSP * CAP
PADROWS = NSP * SLOT
META = 16
FFL = 256
EPS = 1e-06
LOW = -1e30
bf = jnp.bfloat16
f32 = jnp.float32

INTERPRET = False


def call(body, out_shape, inputs, smem=0, scratch=(), limit=12):
    specs = [pl.BlockSpec(memory_space=pltpu.SMEM)] * smem
    specs += [pl.BlockSpec(memory_space=pltpu.VMEM)] * (len(inputs) - smem)
    many = isinstance(out_shape, (tuple, list))
    vm = pl.BlockSpec(memory_space=pltpu.VMEM)
    return pl.pallas_call(
        body,
        out_shape=out_shape,
        in_specs=specs,
        out_specs=tuple([vm] * len(out_shape)) if many else vm,
        scratch_shapes=list(scratch),
        interpret=INTERPRET,
        compiler_params=pltpu.CompilerParams(vmem_limit_bytes=limit * 1024 * 1024),
    )(*inputs)


def three(v):
    hi = v.astype(bf).astype(f32)
    rest = v - hi
    mid = rest.astype(bf).astype(f32)
    return hi, mid, rest - mid


def attend(at_ref, q_ref, kv_ref, gate_ref, out0_ref, out1_ref, out2_ref, out3_ref, qs_ref, s_ref, m_ref, acc_ref, o_ref):
    z, x = at_ref[0], at_ref[1]
    first = gate_ref[:, pl.ds(pl.multiple_of(z * ROW, ROW), TOK)][:, 0:1]
    row64 = lax.broadcasted_iota(jnp.int32, (HD, TOK), 0)
    ones = jnp.where(row64 < 3, 1.0, 0.0).astype(bf)
    for j in range(NX):
        qs_ref[0:HD, j * TOK : (j + 1) * TOK] = q_ref[j] * bf(HD**-0.5)
        qs_ref[HD : 2 * HD, j * TOK : (j + 1) * TOK] = ones

    def scores(zk):
        place = pl.multiple_of(zk * ROW + x * TOK, TOK)
        hi, mid, lo = three(first - gate_ref[:, pl.ds(place, TOK)])
        extra = jnp.where(row64 == 0, hi, jnp.where(row64 == 1, mid, jnp.where(row64 == 2, lo, 0.0)))
        both = jnp.concatenate([kv_ref[zk, 0:HD, :], extra.astype(bf)], axis=0)
        return jnp.dot(both.T, qs_ref[...], preferred_element_type=f32)

    s = scores(z)
    ki = lax.broadcasted_iota(jnp.int32, (TOK, ROW), 0) + x * TOK
    qi = lax.broadcasted_iota(jnp.int32, (TOK, ROW), 1)
    s = jnp.where(ki <= qi, s, LOW)
    s_ref[z] = s
    m_ref[...] = jnp.broadcast_to(jnp.max(s, axis=0, keepdims=True), (8, ROW))

    def look(zk, carry):
        s = scores(zk)
        s_ref[zk] = s
        m_ref[...] = jnp.maximum(m_ref[...], jnp.max(s, axis=0, keepdims=True))
        return carry

    lax.fori_loop(0, z, look, 0)
    m = m_ref[0:1, :]
    acc_ref[...] = jnp.zeros((HD + 16, ROW), f32)

    def weigh(zk, carry):
        p = jnp.exp(s_ref[zk] - m).astype(bf)
        v = jnp.concatenate([kv_ref[zk, HD : 2 * HD, :], jnp.ones((16, TOK), bf)], axis=0)
        acc_ref[...] += jnp.dot(v, p, preferred_element_type=f32)
        return carry

    lax.fori_loop(0, z + 1, weigh, 0)
    row16 = lax.broadcasted_iota(jnp.int32, (16, ROW), 0)
    total = acc_ref[HD : HD + 1, :]
    hi, mid, lo = three(m + jnp.log(total))
    stats = jnp.where(row16 == 0, hi, jnp.where(row16 == 1, mid, jnp.where(row16 == 2, lo, 0.0))).astype(bf)
    o_ref[0:HD, :] = (acc_ref[0:HD, :] / total).astype(bf)
    o_ref[HD : HD + 16, :] = stats
    for j, out_ref in enumerate((out0_ref, out1_ref, out2_ref, out3_ref)):
        out_ref[...] = o_ref[:, pl.ds(pl.multiple_of(lax.rem(x + j, NX) * TOK, TOK), TOK)]


def merge(*refs):
    parts, out_ref = refs[0:NX], refs[NX]
    ls = []
    for i in range(NX):
        st = parts[i][HD : HD + 16, :].astype(f32)
        ls.append(st[0:1] + st[1:2] + st[2:3])
    m = ls[0]
    for v in ls[1:]:
        m = jnp.maximum(m, v)
    acc = jnp.zeros((HD, TOK), f32)
    total = jnp.zeros((1, TOK), f32)
    for i in range(NX):
        w = jnp.exp(ls[i] - m)
        total = total + w
        acc = acc + w * parts[i][0:HD, :].astype(f32)
    out_ref[...] = (acc / total).astype(bf)


def prepare(k_ref, v_ref, w_ref, kv_ref, out_ref):
    for z in range(NZ):
        kv_ref[z, 0:HD, :] = k_ref[...]
        kv_ref[z, HD : 2 * HD, :] = v_ref[...]
    for y in range(NY):
        for c in range(NC):
            for q in range(2):
                block = (y % (NY // 2) + q * (NY // 2)) * NC + c
                out_ref[y * NC + c, q * HD : (q + 1) * HD, :] = w_ref[:, block * COLS : (block + 1) * COLS]


def route(routes_ref, pick_ref, slots_ref):
    e0, e1 = routes_ref[0:1, :], routes_ref[1:2, :]
    io = lax.broadcasted_iota(jnp.int32, (NSP, TOK), 0)
    h0, h1 = io == e0, io == e1
    hit = jnp.where(h0, 1.0, jnp.where(h1, 1.0, 0.0)).astype(bf)
    ia = lax.broadcasted_iota(jnp.int32, (TOK, TOK), 0)
    ib = lax.broadcasted_iota(jnp.int32, (TOK, TOK), 1)
    upper = jnp.where(ia < ib, 1.0, 0.0).astype(bf)
    before = jnp.dot(hit, upper, preferred_element_type=f32)
    r0 = jnp.sum(jnp.where(h0, before, 0.0), axis=0, keepdims=True).astype(jnp.int32)
    r1 = jnp.sum(jnp.where(h1, before, 0.0), axis=0, keepdims=True).astype(jnp.int32)
    slots_ref[...] = jnp.concatenate([2 * SLOT * e0 + r0, 2 * SLOT * e1 + r1, jnp.zeros((6, TOK), jnp.int32)], axis=0)
    s0 = e0 * SEND + r0
    s1 = e1 * SEND + r1
    ir = lax.broadcasted_iota(jnp.int32, (NSP * SEND, TOK), 0)
    hits = (ir == s0) | (ir == s1) | (ir == s0 + CAP) | (ir == s1 + CAP)
    pick_ref[...] = jnp.where(hits, 1.0, 0.0).astype(bf)


def project(at_ref, att_ref, w_ref, resid_ref, gain_ref, pick_ref, stream_ref, out_ref):
    c0 = pl.multiple_of(at_ref[0], COLS)
    c1 = pl.multiple_of(at_ref[1], COLS)
    weights = [jnp.concatenate([w_ref[t, q * HD : (q + 1) * HD, :] for t in range(NTP)], axis=0) for q in range(2)]
    w = jnp.concatenate(weights, axis=1)
    mixed = lax.dot_general(att_ref[...], w, (((0,), (0,)), ((), ())), preferred_element_type=f32)
    resid = jnp.concatenate([resid_ref[:, pl.ds(c0, COLS)], resid_ref[:, pl.ds(c1, COLS)]], axis=1)
    gain = jnp.concatenate([gain_ref[:, pl.ds(c0, COLS)], gain_ref[:, pl.ds(c1, COLS)]], axis=1)
    stream = resid.astype(f32) + mixed
    stream_ref[...] = jnp.where(at_ref[2] == 0, stream[:, 0:COLS], stream[:, COLS:])
    square = jnp.sum(stream * stream, axis=1, keepdims=True)
    hi = square.astype(bf)
    lo = (square - hi.astype(f32)).astype(bf)
    scaled = (stream * gain).astype(bf)
    wide = (TOK, COLS)
    rows = jnp.concatenate([scaled, jnp.broadcast_to(hi, wide), jnp.broadcast_to(lo, wide)], axis=1)
    sent = jnp.dot(pick_ref[...], rows, preferred_element_type=f32).reshape(NSP, SEND, 4 * COLS)
    shape = (NSP, SEND, COLS)
    rank = lax.broadcasted_iota(jnp.int32, shape, 1)
    lane = lax.broadcasted_iota(jnp.int32, shape, 2)
    data = jnp.where(rank < CAP, sent[:, :, 0:COLS], sent[:, :, COLS : 2 * COLS])
    same = (lane == rank) & (rank < CAP)
    mh = jnp.sum(jnp.where(same, sent[:, :, 2 * COLS : 3 * COLS], 0.0), axis=1, keepdims=True)
    ml = jnp.sum(jnp.where(same, sent[:, :, 3 * COLS :], 0.0), axis=1, keepdims=True)
    data = jnp.where(rank == 2 * CAP, mh, jnp.where(rank == 2 * CAP + 1, ml, data))
    out_ref[...] = data.astype(bf)


def squeeze(in_ref, all_ref, low_ref, high_ref, rows_ref):
    rank = lax.broadcasted_iota(jnp.int32, (NSP, SEND, COLS), 1)
    x = in_ref[...].astype(f32)
    part = jnp.sum(jnp.where((rank == 2 * CAP) | (rank == 2 * CAP + 1), x, 0.0), axis=1)
    lane = lax.broadcasted_iota(jnp.int32, (NSP, COLS), 1)
    part = jnp.where(lane < CAP, part, 0.0)
    packed = part[0:8]
    for g in range(1, 4):
        packed = packed + pltpu.roll(part[8 * g : 8 * g + 8], 32 * g, 1)
    hi = packed.astype(bf).astype(f32)
    for i in range(NSP):
        x = in_ref[i].astype(f32)
        rows_ref[ROWS + CAP * i : ROWS + CAP * i + CAP, :] = x[0:CAP, :]
        rows_ref[CAP * i : CAP * i + CAP, :] = x[CAP : 2 * CAP, :]
    rows_ref[2 * ROWS : 2 * ROWS + 8, :] = hi
    rows_ref[2 * ROWS + 8 : 2 * ROWS + META, :] = packed - hi
    all_ref[...] = rows_ref[...].astype(bf)
    high_ref[...] = rows_ref[0:ROWS, :].astype(bf)
    low_ref[...] = rows_ref[ROWS : 2 * ROWS + META, :].astype(bf)


PIECES = (
    (0, 0, 0, ROWS),
    (0, 1, 0, 0),
    (3, 0, 1, ROWS),
    (3, 1, 1, 0),
    (1, 0, 2, ROWS),
    (1, 1, 2, 0),
    (2, 0, 3, 0),
    (2, 1, 4, 0),
)
METAS = ((0, 2 * ROWS), (1, 2 * ROWS), (2, 2 * ROWS), (3, ROWS))


SENDS = (
    (0, 0, 2, 0),
    (0, ROWS, 2, 1),
    (1, 0, 1, 0),
    (1, ROWS, 1, 1),
    (1, 2 * ROWS, 3, 0),
    (1, 3 * ROWS, 3, 1),
    (1, 4 * ROWS, 0, 0),
    (1, 5 * ROWS, 0, 1),
)


def experts(at_ref, *refs):
    every, near, far = refs[5:8]
    rows = 2 * ROWS + META
    owns = refs[0:5]
    others = (every, near.at[0:rows], near.at[rows:], far.at[0 : ROWS + META], far.at[ROWS + META :])
    wg_ref, wu_ref, wd_ref = refs[8:11]
    outs = refs[11:15]
    g_ref, u_ref, h_ref = refs[15:]
    y, c = at_ref[0], at_ref[1]
    total = jnp.zeros((8, COLS), f32)
    for pieces in (owns, others):
        for n, at in METAS:
            meta = pieces[n][at : at + META, :].astype(f32)
            total = total + meta[0:8] + meta[8:16]
    scale8 = lax.rsqrt(total / D + EPS)
    shape = (ROWS, COLS)
    row = lax.broadcasted_iota(jnp.int32, shape, 0).astype(f32)
    lane = lax.broadcasted_iota(jnp.int32, shape, 1).astype(f32)
    src = jnp.floor((row + 0.5) * (1.0 / CAP))
    group = jnp.floor((src + 0.5) * 0.125)
    sub = src - 8.0 * group
    target = 32.0 * group + (row - CAP * src)
    spread = jnp.zeros(shape, f32)
    for a in range(8):
        spread = jnp.where(sub == a, scale8[a : a + 1, :], spread)
    scale = jnp.sum(jnp.where(lane == target, spread, 0.0), axis=1, keepdims=True)
    for step, (off, upper, n, at) in enumerate(PIECES):
        xx = jnp.concatenate([owns[n][at : at + ROWS, :], others[n][at : at + ROWS, :]], axis=1)
        block = lax.rem(y + off, NY // 2) + upper * (NY // 2)
        first = pl.multiple_of((2 * block + c) * COLS, COLS)
        second = pl.multiple_of((2 * block + 1 - c) * COLS, COLS)
        for w_ref, acc_ref in ((wg_ref, g_ref), (wu_ref, u_ref)):
            w = jnp.concatenate([w_ref[pl.ds(first, COLS), :], w_ref[pl.ds(second, COLS), :]], axis=0)
            part = jnp.dot(xx, w, preferred_element_type=f32)
            if step == 0:
                acc_ref[...] = part
            else:
                acc_ref[...] += part
    gate = g_ref[...] * scale
    up = u_ref[...] * scale
    h_ref[...] = (gate / (1.0 + jnp.exp(-gate)) * up).astype(bf)
    even = c == 0
    for ref, at, off, upper in SENDS:
        block = lax.rem(y + off, HALF) + upper * HALF
        place = pl.multiple_of(2 * block * COLS, 2 * COLS)
        res = jnp.dot(h_ref[...], wd_ref[:, pl.ds(place, 2 * COLS)], preferred_element_type=f32)
        low, high = res[:, 0:COLS], res[:, COLS:]
        outs[ref][at : at + ROWS, :] = jnp.where(even, low, high).astype(bf)
        outs[ref + 2][at : at + ROWS, :] = jnp.where(even, high, low).astype(bf)


def gather_sum(mine_ref, theirs_ref, n0_ref, n1_ref, f0_ref, f1_ref, out_ref, rows_ref):
    base = 4 * ROWS
    pad = jnp.zeros((SLOT - CAP, COLS), f32)
    for q, far_ref in enumerate((f0_ref, f1_ref)):
        at = slice(q * ROWS, (q + 1) * ROWS)
        kept = slice(base + q * ROWS, base + (q + 1) * ROWS)
        acc = mine_ref[kept, :].astype(f32) + theirs_ref[kept, :].astype(f32)
        acc = acc + n0_ref[at, :].astype(f32) + n1_ref[at, :].astype(f32)
        rows_ref[...] = acc + far_ref[...].astype(f32)
        for i in range(NSP):
            out_ref[2 * i + q] = jnp.concatenate([rows_ref[CAP * i : CAP * i + CAP, :], pad], axis=0).astype(bf)


def finish(ret_ref, slots_ref, rw_ref, stream_ref, out_ref):
    slots = slots_ref[...].astype(f32).T
    weight = jnp.concatenate([rw_ref[...], jnp.zeros((6, TOK), f32)], axis=0).T
    lane = lax.broadcasted_iota(jnp.int32, (TOK, 2 * PADROWS), 1).astype(f32)
    out = stream_ref[...]
    for k in range(2):
        slot = slots[:, k : k + 1]
        pick = jnp.where((lane == slot) | (lane == slot + SLOT), 1.0, 0.0).astype(bf)
        got = jnp.dot(pick, ret_ref[...], preferred_element_type=f32)
        out = out + weight[:, k : k + 1] * got
    out_ref[...] = out.astype(bf)


def shift(v, by):
    return lax.ppermute(v, Y, [(i, (i + by) % NY) for i in range(NY)])


def exchange(v, axis):
    return lax.all_to_all(v, axis, 0, 0, tiled=True)


def layer(
    queries,
    keys,
    values,
    cum_gate,
    out_weight,
    resid,
    norm_gain,
    routes,
    route_weight,
    gate_weight,
    up_weight,
    down_weight,
):
    z, x, y, c = (lax.axis_index(a) for a in ("z", "x", Y, "c"))
    sds = jax.ShapeDtypeStruct
    half = NY // 2
    low = (lax.rem(y, half) * NC + c) * COLS
    at_cols = jnp.stack([low, low + half * NC * COLS, y // half]).astype(jnp.int32)
    at = jnp.stack([z, x]).astype(jnp.int32)
    kv_send, w_send = call(
        prepare,
        (sds((NZ, 2 * HD, TOK), bf), sds((NTP, 2 * HD, COLS), bf)),
        (keys.T, values.T, out_weight),
    )
    kv_send, w_send, at, at_cols = lax.optimization_barrier((kv_send, w_send, at, at_cols))
    kv = exchange(kv_send, "z")
    q_send, kv = lax.optimization_barrier((jnp.broadcast_to(queries.T[None], (NX, HD, TOK)), kv))
    q = exchange(q_send, "x")
    w_cols = exchange(w_send, TP)
    sent = call(
        attend,
        (sds((HD + 16, TOK), bf),) * NX,
        (at, q, kv, cum_gate),
        smem=1,
        scratch=(
            pltpu.VMEM((2 * HD, ROW), bf),
            pltpu.VMEM((NZ, TOK, ROW), f32),
            pltpu.VMEM((8, ROW), f32),
            pltpu.VMEM((HD + 16, ROW), f32),
            pltpu.VMEM((HD + 16, ROW), bf),
        ),
        limit=24,
    )
    parts = [sent[0]]
    for n in range(1, NX):
        parts.append(lax.ppermute(sent[n], "x", [(i, (i + n) % NX) for i in range(NX)]))
    pick, slots = call(
        route, (sds((NSP * SEND, TOK), bf), sds((8, TOK), jnp.int32)), (routes.T,)
    )
    attended = call(merge, sds((HD, TOK), bf), tuple(parts))
    attended = lax.all_gather(attended, TP, axis=0, tiled=True)
    stream, outgoing = call(
        project,
        (sds((TOK, COLS), f32), sds((NSP, SEND, COLS), bf)),
        (at_cols, attended, w_cols, resid, norm_gain.reshape(1, D), pick),
        smem=1,
    )
    arrived = exchange(outgoing, SP)
    rows = 2 * ROWS + META
    every, lower, higher = call(
        squeeze,
        (sds((rows, COLS), bf), sds((ROWS + META, COLS), bf), sds((ROWS, COLS), bf)),
        (arrived,),
        scratch=(pltpu.VMEM((rows, COLS), f32),),
    )
    swap = [(0, 1), (1, 0)]
    owns = [every]
    for v, by in ((every, 1), (every, -1), (lower, 2), (higher, -2)):
        owns.append(shift(v, by))
    others = []
    for v in (every, jnp.concatenate(owns[1:3], axis=0), jnp.concatenate(owns[3:5], axis=0)):
        others.append(lax.ppermute(v, "c", swap))
    far_out, near_out = sds((2 * ROWS, COLS), bf), sds((6 * ROWS, COLS), bf)
    far_mine, near_mine, far_theirs, near_theirs = call(
        experts,
        (far_out, near_out, far_out, near_out),
        (jnp.stack([y, c]).astype(jnp.int32), *owns, *others, gate_weight[0], up_weight[0], down_weight[0]),
        smem=1,
        scratch=(pltpu.VMEM((ROWS, FFL), f32), pltpu.VMEM((ROWS, FFL), f32), pltpu.VMEM((ROWS, FFL), bf)),
        limit=24,
    )
    far_theirs = lax.ppermute(far_theirs, "c", swap)
    near_theirs = lax.ppermute(near_theirs, "c", swap)

    def pair(a, b, first, count):
        part = slice(first * ROWS, (first + count) * ROWS)
        return (a[part].astype(f32) + b[part].astype(f32)).astype(bf)

    got = []
    for a, b, first, count, by in (
        (far_mine, far_theirs, 0, 1, 2),
        (far_mine, far_theirs, 1, 1, -2),
        (near_mine, near_theirs, 0, 2, 1),
        (near_mine, near_theirs, 2, 2, -1),
    ):
        got.append(shift(pair(a, b, first, count), by))
    back = call(
        gather_sum,
        sds((2 * NSP, SLOT, COLS), bf),
        (near_mine, near_theirs, got[2], got[3], got[0], got[1]),
        scratch=(pltpu.VMEM((ROWS, COLS), f32),),
    )
    returned = exchange(back, ("z", "x", "yh")).reshape(2 * PADROWS, COLS)
    return call(finish, sds((TOK, COLS), bf), (returned, slots, route_weight.T, stream))


def solution(mesh):
    grid = Mesh(mesh.devices.reshape(NZ, NX, 2, HALF, NC), ("z", "x", "yh", "yl", "c"))
    return jax.shard_map(
        layer,
        mesh=grid,
        in_specs=(
            P(SP, TP),
            P(SP, TP),
            P(SP, TP),
            P(TP, None),
            P(TP, None),
            P(SP, None),
            P(),
            P(SP, None),
            P(SP, None),
            P(SP, None, TP),
            P(SP, None, TP),
            P(SP, TP, None),
        ),
        out_specs=P(SP, TP),
        check_vma=False,
    )
```

```python
import jax
import jax.numpy as jnp
from jax import lax
from jax.experimental import pallas as pl
from jax.experimental.pallas import tpu as pltpu
from jax.sharding import Mesh, PartitionSpec as P


NZ, NX, NY, NC = 8, 4, 8, 2
NSP, NTP = NZ * NX, NY * NC
Y = ("yh", "yl")
SP, TP = ("z", "x"), ("yh", "yl", "c")
HALF = NY // 2
HD = 64
TOK = 256
D = 2048
COLS = D // NTP
ROW = NX * TOK
CAP = 20
SLOT = 24
SEND = 2 * CAP
ROWS = NSP * CAP
PADROWS = NSP * SLOT
FFL = 256
EPS = 1e-06
LOW = -1e30
bf = jnp.bfloat16
f32 = jnp.float32

INTERPRET = False


def call(body, out_shape, inputs, smem=0, scratch=(), limit=12, space=pltpu.VMEM):
    specs = [pl.BlockSpec(memory_space=pltpu.SMEM)] * smem
    specs += [pl.BlockSpec(memory_space=space)] * (len(inputs) - smem)
    many = isinstance(out_shape, (tuple, list))
    vm = pl.BlockSpec(memory_space=pltpu.VMEM)
    return pl.pallas_call(
        body,
        out_shape=out_shape,
        in_specs=specs,
        out_specs=tuple([vm] * len(out_shape)) if many else vm,
        scratch_shapes=list(scratch),
        interpret=INTERPRET,
        compiler_params=pltpu.CompilerParams(vmem_limit_bytes=limit * 1024 * 1024),
    )(*inputs)


def three(v):
    hi = v.astype(bf).astype(f32)
    rest = v - hi
    mid = rest.astype(bf).astype(f32)
    return hi, mid, rest - mid


def attend(at_ref, q_ref, kv_ref, gate_ref, out0_ref, out1_ref, out2_ref, out3_ref, qs_ref, s_ref, m_ref, acc_ref, o_ref):
    z, x = at_ref[0], at_ref[1]
    first = gate_ref[:, pl.ds(pl.multiple_of(z * ROW, ROW), TOK)][:, 0:1]
    row64 = lax.broadcasted_iota(jnp.int32, (HD, TOK), 0)
    ones = jnp.where(row64 < 3, 1.0, 0.0).astype(bf)
    for j in range(NX):
        qs_ref[0:HD, j * TOK : (j + 1) * TOK] = q_ref[j] * bf(HD**-0.5)
        qs_ref[HD : 2 * HD, j * TOK : (j + 1) * TOK] = ones

    def scores(zk):
        place = pl.multiple_of(zk * ROW + x * TOK, TOK)
        hi, mid, lo = three(first - gate_ref[:, pl.ds(place, TOK)])
        extra = jnp.where(row64 == 0, hi, jnp.where(row64 == 1, mid, jnp.where(row64 == 2, lo, 0.0)))
        both = jnp.concatenate([kv_ref[zk, 0:HD, :], extra.astype(bf)], axis=0)
        return jnp.dot(both.T, qs_ref[...], preferred_element_type=f32)

    s = scores(z)
    ki = lax.broadcasted_iota(jnp.int32, (TOK, ROW), 0) + x * TOK
    qi = lax.broadcasted_iota(jnp.int32, (TOK, ROW), 1)
    s = jnp.where(ki <= qi, s, LOW)
    s_ref[z] = s
    m_ref[...] = jnp.broadcast_to(jnp.max(s, axis=0, keepdims=True), (8, ROW))

    def look(zk, carry):
        s = scores(zk)
        s_ref[zk] = s
        m_ref[...] = jnp.maximum(m_ref[...], jnp.max(s, axis=0, keepdims=True))
        return carry

    def look_two(i, carry):
        one, two = scores(2 * i), scores(2 * i + 1)
        s_ref[2 * i] = one
        s_ref[2 * i + 1] = two
        top = jnp.max(jnp.maximum(one, two), axis=0, keepdims=True)
        m_ref[...] = jnp.maximum(m_ref[...], top)
        return carry

    lax.fori_loop(0, z // 2, look_two, 0)
    lax.fori_loop(z // 2 * 2, z, look, 0)
    m = m_ref[0:1, :]
    acc_ref[...] = jnp.zeros((HD + 16, ROW), f32)

    def weigh(zk, carry):
        p = jnp.exp(s_ref[zk] - m).astype(bf)
        v = jnp.concatenate([kv_ref[zk, HD : 2 * HD, :], jnp.ones((16, TOK), bf)], axis=0)
        acc_ref[...] += jnp.dot(v, p, preferred_element_type=f32)
        return carry

    def weigh_two(i, carry):
        zk = 2 * i
        p = jnp.exp(s_ref[pl.ds(zk, 2)].reshape(2 * TOK, ROW) - m).astype(bf)
        v = jnp.concatenate([kv_ref[zk, HD : 2 * HD, :], kv_ref[zk + 1, HD : 2 * HD, :]], axis=1)
        v = jnp.concatenate([v, jnp.ones((16, 2 * TOK), bf)], axis=0)
        acc_ref[...] += jnp.dot(v, p, preferred_element_type=f32)
        return carry

    lax.fori_loop(0, (z + 1) // 2, weigh_two, 0)
    lax.fori_loop((z + 1) // 2 * 2, z + 1, weigh, 0)
    row16 = lax.broadcasted_iota(jnp.int32, (16, ROW), 0)
    total = acc_ref[HD : HD + 1, :]
    hi, mid, lo = three(m + jnp.log(total))
    stats = jnp.where(row16 == 0, hi, jnp.where(row16 == 1, mid, jnp.where(row16 == 2, lo, 0.0))).astype(bf)
    o_ref[0:HD, :] = (acc_ref[0:HD, :] / total).astype(bf)
    o_ref[HD : HD + 16, :] = stats
    for j, out_ref in enumerate((out0_ref, out1_ref, out2_ref, out3_ref)):
        out_ref[...] = o_ref[:, pl.ds(pl.multiple_of(lax.rem(x + j, NX) * TOK, TOK), TOK)]


def merge(*refs):
    parts, out_ref = refs[0:NX], refs[NX]
    ls = []
    for i in range(NX):
        st = parts[i][HD : HD + 16, :].astype(f32)
        ls.append(st[0:1] + st[1:2] + st[2:3])
    m = ls[0]
    for v in ls[1:]:
        m = jnp.maximum(m, v)
    acc = jnp.zeros((HD, TOK), f32)
    total = jnp.zeros((1, TOK), f32)
    for i in range(NX):
        w = jnp.exp(ls[i] - m)
        total = total + w
        acc = acc + w * parts[i][0:HD, :].astype(f32)
    out_ref[...] = (acc / total).astype(bf)


def prepare(k_ref, v_ref, q_ref, w_ref, kv_ref, qs_ref, out_ref, kb_ref, vb_ref, qb_ref, wb_ref, sems):
    pairs = ((k_ref, kb_ref), (v_ref, vb_ref), (q_ref, qb_ref), (w_ref, wb_ref))
    copies = [pltpu.make_async_copy(a, b, sems.at[i]) for i, (a, b) in enumerate(pairs)]
    for copy in copies:
        copy.start()
    for copy in copies[0:3]:
        copy.wait()
    for z in range(NZ):
        kv_ref[z, 0:HD, :] = kb_ref[...]
        kv_ref[z, HD : 2 * HD, :] = vb_ref[...]
    for x in range(NX):
        qs_ref[x] = qb_ref[...]
    copies[3].wait()
    for y in range(NY):
        for c in range(NC):
            for q in range(2):
                block = (y % HALF + q * HALF) * NC + c
                out_ref[y * NC + c, q * HD : (q + 1) * HD, :] = wb_ref[:, block * COLS : (block + 1) * COLS]


def route(routes_ref, pick_ref, slots_ref):
    e0, e1 = routes_ref[0:1, :], routes_ref[1:2, :]
    io = lax.broadcasted_iota(jnp.int32, (NSP, TOK), 0)
    h0, h1 = io == e0, io == e1
    hit = jnp.where(h0, 1.0, jnp.where(h1, 1.0, 0.0)).astype(bf)
    ia = lax.broadcasted_iota(jnp.int32, (TOK, TOK), 0)
    ib = lax.broadcasted_iota(jnp.int32, (TOK, TOK), 1)
    upper = jnp.where(ia < ib, 1.0, 0.0).astype(bf)
    before = jnp.dot(hit, upper, preferred_element_type=f32)
    r0 = jnp.sum(jnp.where(h0, before, 0.0), axis=0, keepdims=True).astype(jnp.int32)
    r1 = jnp.sum(jnp.where(h1, before, 0.0), axis=0, keepdims=True).astype(jnp.int32)
    slots_ref[...] = jnp.concatenate([2 * SLOT * e0 + r0, 2 * SLOT * e1 + r1, jnp.zeros((6, TOK), jnp.int32)], axis=0)
    s0 = e0 * SEND + r0
    s1 = e1 * SEND + r1
    ir = lax.broadcasted_iota(jnp.int32, (NSP * SEND, TOK), 0)
    hits = (ir == s0) | (ir == s1) | (ir == s0 + CAP) | (ir == s1 + CAP)
    pick_ref[...] = jnp.where(hits, 1.0, 0.0).astype(bf)


def project(at_ref, att_ref, w_ref, resid_ref, gain_ref, pick_ref, stream_ref, out_ref):
    c0 = pl.multiple_of(at_ref[0], COLS)
    c1 = pl.multiple_of(at_ref[1], COLS)
    weights = [jnp.concatenate([w_ref[t, q * HD : (q + 1) * HD, :] for t in range(NTP)], axis=0) for q in range(2)]
    w = jnp.concatenate(weights, axis=1)
    mixed = lax.dot_general(att_ref[...], w, (((0,), (0,)), ((), ())), preferred_element_type=f32)
    resid = jnp.concatenate([resid_ref[:, pl.ds(c0, COLS)], resid_ref[:, pl.ds(c1, COLS)]], axis=1)
    gain = jnp.concatenate([gain_ref[:, pl.ds(c0, COLS)], gain_ref[:, pl.ds(c1, COLS)]], axis=1)
    stream = resid.astype(f32) + mixed
    stream_ref[...] = jnp.where(at_ref[2] == 0, stream[:, 0:COLS], stream[:, COLS:])
    scaled = (stream * gain).astype(bf)
    sent = jnp.dot(pick_ref[...], scaled, preferred_element_type=f32).reshape(NSP, SEND, 2 * COLS)
    rank = lax.broadcasted_iota(jnp.int32, (NSP, SEND, COLS), 1)
    out_ref[...] = jnp.where(rank < CAP, sent[:, :, 0:COLS], sent[:, :, COLS:]).astype(bf)


def squeeze(in_ref, all_ref, low_ref, high_ref, rows_ref):
    for i in range(NSP):
        x = in_ref[i].astype(f32)
        rows_ref[ROWS + CAP * i : ROWS + CAP * i + CAP, :] = x[0:CAP, :]
        rows_ref[CAP * i : CAP * i + CAP, :] = x[CAP : 2 * CAP, :]
    all_ref[...] = rows_ref[...].astype(bf)
    high_ref[...] = rows_ref[0:ROWS, :].astype(bf)
    low_ref[...] = rows_ref[ROWS:, :].astype(bf)


NEAR = ((0, 0, 0, ROWS), (0, 1, 0, 0), (3, 0, 1, ROWS), (3, 1, 1, 0), (1, 0, 2, ROWS), (1, 1, 2, 0))
FAR = ((2, 0, 0, 0), (2, 1, 1, 0))
SENDS = (
    (0, 0, 2, 0),
    (0, ROWS, 2, 1),
    (1, 0, 1, 0),
    (1, ROWS, 1, 1),
    (1, 2 * ROWS, 3, 0),
    (1, 3 * ROWS, 3, 1),
    (1, 4 * ROWS, 0, 0),
    (1, 5 * ROWS, 0, 1),
)


def accumulate(y, c, pieces, owns, others, wg_ref, wu_ref, gain_ref, g_ref, u_ref, sq_ref, fresh):
    for off, upper, n, at in pieces:
        mine, theirs = owns[n][at : at + ROWS, :], others[n][at : at + ROWS, :]
        block = lax.rem(y + off, HALF) + upper * HALF
        first = pl.multiple_of((2 * block + c) * COLS, COLS)
        second = pl.multiple_of((2 * block + 1 - c) * COLS, COLS)
        xx = jnp.concatenate([mine, theirs], axis=1)
        for w_ref, acc_ref in ((wg_ref, g_ref), (wu_ref, u_ref)):
            w = jnp.concatenate([w_ref[pl.ds(first, COLS), :], w_ref[pl.ds(second, COLS), :]], axis=0)
            part = jnp.dot(xx, w, preferred_element_type=f32)
            acc_ref[...] = part if fresh else acc_ref[...] + part
        a = mine.astype(f32) * (1.0 / gain_ref[:, pl.ds(first, COLS)])
        b = theirs.astype(f32) * (1.0 / gain_ref[:, pl.ds(second, COLS)])
        part = a * a + b * b
        sq_ref[...] = part if fresh else sq_ref[...] + part
        fresh = False


def experts_near(at_ref, every_ref, n0_ref, n1_ref, swap_ref, near_ref, wg_ref, wu_ref, gain_ref, g_ref, u_ref, sq_ref):
    owns = (every_ref, n0_ref, n1_ref)
    others = (swap_ref, near_ref.at[0 : 2 * ROWS], near_ref.at[2 * ROWS :])
    accumulate(at_ref[0], at_ref[1], NEAR, owns, others, wg_ref, wu_ref, gain_ref, g_ref, u_ref, sq_ref, True)


def experts(at_ref, f0_ref, f1_ref, far_ref, g_in, u_in, sq_in, wg_ref, wu_ref, wd_ref, gain_ref, *refs):
    outs = refs[0:4]
    g_ref, u_ref, sq_ref, h_ref = refs[4:]
    y, c = at_ref[0], at_ref[1]
    others = (far_ref.at[0:ROWS], far_ref.at[ROWS:])
    g_ref[...] = g_in[...]
    u_ref[...] = u_in[...]
    sq_ref[...] = sq_in[...]
    accumulate(y, c, FAR, (f0_ref, f1_ref), others, wg_ref, wu_ref, gain_ref, g_ref, u_ref, sq_ref, False)
    scale = lax.rsqrt(jnp.sum(sq_ref[...], axis=1, keepdims=True) / D + EPS)
    gate = g_ref[...] * scale
    up = u_ref[...] * scale
    h_ref[...] = (gate / (1.0 + jnp.exp(-gate)) * up).astype(bf)
    even = c == 0
    for ref, at, off, upper in SENDS:
        block = lax.rem(y + off, HALF) + upper * HALF
        place = pl.multiple_of(2 * block * COLS, 2 * COLS)
        res = jnp.dot(h_ref[...], wd_ref[:, pl.ds(place, 2 * COLS)], preferred_element_type=f32)
        low, high = res[:, 0:COLS], res[:, COLS:]
        outs[ref][at : at + ROWS, :] = jnp.where(even, low, high).astype(bf)
        outs[ref + 2][at : at + ROWS, :] = jnp.where(even, high, low).astype(bf)


def gather_sum(mine_ref, theirs_ref, n0_ref, n1_ref, f0_ref, f1_ref, out_ref, rows_ref):
    base = 4 * ROWS
    pad = jnp.zeros((SLOT - CAP, COLS), f32)
    for q, far_ref in enumerate((f0_ref, f1_ref)):
        at = slice(q * ROWS, (q + 1) * ROWS)
        kept = slice(base + q * ROWS, base + (q + 1) * ROWS)
        acc = mine_ref[kept, :].astype(f32) + theirs_ref[kept, :].astype(f32)
        acc = acc + n0_ref[at, :].astype(f32) + n1_ref[at, :].astype(f32)
        rows_ref[...] = acc + far_ref[...].astype(f32)
        for i in range(NSP):
            out_ref[2 * i + q] = jnp.concatenate([rows_ref[CAP * i : CAP * i + CAP, :], pad], axis=0).astype(bf)


def finish(ret_ref, slots_ref, rw_ref, stream_ref, out_ref):
    slots = slots_ref[...].astype(f32).T
    weight = jnp.concatenate([rw_ref[...], jnp.zeros((6, TOK), f32)], axis=0).T
    lane = lax.broadcasted_iota(jnp.int32, (TOK, 2 * PADROWS), 1).astype(f32)
    out = stream_ref[...]
    for k in range(2):
        slot = slots[:, k : k + 1]
        pick = jnp.where((lane == slot) | (lane == slot + SLOT), 1.0, 0.0).astype(bf)
        got = jnp.dot(pick, ret_ref[...], preferred_element_type=f32)
        out = out + weight[:, k : k + 1] * got
    out_ref[...] = out.astype(bf)


def shift(v, by):
    return lax.ppermute(v, Y, [(i, (i + by) % NY) for i in range(NY)])


def exchange(v, axis):
    return lax.all_to_all(v, axis, 0, 0, tiled=True)


def layer(
    queries,
    keys,
    values,
    cum_gate,
    out_weight,
    resid,
    norm_gain,
    routes,
    route_weight,
    gate_weight,
    up_weight,
    down_weight,
):
    z, x, y, c = (lax.axis_index(a) for a in ("z", "x", Y, "c"))
    sds = jax.ShapeDtypeStruct
    half = NY // 2
    low = (lax.rem(y, half) * NC + c) * COLS
    at_cols = jnp.stack([low, low + half * NC * COLS, y // half]).astype(jnp.int32)
    at = jnp.stack([z, x]).astype(jnp.int32)
    small = pltpu.VMEM((HD, TOK), bf)
    kv_send, q_send, w_send = call(
        prepare,
        (sds((NZ, 2 * HD, TOK), bf), sds((NX, HD, TOK), bf), sds((NTP, 2 * HD, COLS), bf)),
        (keys.T, values.T, queries.T, out_weight),
        scratch=(small, small, small, pltpu.VMEM((HD, D), bf), pltpu.SemaphoreType.DMA((4,))),
        space=pl.ANY,
    )
    kv_send, w_send, at, at_cols = lax.optimization_barrier((kv_send, w_send, at, at_cols))
    kv = exchange(kv_send, "z")
    q_send, kv = lax.optimization_barrier((q_send, kv))
    q = exchange(q_send, "x")
    w_cols = exchange(w_send, TP)
    sent = call(
        attend,
        (sds((HD + 16, TOK), bf),) * NX,
        (at, q, kv, cum_gate),
        smem=1,
        scratch=(
            pltpu.VMEM((2 * HD, ROW), bf),
            pltpu.VMEM((NZ, TOK, ROW), f32),
            pltpu.VMEM((8, ROW), f32),
            pltpu.VMEM((HD + 16, ROW), f32),
            pltpu.VMEM((HD + 16, ROW), bf),
        ),
        limit=24,
    )
    parts = [sent[0]]
    for n in range(1, NX):
        parts.append(lax.ppermute(sent[n], "x", [(i, (i + n) % NX) for i in range(NX)]))
    pick, slots = call(
        route, (sds((NSP * SEND, TOK), bf), sds((8, TOK), jnp.int32)), (routes.T,)
    )
    attended = call(merge, sds((HD, TOK), bf), tuple(parts))
    attended = lax.all_gather(attended, TP, axis=0, tiled=True)
    stream, outgoing = call(
        project,
        (sds((TOK, COLS), f32), sds((NSP, SEND, COLS), bf)),
        (at_cols, attended, w_cols, resid, norm_gain.reshape(1, D), pick),
        smem=1,
    )
    arrived = exchange(outgoing, SP)
    every, lower, higher = call(
        squeeze,
        (sds((2 * ROWS, COLS), bf), sds((ROWS, COLS), bf), sds((ROWS, COLS), bf)),
        (arrived,),
        scratch=(pltpu.VMEM((2 * ROWS, COLS), f32),),
    )
    swap = [(0, 1), (1, 0)]
    owns = [every]
    for v, by in ((every, 1), (every, -1), (lower, 2), (higher, -2)):
        owns.append(shift(v, by))
    others = []
    for v in (every, jnp.concatenate(owns[1:3], axis=0), jnp.concatenate(owns[3:5], axis=0)):
        others.append(lax.ppermute(v, "c", swap))
    gain = norm_gain.reshape(1, D)
    at_yc = jnp.stack([y, c]).astype(jnp.int32)
    sums = (sds((ROWS, FFL), f32), sds((ROWS, FFL), f32), sds((ROWS, COLS), f32))
    partial = call(experts_near, sums, (at_yc, *owns[0:3], *others[0:2], gate_weight[0], up_weight[0], gain), smem=1)
    far_out, near_out = sds((2 * ROWS, COLS), bf), sds((6 * ROWS, COLS), bf)
    far_mine, near_mine, far_theirs, near_theirs = call(
        experts,
        (far_out, near_out, far_out, near_out),
        (at_yc, *owns[3:5], others[2], *partial, gate_weight[0], up_weight[0], down_weight[0], gain),
        smem=1,
        scratch=[pltpu.VMEM(v.shape, f32) for v in sums] + [pltpu.VMEM((ROWS, FFL), bf)],
    )
    far_theirs = lax.ppermute(far_theirs, "c", swap)
    near_theirs = lax.ppermute(near_theirs, "c", swap)

    def pair(a, b, first, count):
        part = slice(first * ROWS, (first + count) * ROWS)
        return (a[part].astype(f32) + b[part].astype(f32)).astype(bf)

    got = []
    for a, b, first, count, by in (
        (far_mine, far_theirs, 0, 1, 2),
        (far_mine, far_theirs, 1, 1, -2),
        (near_mine, near_theirs, 0, 2, 1),
        (near_mine, near_theirs, 2, 2, -1),
    ):
        got.append(shift(pair(a, b, first, count), by))
    back = call(
        gather_sum,
        sds((2 * NSP, SLOT, COLS), bf),
        (near_mine, near_theirs, got[2], got[3], got[0], got[1]),
        scratch=(pltpu.VMEM((ROWS, COLS), f32),),
    )
    returned = exchange(back, ("z", "x", "yh")).reshape(2 * PADROWS, COLS)
    return call(finish, sds((TOK, COLS), bf), (returned, slots, route_weight.T, stream))


def solution(mesh):
    grid = Mesh(mesh.devices.reshape(NZ, NX, 2, HALF, NC), ("z", "x", "yh", "yl", "c"))
    return jax.shard_map(
        layer,
        mesh=grid,
        in_specs=(
            P(SP, TP),
            P(SP, TP),
            P(SP, TP),
            P(TP, None),
            P(TP, None),
            P(SP, None),
            P(),
            P(SP, None),
            P(SP, None),
            P(SP, None, TP),
            P(SP, None, TP),
            P(SP, TP, None),
        ),
        out_specs=P(SP, TP),
        check_vma=False,
    )
```

```python
import jax
import jax.numpy as jnp
from jax import lax
from jax.experimental import pallas as pl
from jax.experimental.pallas import tpu as pltpu
from jax.sharding import Mesh, PartitionSpec as P


NZ, NX, NY, NC = 8, 4, 8, 2
NSP, NTP = NZ * NX, NY * NC
Y = ("yh", "yl")
SP, TP = ("z", "x"), ("yh", "yl", "c")
HALF = NY // 2
HD = 64
TOK = 256
D = 2048
COLS = D // NTP
ROW = NX * TOK
CAP = 20
SLOT = 24
SEND = 2 * CAP
ROWS = NSP * CAP
PADROWS = NSP * SLOT
FFL = 256
EPS = 1e-06
LOW = -1e30
bf = jnp.bfloat16
f32 = jnp.float32

INTERPRET = False


def call(body, out_shape, inputs, smem=0, scratch=(), limit=12, space=pltpu.VMEM):
    specs = [pl.BlockSpec(memory_space=pltpu.SMEM)] * smem
    specs += [pl.BlockSpec(memory_space=space)] * (len(inputs) - smem)
    many = isinstance(out_shape, (tuple, list))
    vm = pl.BlockSpec(memory_space=pltpu.VMEM)
    return pl.pallas_call(
        body,
        out_shape=out_shape,
        in_specs=specs,
        out_specs=tuple([vm] * len(out_shape)) if many else vm,
        scratch_shapes=list(scratch),
        interpret=INTERPRET,
        compiler_params=pltpu.CompilerParams(vmem_limit_bytes=limit * 1024 * 1024),
    )(*inputs)


def three(v):
    hi = v.astype(bf).astype(f32)
    rest = v - hi
    mid = rest.astype(bf).astype(f32)
    return hi, mid, rest - mid


def attend(at_ref, q_ref, kv_ref, gate_ref, out0_ref, out1_ref, out2_ref, out3_ref, qs_ref, s_ref, m_ref, acc_ref, o_ref):
    z, x = at_ref[0], at_ref[1]
    first = gate_ref[:, pl.ds(pl.multiple_of(z * ROW, ROW), TOK)][:, 0:1]
    row64 = lax.broadcasted_iota(jnp.int32, (HD, TOK), 0)
    ones = jnp.where(row64 < 3, 1.0, 0.0).astype(bf)
    for j in range(NX):
        qs_ref[0:HD, j * TOK : (j + 1) * TOK] = q_ref[j] * bf(HD**-0.5)
        qs_ref[HD : 2 * HD, j * TOK : (j + 1) * TOK] = ones

    def scores(zk):
        place = pl.multiple_of(zk * ROW + x * TOK, TOK)
        hi, mid, lo = three(first - gate_ref[:, pl.ds(place, TOK)])
        extra = jnp.where(row64 == 0, hi, jnp.where(row64 == 1, mid, jnp.where(row64 == 2, lo, 0.0)))
        both = jnp.concatenate([kv_ref[zk, 0:HD, :], extra.astype(bf)], axis=0)
        return jnp.dot(both.T, qs_ref[...], preferred_element_type=f32)

    s = scores(z)
    ki = lax.broadcasted_iota(jnp.int32, (TOK, ROW), 0) + x * TOK
    qi = lax.broadcasted_iota(jnp.int32, (TOK, ROW), 1)
    s = jnp.where(ki <= qi, s, LOW)
    s_ref[z] = s
    m_ref[...] = jnp.broadcast_to(jnp.max(s, axis=0, keepdims=True), (8, ROW))

    def look(zk, carry):
        s = scores(zk)
        s_ref[zk] = s
        m_ref[...] = jnp.maximum(m_ref[...], jnp.max(s, axis=0, keepdims=True))
        return carry

    def look_two(i, carry):
        one, two = scores(2 * i), scores(2 * i + 1)
        s_ref[2 * i] = one
        s_ref[2 * i + 1] = two
        top = jnp.max(jnp.maximum(one, two), axis=0, keepdims=True)
        m_ref[...] = jnp.maximum(m_ref[...], top)
        return carry

    lax.fori_loop(0, z // 2, look_two, 0)
    lax.fori_loop(z // 2 * 2, z, look, 0)
    m = m_ref[0:1, :]
    acc_ref[...] = jnp.zeros((HD + 16, ROW), f32)

    def weigh(zk, carry):
        p = jnp.exp(s_ref[zk] - m).astype(bf)
        v = jnp.concatenate([kv_ref[zk, HD : 2 * HD, :], jnp.ones((16, TOK), bf)], axis=0)
        acc_ref[...] += jnp.dot(v, p, preferred_element_type=f32)
        return carry

    def weigh_two(i, carry):
        zk = 2 * i
        p = jnp.exp(s_ref[pl.ds(zk, 2)].reshape(2 * TOK, ROW) - m).astype(bf)
        v = jnp.concatenate([kv_ref[zk, HD : 2 * HD, :], kv_ref[zk + 1, HD : 2 * HD, :]], axis=1)
        v = jnp.concatenate([v, jnp.ones((16, 2 * TOK), bf)], axis=0)
        acc_ref[...] += jnp.dot(v, p, preferred_element_type=f32)
        return carry

    lax.fori_loop(0, (z + 1) // 2, weigh_two, 0)
    lax.fori_loop((z + 1) // 2 * 2, z + 1, weigh, 0)
    row16 = lax.broadcasted_iota(jnp.int32, (16, ROW), 0)
    total = acc_ref[HD : HD + 1, :]
    hi, mid, lo = three(m + jnp.log(total))
    stats = jnp.where(row16 == 0, hi, jnp.where(row16 == 1, mid, jnp.where(row16 == 2, lo, 0.0))).astype(bf)
    o_ref[0:HD, :] = (acc_ref[0:HD, :] / total).astype(bf)
    o_ref[HD : HD + 16, :] = stats
    for j, out_ref in enumerate((out0_ref, out1_ref, out2_ref, out3_ref)):
        out_ref[...] = o_ref[:, pl.ds(pl.multiple_of(lax.rem(x + j, NX) * TOK, TOK), TOK)]


def merge(*refs):
    parts, out_ref = refs[0:NX], refs[NX]
    ls = []
    for i in range(NX):
        st = parts[i][HD : HD + 16, :].astype(f32)
        ls.append(st[0:1] + st[1:2] + st[2:3])
    m = ls[0]
    for v in ls[1:]:
        m = jnp.maximum(m, v)
    acc = jnp.zeros((HD, TOK), f32)
    total = jnp.zeros((1, TOK), f32)
    for i in range(NX):
        w = jnp.exp(ls[i] - m)
        total = total + w
        acc = acc + w * parts[i][0:HD, :].astype(f32)
    out = (acc / total).astype(bf)
    for y in range(NY):
        out_ref[y] = out


def prepare(k_ref, v_ref, q_ref, w_ref, kv_ref, qs_ref, out_ref, kb_ref, vb_ref, qb_ref, wb_ref, sems):
    pairs = ((k_ref, kb_ref), (v_ref, vb_ref), (q_ref, qb_ref), (w_ref, wb_ref))
    copies = [pltpu.make_async_copy(a, b, sems.at[i]) for i, (a, b) in enumerate(pairs)]
    for copy in copies:
        copy.start()
    for copy in copies[0:3]:
        copy.wait()
    for z in range(NZ):
        kv_ref[z, 0:HD, :] = kb_ref[...]
        kv_ref[z, HD : 2 * HD, :] = vb_ref[...]
    for x in range(NX):
        qs_ref[x] = qb_ref[...]
    copies[3].wait()
    for y in range(NY):
        for c in range(NC):
            for q in range(2):
                block = (y % HALF + q * HALF) * NC + c
                out_ref[y * NC + c, q * HD : (q + 1) * HD, :] = wb_ref[:, block * COLS : (block + 1) * COLS]


def route(routes_ref, pick_ref, slots_ref):
    e0, e1 = routes_ref[0:1, :], routes_ref[1:2, :]
    io = lax.broadcasted_iota(jnp.int32, (NSP, TOK), 0)
    h0, h1 = io == e0, io == e1
    hit = jnp.where(h0, 1.0, jnp.where(h1, 1.0, 0.0)).astype(bf)
    ia = lax.broadcasted_iota(jnp.int32, (TOK, TOK), 0)
    ib = lax.broadcasted_iota(jnp.int32, (TOK, TOK), 1)
    upper = jnp.where(ia < ib, 1.0, 0.0).astype(bf)
    before = jnp.dot(hit, upper, preferred_element_type=f32)
    r0 = jnp.sum(jnp.where(h0, before, 0.0), axis=0, keepdims=True).astype(jnp.int32)
    r1 = jnp.sum(jnp.where(h1, before, 0.0), axis=0, keepdims=True).astype(jnp.int32)
    slots_ref[...] = jnp.concatenate([2 * SLOT * e0 + r0, 2 * SLOT * e1 + r1, jnp.zeros((6, TOK), jnp.int32)], axis=0)
    s0 = e0 * SEND + r0
    s1 = e1 * SEND + r1
    ir = lax.broadcasted_iota(jnp.int32, (NSP * SEND, TOK), 0)
    hits = (ir == s0) | (ir == s1) | (ir == s0 + CAP) | (ir == s1 + CAP)
    pick_ref[...] = jnp.where(hits, 1.0, 0.0).astype(bf)


def project(at_ref, own_ref, partner_ref, w_ref, resid_ref, gain_ref, pick_ref, stream_ref, out_ref):
    c0 = pl.multiple_of(at_ref[0], COLS)
    c1 = pl.multiple_of(at_ref[1], COLS)
    c = at_ref[3]
    heads = [2 * y + c for y in range(NY)] + [2 * y + 1 - c for y in range(NY)]
    weights = [jnp.concatenate([w_ref[t, q * HD : (q + 1) * HD, :] for t in heads], axis=0) for q in range(2)]
    w = jnp.concatenate(weights, axis=1)
    att = jnp.concatenate([ref[...].reshape(NY * HD, TOK) for ref in (own_ref, partner_ref)], axis=0)
    mixed = lax.dot_general(att, w, (((0,), (0,)), ((), ())), preferred_element_type=f32)
    resid = jnp.concatenate([resid_ref[:, pl.ds(c0, COLS)], resid_ref[:, pl.ds(c1, COLS)]], axis=1)
    gain = jnp.concatenate([gain_ref[:, pl.ds(c0, COLS)], gain_ref[:, pl.ds(c1, COLS)]], axis=1)
    stream = resid.astype(f32) + mixed
    stream_ref[...] = jnp.where(at_ref[2] == 0, stream[:, 0:COLS], stream[:, COLS:])
    scaled = (stream * gain).astype(bf)
    sent = jnp.dot(pick_ref[...], scaled, preferred_element_type=f32).reshape(NSP, SEND, 2 * COLS)
    rank = lax.broadcasted_iota(jnp.int32, (NSP, SEND, COLS), 1)
    out_ref[...] = jnp.where(rank < CAP, sent[:, :, 0:COLS], sent[:, :, COLS:]).astype(bf)


def squeeze(in_ref, all_ref, low_ref, high_ref, rows_ref):
    for i in range(NSP):
        x = in_ref[i].astype(f32)
        rows_ref[ROWS + CAP * i : ROWS + CAP * i + CAP, :] = x[0:CAP, :]
        rows_ref[CAP * i : CAP * i + CAP, :] = x[CAP : 2 * CAP, :]
    all_ref[...] = rows_ref[...].astype(bf)
    high_ref[...] = rows_ref[0:ROWS, :].astype(bf)
    low_ref[...] = rows_ref[ROWS:, :].astype(bf)


NEAR = ((0, 0, 0, ROWS), (0, 1, 0, 0), (3, 0, 1, ROWS), (3, 1, 1, 0), (1, 0, 2, ROWS), (1, 1, 2, 0))
FAR = ((2, 0, 0, 0), (2, 1, 1, 0))
SENDS = (
    (0, 0, 2, 0),
    (0, ROWS, 2, 1),
    (1, 0, 1, 0),
    (1, ROWS, 1, 1),
    (1, 2 * ROWS, 3, 0),
    (1, 3 * ROWS, 3, 1),
    (1, 4 * ROWS, 0, 0),
    (1, 5 * ROWS, 0, 1),
)


def accumulate(y, c, pieces, owns, others, wg_ref, wu_ref, gain_ref, g_ref, u_ref, sq_ref, fresh):
    for off, upper, n, at in pieces:
        mine, theirs = owns[n][at : at + ROWS, :], others[n][at : at + ROWS, :]
        block = lax.rem(y + off, HALF) + upper * HALF
        first = pl.multiple_of((2 * block + c) * COLS, COLS)
        second = pl.multiple_of((2 * block + 1 - c) * COLS, COLS)
        xx = jnp.concatenate([mine, theirs], axis=1)
        for w_ref, acc_ref in ((wg_ref, g_ref), (wu_ref, u_ref)):
            w = jnp.concatenate([w_ref[pl.ds(first, COLS), :], w_ref[pl.ds(second, COLS), :]], axis=0)
            part = jnp.dot(xx, w, preferred_element_type=f32)
            acc_ref[...] = part if fresh else acc_ref[...] + part
        a = mine.astype(f32) * (1.0 / gain_ref[:, pl.ds(first, COLS)])
        b = theirs.astype(f32) * (1.0 / gain_ref[:, pl.ds(second, COLS)])
        part = a * a + b * b
        sq_ref[...] = part if fresh else sq_ref[...] + part
        fresh = False


def experts_near(at_ref, every_ref, n0_ref, n1_ref, swap_ref, near_ref, wg_ref, wu_ref, gain_ref, g_ref, u_ref, sq_ref):
    owns = (every_ref, n0_ref, n1_ref)
    others = (swap_ref, near_ref.at[0 : 2 * ROWS], near_ref.at[2 * ROWS :])
    accumulate(at_ref[0], at_ref[1], NEAR, owns, others, wg_ref, wu_ref, gain_ref, g_ref, u_ref, sq_ref, True)


def experts(at_ref, f0_ref, f1_ref, far_ref, g_in, u_in, sq_in, wg_ref, wu_ref, wd_ref, gain_ref, *refs):
    outs = refs[0:4]
    g_ref, u_ref, sq_ref, h_ref = refs[4:]
    y, c = at_ref[0], at_ref[1]
    others = (far_ref.at[0:ROWS], far_ref.at[ROWS:])
    g_ref[...] = g_in[...]
    u_ref[...] = u_in[...]
    sq_ref[...] = sq_in[...]
    accumulate(y, c, FAR, (f0_ref, f1_ref), others, wg_ref, wu_ref, gain_ref, g_ref, u_ref, sq_ref, False)
    scale = lax.rsqrt(jnp.sum(sq_ref[...], axis=1, keepdims=True) / D + EPS)
    gate = g_ref[...] * scale
    up = u_ref[...] * scale
    h_ref[...] = (gate / (1.0 + jnp.exp(-gate)) * up).astype(bf)
    even = c == 0
    for ref, at, off, upper in SENDS:
        block = lax.rem(y + off, HALF) + upper * HALF
        place = pl.multiple_of(2 * block * COLS, 2 * COLS)
        res = jnp.dot(h_ref[...], wd_ref[:, pl.ds(place, 2 * COLS)], preferred_element_type=f32)
        low, high = res[:, 0:COLS], res[:, COLS:]
        outs[ref][at : at + ROWS, :] = jnp.where(even, low, high).astype(bf)
        outs[ref + 2][at : at + ROWS, :] = jnp.where(even, high, low).astype(bf)


def gather_sum(mine_ref, theirs_ref, n0_ref, n1_ref, f0_ref, f1_ref, out_ref, rows_ref):
    base = 4 * ROWS
    pad = jnp.zeros((SLOT - CAP, COLS), f32)
    for q, far_ref in enumerate((f0_ref, f1_ref)):
        at = slice(q * ROWS, (q + 1) * ROWS)
        kept = slice(base + q * ROWS, base + (q + 1) * ROWS)
        acc = mine_ref[kept, :].astype(f32) + theirs_ref[kept, :].astype(f32)
        acc = acc + n0_ref[at, :].astype(f32) + n1_ref[at, :].astype(f32)
        rows_ref[...] = acc + far_ref[...].astype(f32)
        for i in range(NSP):
            out_ref[2 * i + q] = jnp.concatenate([rows_ref[CAP * i : CAP * i + CAP, :], pad], axis=0).astype(bf)


def finish(ret_ref, slots_ref, rw_ref, stream_ref, out_ref):
    slots = slots_ref[...].astype(f32).T
    weight = jnp.concatenate([rw_ref[...], jnp.zeros((6, TOK), f32)], axis=0).T
    lane = lax.broadcasted_iota(jnp.int32, (TOK, 2 * PADROWS), 1).astype(f32)
    out = stream_ref[...]
    for k in range(2):
        slot = slots[:, k : k + 1]
        pick = jnp.where((lane == slot) | (lane == slot + SLOT), 1.0, 0.0).astype(bf)
        got = jnp.dot(pick, ret_ref[...], preferred_element_type=f32)
        out = out + weight[:, k : k + 1] * got
    out_ref[...] = out.astype(bf)


def shift(v, by):
    return lax.ppermute(v, Y, [(i, (i + by) % NY) for i in range(NY)])


def exchange(v, axis):
    return lax.all_to_all(v, axis, 0, 0, tiled=True)


def layer(
    queries,
    keys,
    values,
    cum_gate,
    out_weight,
    resid,
    norm_gain,
    routes,
    route_weight,
    gate_weight,
    up_weight,
    down_weight,
):
    z, x, y, c = (lax.axis_index(a) for a in ("z", "x", Y, "c"))
    sds = jax.ShapeDtypeStruct
    half = NY // 2
    low = (lax.rem(y, half) * NC + c) * COLS
    at_cols = jnp.stack([low, low + half * NC * COLS, y // half, c]).astype(jnp.int32)
    at = jnp.stack([z, x]).astype(jnp.int32)
    small = pltpu.VMEM((HD, TOK), bf)
    kv_send, q_send, w_send = call(
        prepare,
        (sds((NZ, 2 * HD, TOK), bf), sds((NX, HD, TOK), bf), sds((NTP, 2 * HD, COLS), bf)),
        (keys.T, values.T, queries.T, out_weight),
        scratch=(small, small, small, pltpu.VMEM((HD, D), bf), pltpu.SemaphoreType.DMA((4,))),
        space=pltpu.HBM,
    )
    kv_send, w_send, at, at_cols = lax.optimization_barrier((kv_send, w_send, at, at_cols))
    kv = exchange(kv_send, "z")
    q_send, kv = lax.optimization_barrier((q_send, kv))
    q = exchange(q_send, "x")
    w_cols = exchange(w_send, TP)
    sent = call(
        attend,
        (sds((HD + 16, TOK), bf),) * NX,
        (at, q, kv, cum_gate),
        smem=1,
        scratch=(
            pltpu.VMEM((2 * HD, ROW), bf),
            pltpu.VMEM((NZ, TOK, ROW), f32),
            pltpu.VMEM((8, ROW), f32),
            pltpu.VMEM((HD + 16, ROW), f32),
            pltpu.VMEM((HD + 16, ROW), bf),
        ),
        limit=24,
    )
    parts = [sent[0]]
    for n in range(1, NX):
        parts.append(lax.ppermute(sent[n], "x", [(i, (i + n) % NX) for i in range(NX)]))
    pick, slots = call(
        route, (sds((NSP * SEND, TOK), bf), sds((8, TOK), jnp.int32)), (routes.T,)
    )
    swap = [(0, 1), (1, 0)]
    attended, w_cols = lax.optimization_barrier((call(merge, sds((NY, HD, TOK), bf), tuple(parts)), w_cols))
    attended = exchange(attended, Y)
    partner = lax.ppermute(attended, "c", swap)
    stream, outgoing = call(
        project,
        (sds((TOK, COLS), f32), sds((NSP, SEND, COLS), bf)),
        (at_cols, attended, partner, w_cols, resid, norm_gain.reshape(1, D), pick),
        smem=1,
    )
    arrived = exchange(outgoing, SP)
    every, lower, higher = call(
        squeeze,
        (sds((2 * ROWS, COLS), bf), sds((ROWS, COLS), bf), sds((ROWS, COLS), bf)),
        (arrived,),
        scratch=(pltpu.VMEM((2 * ROWS, COLS), f32),),
    )
    owns = [every]
    for v, by in ((every, 1), (every, -1), (lower, 2), (higher, -2)):
        owns.append(shift(v, by))
    others = []
    for v in (every, jnp.concatenate(owns[1:3], axis=0), jnp.concatenate(owns[3:5], axis=0)):
        others.append(lax.ppermute(v, "c", swap))
    gain = norm_gain.reshape(1, D)
    at_yc = jnp.stack([y, c]).astype(jnp.int32)
    sums = (sds((ROWS, FFL), f32), sds((ROWS, FFL), f32), sds((ROWS, COLS), f32))
    partial = call(experts_near, sums, (at_yc, *owns[0:3], *others[0:2], gate_weight[0], up_weight[0], gain), smem=1)
    far_out, near_out = sds((2 * ROWS, COLS), bf), sds((6 * ROWS, COLS), bf)
    far_mine, near_mine, far_theirs, near_theirs = call(
        experts,
        (far_out, near_out, far_out, near_out),
        (at_yc, *owns[3:5], others[2], *partial, gate_weight[0], up_weight[0], down_weight[0], gain),
        smem=1,
        scratch=[pltpu.VMEM(v.shape, f32) for v in sums] + [pltpu.VMEM((ROWS, FFL), bf)],
    )
    far_theirs = lax.ppermute(far_theirs, "c", swap)
    near_theirs = lax.ppermute(near_theirs, "c", swap)

    def pair(a, b, first, count):
        part = slice(first * ROWS, (first + count) * ROWS)
        return (a[part].astype(f32) + b[part].astype(f32)).astype(bf)

    got = []
    for a, b, first, count, by in (
        (far_mine, far_theirs, 0, 1, 2),
        (far_mine, far_theirs, 1, 1, -2),
        (near_mine, near_theirs, 0, 2, 1),
        (near_mine, near_theirs, 2, 2, -1),
    ):
        got.append(shift(pair(a, b, first, count), by))
    back = call(
        gather_sum,
        sds((2 * NSP, SLOT, COLS), bf),
        (near_mine, near_theirs, got[2], got[3], got[0], got[1]),
        scratch=(pltpu.VMEM((ROWS, COLS), f32),),
    )
    returned = exchange(back, ("z", "x", "yh")).reshape(2 * PADROWS, COLS)
    return call(finish, sds((TOK, COLS), bf), (returned, slots, route_weight.T, stream))


def solution(mesh):
    grid = Mesh(mesh.devices.reshape(NZ, NX, 2, HALF, NC), ("z", "x", "yh", "yl", "c"))
    return jax.shard_map(
        layer,
        mesh=grid,
        in_specs=(
            P(SP, TP),
            P(SP, TP),
            P(SP, TP),
            P(TP, None),
            P(TP, None),
            P(SP, None),
            P(),
            P(SP, None),
            P(SP, None),
            P(SP, None, TP),
            P(SP, None, TP),
            P(SP, TP, None),
        ),
        out_specs=P(SP, TP),
        check_vma=False,
    )
```

```python
import jax
import jax.numpy as jnp
from jax import lax
from jax.experimental import pallas as pl
from jax.experimental.pallas import tpu as pltpu
from jax.sharding import Mesh, PartitionSpec as P


NZ, NX, NY, NC = 8, 4, 8, 2
NSP, NTP = NZ * NX, NY * NC
Y = ("yh", "yl")
SP, TP = ("z", "x"), ("yh", "yl", "c")
HALF = NY // 2
HD = 64
TOK = 256
D = 2048
COLS = D // NTP
ROW = NX * TOK
CAP = 20
SLOT = 24
SEND = 2 * CAP
ROWS = NSP * CAP
PADROWS = NSP * SLOT
FFL = 256
EPS = 1e-06
LOW = -1e30
bf = jnp.bfloat16
f32 = jnp.float32

INTERPRET = False


def call(body, out_shape, inputs, smem=0, scratch=(), limit=12):
    specs = [pl.BlockSpec(memory_space=pltpu.SMEM)] * smem
    specs += [pl.BlockSpec(memory_space=pltpu.VMEM)] * (len(inputs) - smem)
    many = isinstance(out_shape, (tuple, list))
    vm = pl.BlockSpec(memory_space=pltpu.VMEM)
    return pl.pallas_call(
        body,
        out_shape=out_shape,
        in_specs=specs,
        out_specs=tuple([vm] * len(out_shape)) if many else vm,
        scratch_shapes=list(scratch),
        interpret=INTERPRET,
        compiler_params=pltpu.CompilerParams(vmem_limit_bytes=limit * 1024 * 1024),
    )(*inputs)


def three(v):
    hi = v.astype(bf).astype(f32)
    rest = v - hi
    mid = rest.astype(bf).astype(f32)
    return hi, mid, rest - mid


def attend(at_ref, q_ref, kv_ref, gate_ref, out0_ref, out1_ref, out2_ref, out3_ref, qs_ref, s_ref, m_ref, acc_ref, o_ref):
    z, x = at_ref[0], at_ref[1]
    first = gate_ref[:, pl.ds(pl.multiple_of(z * ROW, ROW), TOK)][:, 0:1]
    row64 = lax.broadcasted_iota(jnp.int32, (HD, TOK), 0)
    ones = jnp.where(row64 < 3, 1.0, 0.0).astype(bf)
    for j in range(NX):
        qs_ref[0:HD, j * TOK : (j + 1) * TOK] = q_ref[j] * bf(HD**-0.5)
        qs_ref[HD : 2 * HD, j * TOK : (j + 1) * TOK] = ones

    def scores(zk):
        place = pl.multiple_of(zk * ROW + x * TOK, TOK)
        hi, mid, lo = three(first - gate_ref[:, pl.ds(place, TOK)])
        extra = jnp.where(row64 == 0, hi, jnp.where(row64 == 1, mid, jnp.where(row64 == 2, lo, 0.0)))
        both = jnp.concatenate([kv_ref[zk, 0:HD, :], extra.astype(bf)], axis=0)
        return jnp.dot(both.T, qs_ref[...], preferred_element_type=f32)

    s = scores(z)
    ki = lax.broadcasted_iota(jnp.int32, (TOK, ROW), 0) + x * TOK
    qi = lax.broadcasted_iota(jnp.int32, (TOK, ROW), 1)
    s = jnp.where(ki <= qi, s, LOW)
    s_ref[z] = s
    m_ref[...] = jnp.broadcast_to(jnp.max(s, axis=0, keepdims=True), (8, ROW))

    def look(zk, carry):
        s = scores(zk)
        s_ref[zk] = s
        m_ref[...] = jnp.maximum(m_ref[...], jnp.max(s, axis=0, keepdims=True))
        return carry

    def look_two(i, carry):
        one, two = scores(2 * i), scores(2 * i + 1)
        s_ref[2 * i] = one
        s_ref[2 * i + 1] = two
        top = jnp.max(jnp.maximum(one, two), axis=0, keepdims=True)
        m_ref[...] = jnp.maximum(m_ref[...], top)
        return carry

    lax.fori_loop(0, z // 2, look_two, 0)
    lax.fori_loop(z // 2 * 2, z, look, 0)
    m = m_ref[0:1, :]
    acc_ref[...] = jnp.zeros((HD + 16, ROW), f32)

    def weigh(zk, carry):
        p = jnp.exp(s_ref[zk] - m).astype(bf)
        v = jnp.concatenate([kv_ref[zk, HD : 2 * HD, :], jnp.ones((16, TOK), bf)], axis=0)
        acc_ref[...] += jnp.dot(v, p, preferred_element_type=f32)
        return carry

    def weigh_two(i, carry):
        zk = 2 * i
        p = jnp.exp(s_ref[pl.ds(zk, 2)].reshape(2 * TOK, ROW) - m).astype(bf)
        v = jnp.concatenate([kv_ref[zk, HD : 2 * HD, :], kv_ref[zk + 1, HD : 2 * HD, :]], axis=1)
        v = jnp.concatenate([v, jnp.ones((16, 2 * TOK), bf)], axis=0)
        acc_ref[...] += jnp.dot(v, p, preferred_element_type=f32)
        return carry

    lax.fori_loop(0, (z + 1) // 2, weigh_two, 0)
    lax.fori_loop((z + 1) // 2 * 2, z + 1, weigh, 0)
    row16 = lax.broadcasted_iota(jnp.int32, (16, ROW), 0)
    total = acc_ref[HD : HD + 1, :]
    hi, mid, lo = three(m + jnp.log(total))
    stats = jnp.where(row16 == 0, hi, jnp.where(row16 == 1, mid, jnp.where(row16 == 2, lo, 0.0))).astype(bf)
    o_ref[0:HD, :] = (acc_ref[0:HD, :] / total).astype(bf)
    o_ref[HD : HD + 16, :] = stats
    for j, out_ref in enumerate((out0_ref, out1_ref, out2_ref, out3_ref)):
        out_ref[...] = o_ref[:, pl.ds(pl.multiple_of(lax.rem(x + j, NX) * TOK, TOK), TOK)]


def merge(*refs):
    parts, out_ref = refs[0:NX], refs[NX]
    ls = []
    for i in range(NX):
        st = parts[i][HD : HD + 16, :].astype(f32)
        ls.append(st[0:1] + st[1:2] + st[2:3])
    m = ls[0]
    for v in ls[1:]:
        m = jnp.maximum(m, v)
    acc = jnp.zeros((HD, TOK), f32)
    total = jnp.zeros((1, TOK), f32)
    for i in range(NX):
        w = jnp.exp(ls[i] - m)
        total = total + w
        acc = acc + w * parts[i][0:HD, :].astype(f32)
    out_ref[...] = (acc / total).astype(bf)


def prepare(kvq_ref, w_ref, kv_ref, qs_ref, out_ref):
    for z in range(NZ):
        kv_ref[z] = kvq_ref[0 : 2 * HD, :]
    for x in range(NX):
        qs_ref[x] = kvq_ref[2 * HD :, :]
    for y in range(NY):
        for c in range(NC):
            for q in range(2):
                block = (y % HALF + q * HALF) * NC + c
                out_ref[y * NC + c, q * HD : (q + 1) * HD, :] = w_ref[:, block * COLS : (block + 1) * COLS]


def route(routes_ref, pick_ref, back_ref):
    e0, e1 = routes_ref[0:1, :], routes_ref[1:2, :]
    io = lax.broadcasted_iota(jnp.int32, (NSP, TOK), 0)
    h0, h1 = io == e0, io == e1
    hit = jnp.where(h0, 1.0, jnp.where(h1, 1.0, 0.0)).astype(bf)
    ia = lax.broadcasted_iota(jnp.int32, (TOK, TOK), 0)
    ib = lax.broadcasted_iota(jnp.int32, (TOK, TOK), 1)
    upper = jnp.where(ia < ib, 1.0, 0.0).astype(bf)
    before = jnp.dot(hit, upper, preferred_element_type=f32)
    r0 = jnp.sum(jnp.where(h0, before, 0.0), axis=0, keepdims=True).astype(jnp.int32)
    r1 = jnp.sum(jnp.where(h1, before, 0.0), axis=0, keepdims=True).astype(jnp.int32)
    slots = jnp.concatenate([2 * SLOT * e0 + r0, 2 * SLOT * e1 + r1, jnp.zeros((6, TOK), jnp.int32)], axis=0)
    slots = slots.astype(f32).T
    at = lax.broadcasted_iota(jnp.int32, (TOK, 2 * PADROWS), 1).astype(f32)
    for k in range(2):
        slot = slots[:, k : k + 1]
        back_ref[k * TOK : (k + 1) * TOK, :] = jnp.where((at == slot) | (at == slot + SLOT), 1.0, 0.0).astype(bf)
    s0 = e0 * SEND + r0
    s1 = e1 * SEND + r1
    ir = lax.broadcasted_iota(jnp.int32, (NSP * SEND, TOK), 0)
    hits = (ir == s0) | (ir == s1) | (ir == s0 + CAP) | (ir == s1 + CAP)
    pick_ref[...] = jnp.where(hits, 1.0, 0.0).astype(bf)


def project(at_ref, att_ref, w_ref, resid_ref, gain_ref, pick_ref, stream_ref, out_ref):
    c0 = pl.multiple_of(at_ref[0], COLS)
    c1 = pl.multiple_of(at_ref[1], COLS)
    weights = [jnp.concatenate([w_ref[t, q * HD : (q + 1) * HD, :] for t in range(NTP)], axis=0) for q in range(2)]
    w = jnp.concatenate(weights, axis=1)
    mixed = lax.dot_general(att_ref[...], w, (((0,), (0,)), ((), ())), preferred_element_type=f32)
    resid = jnp.concatenate([resid_ref[:, pl.ds(c0, COLS)], resid_ref[:, pl.ds(c1, COLS)]], axis=1)
    gain = jnp.concatenate([gain_ref[:, pl.ds(c0, COLS)], gain_ref[:, pl.ds(c1, COLS)]], axis=1)
    stream = resid.astype(f32) + mixed
    stream_ref[...] = jnp.where(at_ref[2] == 0, stream[:, 0:COLS], stream[:, COLS:])
    scaled = (stream * gain).astype(bf)
    sent = jnp.dot(pick_ref[...], scaled, preferred_element_type=f32).reshape(NSP, SEND, 2 * COLS)
    rank = lax.broadcasted_iota(jnp.int32, (NSP, SEND, COLS), 1)
    out_ref[...] = jnp.where(rank < CAP, sent[:, :, 0:COLS], sent[:, :, COLS:]).astype(bf)


def squeeze(in_ref, all_ref, low_ref, high_ref, rows_ref):
    for i in range(NSP):
        x = in_ref[i].astype(f32)
        rows_ref[ROWS + CAP * i : ROWS + CAP * i + CAP, :] = x[0:CAP, :]
        rows_ref[CAP * i : CAP * i + CAP, :] = x[CAP : 2 * CAP, :]
    all_ref[...] = rows_ref[...].astype(bf)
    high_ref[...] = rows_ref[0:ROWS, :].astype(bf)
    low_ref[...] = rows_ref[ROWS:, :].astype(bf)


NEAR = ((0, 0, 0, ROWS), (0, 1, 0, 0), (3, 0, 1, ROWS), (3, 1, 1, 0), (1, 0, 2, ROWS), (1, 1, 2, 0))
FAR = ((2, 0, 0, 0), (2, 1, 1, 0))
SENDS = (
    (0, 0, 2, 0),
    (0, ROWS, 2, 1),
    (1, 0, 1, 0),
    (1, ROWS, 1, 1),
    (1, 2 * ROWS, 3, 0),
    (1, 3 * ROWS, 3, 1),
    (1, 4 * ROWS, 0, 0),
    (1, 5 * ROWS, 0, 1),
)


def accumulate(y, c, pieces, owns, others, wg_ref, wu_ref, gain_ref, g_ref, u_ref, sq_ref, fresh):
    for off, upper, n, at in pieces:
        mine, theirs = owns[n][at : at + ROWS, :], others[n][at : at + ROWS, :]
        block = lax.rem(y + off, HALF) + upper * HALF
        first = pl.multiple_of((2 * block + c) * COLS, COLS)
        second = pl.multiple_of((2 * block + 1 - c) * COLS, COLS)
        xx = jnp.concatenate([mine, theirs], axis=1)
        for w_ref, acc_ref in ((wg_ref, g_ref), (wu_ref, u_ref)):
            w = jnp.concatenate([w_ref[pl.ds(first, COLS), :], w_ref[pl.ds(second, COLS), :]], axis=0)
            part = jnp.dot(xx, w, preferred_element_type=f32)
            acc_ref[...] = part if fresh else acc_ref[...] + part
        a = mine.astype(f32) * (1.0 / gain_ref[:, pl.ds(first, COLS)])
        b = theirs.astype(f32) * (1.0 / gain_ref[:, pl.ds(second, COLS)])
        part = a * a + b * b
        sq_ref[...] = part if fresh else sq_ref[...] + part
        fresh = False


def experts_near(at_ref, every_ref, n0_ref, n1_ref, swap_ref, near_ref, wg_ref, wu_ref, gain_ref, g_ref, u_ref, sq_ref):
    owns = (every_ref, n0_ref, n1_ref)
    others = (swap_ref, near_ref.at[0 : 2 * ROWS], near_ref.at[2 * ROWS :])
    accumulate(at_ref[0], at_ref[1], NEAR, owns, others, wg_ref, wu_ref, gain_ref, g_ref, u_ref, sq_ref, True)


def experts(at_ref, f0_ref, f1_ref, far_ref, g_in, u_in, sq_in, wg_ref, wu_ref, wd_ref, gain_ref, *refs):
    outs = refs[0:4]
    g_ref, u_ref, sq_ref, h_ref = refs[4:]
    y, c = at_ref[0], at_ref[1]
    others = (far_ref.at[0:ROWS], far_ref.at[ROWS:])
    g_ref[...] = g_in[...]
    u_ref[...] = u_in[...]
    sq_ref[...] = sq_in[...]
    accumulate(y, c, FAR, (f0_ref, f1_ref), others, wg_ref, wu_ref, gain_ref, g_ref, u_ref, sq_ref, False)
    scale = lax.rsqrt(jnp.sum(sq_ref[...], axis=1, keepdims=True) / D + EPS)
    gate = g_ref[...] * scale
    up = u_ref[...] * scale
    h_ref[...] = (gate / (1.0 + jnp.exp(-gate)) * up).astype(bf)
    even = c == 0
    for ref, at, off, upper in SENDS:
        block = lax.rem(y + off, HALF) + upper * HALF
        place = pl.multiple_of(2 * block * COLS, 2 * COLS)
        res = jnp.dot(h_ref[...], wd_ref[:, pl.ds(place, 2 * COLS)], preferred_element_type=f32)
        low, high = res[:, 0:COLS], res[:, COLS:]
        outs[ref][at : at + ROWS, :] = jnp.where(even, low, high).astype(bf)
        outs[ref + 2][at : at + ROWS, :] = jnp.where(even, high, low).astype(bf)


def gather_sum(mine_ref, theirs_ref, n0_ref, n1_ref, f0_ref, f1_ref, out_ref, rows_ref):
    base = 4 * ROWS
    pad = jnp.zeros((SLOT - CAP, COLS), f32)
    for q, far_ref in enumerate((f0_ref, f1_ref)):
        at = slice(q * ROWS, (q + 1) * ROWS)
        kept = slice(base + q * ROWS, base + (q + 1) * ROWS)
        acc = mine_ref[kept, :].astype(f32) + theirs_ref[kept, :].astype(f32)
        acc = acc + n0_ref[at, :].astype(f32) + n1_ref[at, :].astype(f32)
        rows_ref[...] = acc + far_ref[...].astype(f32)
        for i in range(NSP):
            out_ref[2 * i + q] = jnp.concatenate([rows_ref[CAP * i : CAP * i + CAP, :], pad], axis=0).astype(bf)


def finish(ret_ref, back_ref, rw_ref, stream_ref, out_ref):
    weight = jnp.concatenate([rw_ref[...], jnp.zeros((6, TOK), f32)], axis=0).T
    got = jnp.dot(back_ref[...], ret_ref[...], preferred_element_type=f32)
    out = stream_ref[...] + weight[:, 0:1] * got[0:TOK, :] + weight[:, 1:2] * got[TOK:, :]
    out_ref[...] = out.astype(bf)


def shift(v, by):
    return lax.ppermute(v, Y, [(i, (i + by) % NY) for i in range(NY)])


def exchange(v, axis):
    return lax.all_to_all(v, axis, 0, 0, tiled=True)


def layer(
    queries,
    keys,
    values,
    cum_gate,
    out_weight,
    resid,
    norm_gain,
    routes,
    route_weight,
    gate_weight,
    up_weight,
    down_weight,
):
    z, x, y, c = (lax.axis_index(a) for a in ("z", "x", Y, "c"))
    sds = jax.ShapeDtypeStruct
    half = NY // 2
    low = (lax.rem(y, half) * NC + c) * COLS
    at_cols = jnp.stack([low, low + half * NC * COLS, y // half]).astype(jnp.int32)
    at = jnp.stack([z, x]).astype(jnp.int32)
    kv_send, q_send, w_send = call(
        prepare,
        (sds((NZ, 2 * HD, TOK), bf), sds((NX, HD, TOK), bf), sds((NTP, 2 * HD, COLS), bf)),
        (jnp.concatenate([keys.T, values.T, queries.T], axis=0), out_weight),
    )
    q_send, w_send, at, at_cols = lax.optimization_barrier((q_send, w_send, at, at_cols))
    q = exchange(q_send, "x")
    kv_send, q = lax.optimization_barrier((kv_send, q))
    kv = exchange(kv_send, "z")
    w_cols = exchange(w_send, TP)
    sent = call(
        attend,
        (sds((HD + 16, TOK), bf),) * NX,
        (at, q, kv, cum_gate),
        smem=1,
        scratch=(
            pltpu.VMEM((2 * HD, ROW), bf),
            pltpu.VMEM((NZ, TOK, ROW), f32),
            pltpu.VMEM((8, ROW), f32),
            pltpu.VMEM((HD + 16, ROW), f32),
            pltpu.VMEM((HD + 16, ROW), bf),
        ),
        limit=24,
    )
    parts = [sent[0]]
    for n in range(1, NX):
        parts.append(lax.ppermute(sent[n], "x", [(i, (i + n) % NX) for i in range(NX)]))
    pick, back_pick = call(
        route, (sds((NSP * SEND, TOK), bf), sds((2 * TOK, 2 * PADROWS), bf)), (routes.T,)
    )
    attended = call(merge, sds((HD, TOK), bf), tuple(parts))
    attended = lax.all_gather(attended, TP, axis=0, tiled=True)
    stream, outgoing = call(
        project,
        (sds((TOK, COLS), f32), sds((NSP, SEND, COLS), bf)),
        (at_cols, attended, w_cols, resid, norm_gain.reshape(1, D), pick),
        smem=1,
    )
    arrived = exchange(outgoing, SP)
    every, lower, higher = call(
        squeeze,
        (sds((2 * ROWS, COLS), bf), sds((ROWS, COLS), bf), sds((ROWS, COLS), bf)),
        (arrived,),
        scratch=(pltpu.VMEM((2 * ROWS, COLS), f32),),
    )
    swap = [(0, 1), (1, 0)]
    owns = [every]
    for v, by in ((every, 1), (every, -1), (lower, 2), (higher, -2)):
        owns.append(shift(v, by))
    others = []
    for v in (every, jnp.concatenate(owns[1:3], axis=0), jnp.concatenate(owns[3:5], axis=0)):
        others.append(lax.ppermute(v, "c", swap))
    gain = norm_gain.reshape(1, D)
    at_yc = jnp.stack([y, c]).astype(jnp.int32)
    sums = (sds((ROWS, FFL), f32), sds((ROWS, FFL), f32), sds((ROWS, COLS), f32))
    partial = call(experts_near, sums, (at_yc, *owns[0:3], *others[0:2], gate_weight[0], up_weight[0], gain), smem=1)
    far_out, near_out = sds((2 * ROWS, COLS), bf), sds((6 * ROWS, COLS), bf)
    far_mine, near_mine, far_theirs, near_theirs = call(
        experts,
        (far_out, near_out, far_out, near_out),
        (at_yc, *owns[3:5], others[2], *partial, gate_weight[0], up_weight[0], down_weight[0], gain),
        smem=1,
        scratch=[pltpu.VMEM(v.shape, f32) for v in sums] + [pltpu.VMEM((ROWS, FFL), bf)],
    )
    far_theirs = lax.ppermute(far_theirs, "c", swap)
    near_theirs = lax.ppermute(near_theirs, "c", swap)

    def pair(a, b, first, count):
        part = slice(first * ROWS, (first + count) * ROWS)
        return (a[part].astype(f32) + b[part].astype(f32)).astype(bf)

    got = []
    for a, b, first, count, by in (
        (far_mine, far_theirs, 0, 1, 2),
        (far_mine, far_theirs, 1, 1, -2),
        (near_mine, near_theirs, 0, 2, 1),
        (near_mine, near_theirs, 2, 2, -1),
    ):
        got.append(shift(pair(a, b, first, count), by))
    back = call(
        gather_sum,
        sds((2 * NSP, SLOT, COLS), bf),
        (near_mine, near_theirs, got[2], got[3], got[0], got[1]),
        scratch=(pltpu.VMEM((ROWS, COLS), f32),),
    )
    returned = exchange(back, ("z", "x", "yh")).reshape(2 * PADROWS, COLS)
    return call(finish, sds((TOK, COLS), bf), (returned, back_pick, route_weight.T, stream))


def solution(mesh):
    grid = Mesh(mesh.devices.reshape(NZ, NX, 2, HALF, NC), ("z", "x", "yh", "yl", "c"))
    return jax.shard_map(
        layer,
        mesh=grid,
        in_specs=(
            P(SP, TP),
            P(SP, TP),
            P(SP, TP),
            P(TP, None),
            P(TP, None),
            P(SP, None),
            P(),
            P(SP, None),
            P(SP, None),
            P(SP, None, TP),
            P(SP, None, TP),
            P(SP, TP, None),
        ),
        out_specs=P(SP, TP),
        check_vma=False,
    )
```

```python
import jax
import jax.numpy as jnp
from jax import lax
from jax.experimental import pallas as pl
from jax.experimental.pallas import tpu as pltpu
from jax.sharding import Mesh, PartitionSpec as P


NZ, NX, NY, NC = 8, 4, 8, 2
NSP, NTP = NZ * NX, NY * NC
Y = ("yh", "yl")
SP, TP = ("z", "x"), ("yh", "yl", "c")
HALF = NY // 2
HD = 64
TOK = 256
D = 2048
COLS = D // NTP
ROW = NX * TOK
CAP = 20
SLOT = 24
SEND = 2 * CAP
ROWS = NSP * CAP
PADROWS = NSP * SLOT
FFL = 256
EPS = 1e-06
LOW = -1e30
bf = jnp.bfloat16
f32 = jnp.float32

INTERPRET = False


def call(body, out_shape, inputs, smem=0, scratch=(), limit=12):
    specs = [pl.BlockSpec(memory_space=pltpu.SMEM)] * smem
    specs += [pl.BlockSpec(memory_space=pltpu.VMEM)] * (len(inputs) - smem)
    many = isinstance(out_shape, (tuple, list))
    vm = pl.BlockSpec(memory_space=pltpu.VMEM)
    return pl.pallas_call(
        body,
        out_shape=out_shape,
        in_specs=specs,
        out_specs=tuple([vm] * len(out_shape)) if many else vm,
        scratch_shapes=list(scratch),
        interpret=INTERPRET,
        compiler_params=pltpu.CompilerParams(vmem_limit_bytes=limit * 1024 * 1024),
    )(*inputs)


def three(v):
    hi = v.astype(bf).astype(f32)
    rest = v - hi
    mid = rest.astype(bf).astype(f32)
    return hi, mid, rest - mid


def attend(at_ref, q_ref, kv_ref, gate_ref, out0_ref, out1_ref, out2_ref, out3_ref, qs_ref, s_ref, m_ref, acc_ref, o_ref):
    z, x = at_ref[0], at_ref[1]
    first = gate_ref[:, pl.ds(pl.multiple_of(z * ROW, ROW), TOK)][:, 0:1]
    row64 = lax.broadcasted_iota(jnp.int32, (HD, TOK), 0)
    ones = jnp.where(row64 < 3, 1.0, 0.0).astype(bf)
    for j in range(NX):
        qs_ref[0:HD, j * TOK : (j + 1) * TOK] = q_ref[j] * bf(HD**-0.5)
        qs_ref[HD : 2 * HD, j * TOK : (j + 1) * TOK] = ones

    def scores(zk):
        place = pl.multiple_of(zk * ROW + x * TOK, TOK)
        hi, mid, lo = three(first - gate_ref[:, pl.ds(place, TOK)])
        extra = jnp.where(row64 == 0, hi, jnp.where(row64 == 1, mid, jnp.where(row64 == 2, lo, 0.0)))
        both = jnp.concatenate([kv_ref[zk, 0:HD, :], extra.astype(bf)], axis=0)
        return jnp.dot(both.T, qs_ref[...], preferred_element_type=f32)

    s = scores(z)
    ki = lax.broadcasted_iota(jnp.int32, (TOK, ROW), 0) + x * TOK
    qi = lax.broadcasted_iota(jnp.int32, (TOK, ROW), 1)
    s = jnp.where(ki <= qi, s, LOW)
    s_ref[z] = s
    m_ref[...] = jnp.broadcast_to(jnp.max(s, axis=0, keepdims=True), (8, ROW))

    def look(zk, carry):
        s = scores(zk)
        s_ref[zk] = s
        m_ref[...] = jnp.maximum(m_ref[...], jnp.max(s, axis=0, keepdims=True))
        return carry

    def look_two(i, carry):
        one, two = scores(2 * i), scores(2 * i + 1)
        s_ref[2 * i] = one
        s_ref[2 * i + 1] = two
        top = jnp.max(jnp.maximum(one, two), axis=0, keepdims=True)
        m_ref[...] = jnp.maximum(m_ref[...], top)
        return carry

    lax.fori_loop(0, z // 2, look_two, 0)
    lax.fori_loop(z // 2 * 2, z, look, 0)
    m = m_ref[0:1, :]
    acc_ref[...] = jnp.zeros((HD + 16, ROW), f32)

    def weigh(zk, carry):
        p = jnp.exp(s_ref[zk] - m).astype(bf)
        v = jnp.concatenate([kv_ref[zk, HD : 2 * HD, :], jnp.ones((16, TOK), bf)], axis=0)
        acc_ref[...] += jnp.dot(v, p, preferred_element_type=f32)
        return carry

    def weigh_two(i, carry):
        zk = 2 * i
        p = jnp.exp(s_ref[pl.ds(zk, 2)].reshape(2 * TOK, ROW) - m).astype(bf)
        v = jnp.concatenate([kv_ref[zk, HD : 2 * HD, :], kv_ref[zk + 1, HD : 2 * HD, :]], axis=1)
        v = jnp.concatenate([v, jnp.ones((16, 2 * TOK), bf)], axis=0)
        acc_ref[...] += jnp.dot(v, p, preferred_element_type=f32)
        return carry

    lax.fori_loop(0, (z + 1) // 2, weigh_two, 0)
    lax.fori_loop((z + 1) // 2 * 2, z + 1, weigh, 0)
    row16 = lax.broadcasted_iota(jnp.int32, (16, ROW), 0)
    total = acc_ref[HD : HD + 1, :]
    hi, mid, lo = three(m + jnp.log(total))
    stats = jnp.where(row16 == 0, hi, jnp.where(row16 == 1, mid, jnp.where(row16 == 2, lo, 0.0))).astype(bf)
    o_ref[0:HD, :] = (acc_ref[0:HD, :] / total).astype(bf)
    o_ref[HD : HD + 16, :] = stats
    for j, out_ref in enumerate((out0_ref, out1_ref, out2_ref, out3_ref)):
        out_ref[...] = o_ref[:, pl.ds(pl.multiple_of(lax.rem(x + j, NX) * TOK, TOK), TOK)]


def merge(*refs):
    parts, out_ref = refs[0:NX], refs[NX]
    ls = []
    for i in range(NX):
        st = parts[i][HD : HD + 16, :].astype(f32)
        ls.append(st[0:1] + st[1:2] + st[2:3])
    m = ls[0]
    for v in ls[1:]:
        m = jnp.maximum(m, v)
    acc = jnp.zeros((HD, TOK), f32)
    total = jnp.zeros((1, TOK), f32)
    for i in range(NX):
        w = jnp.exp(ls[i] - m)
        total = total + w
        acc = acc + w * parts[i][0:HD, :].astype(f32)
    out_ref[...] = (acc / total).astype(bf)


def prepare(kvq_ref, kv_ref, qs_ref):
    for z in range(NZ):
        kv_ref[z] = kvq_ref[0 : 2 * HD, :]
    for x in range(NX):
        qs_ref[x] = kvq_ref[2 * HD :, :]


def spread_weight(w_ref, out_ref):
    for y in range(NY):
        for c in range(NC):
            for q in range(2):
                block = (y % HALF + q * HALF) * NC + c
                out_ref[y * NC + c, q * HD : (q + 1) * HD, :] = w_ref[:, block * COLS : (block + 1) * COLS]


def route(at_ref, routes_ref, resid_ref, pick_ref, back_ref, cols_ref):
    for q in range(2):
        cols_ref[:, q * COLS : (q + 1) * COLS] = resid_ref[:, pl.ds(pl.multiple_of(at_ref[q], COLS), COLS)]
    e0, e1 = routes_ref[0:1, :], routes_ref[1:2, :]
    io = lax.broadcasted_iota(jnp.int32, (NSP, TOK), 0)
    h0, h1 = io == e0, io == e1
    hit = jnp.where(h0, 1.0, jnp.where(h1, 1.0, 0.0)).astype(bf)
    ia = lax.broadcasted_iota(jnp.int32, (TOK, TOK), 0)
    ib = lax.broadcasted_iota(jnp.int32, (TOK, TOK), 1)
    upper = jnp.where(ia < ib, 1.0, 0.0).astype(bf)
    before = jnp.dot(hit, upper, preferred_element_type=f32)
    r0 = jnp.sum(jnp.where(h0, before, 0.0), axis=0, keepdims=True).astype(jnp.int32)
    r1 = jnp.sum(jnp.where(h1, before, 0.0), axis=0, keepdims=True).astype(jnp.int32)
    slots = jnp.concatenate([2 * SLOT * e0 + r0, 2 * SLOT * e1 + r1, jnp.zeros((6, TOK), jnp.int32)], axis=0)
    slots = slots.astype(f32).T
    at = lax.broadcasted_iota(jnp.int32, (TOK, 2 * PADROWS), 1).astype(f32)
    for k in range(2):
        slot = slots[:, k : k + 1]
        back_ref[k * TOK : (k + 1) * TOK, :] = jnp.where((at == slot) | (at == slot + SLOT), 1.0, 0.0).astype(bf)
    s0 = e0 * SEND + r0
    s1 = e1 * SEND + r1
    ir = lax.broadcasted_iota(jnp.int32, (NSP * SEND, TOK), 0)
    hits = (ir == s0) | (ir == s1) | (ir == s0 + CAP) | (ir == s1 + CAP)
    pick_ref[...] = jnp.where(hits, 1.0, 0.0).astype(bf)


def project(at_ref, att_ref, w_ref, resid_ref, gain_ref, pick_ref, stream_ref, out_ref):
    c0 = pl.multiple_of(at_ref[0], COLS)
    c1 = pl.multiple_of(at_ref[1], COLS)
    weights = [jnp.concatenate([w_ref[t, q * HD : (q + 1) * HD, :] for t in range(NTP)], axis=0) for q in range(2)]
    w = jnp.concatenate(weights, axis=1)
    mixed = lax.dot_general(att_ref[...], w, (((0,), (0,)), ((), ())), preferred_element_type=f32)
    gain = jnp.concatenate([gain_ref[:, pl.ds(c0, COLS)], gain_ref[:, pl.ds(c1, COLS)]], axis=1)
    stream = resid_ref[...].astype(f32) + mixed
    stream_ref[...] = jnp.where(at_ref[2] == 0, stream[:, 0:COLS], stream[:, COLS:])
    scaled = (stream * gain).astype(bf)
    sent = jnp.dot(pick_ref[...], scaled, preferred_element_type=f32).reshape(NSP, SEND, 2 * COLS)
    rank = lax.broadcasted_iota(jnp.int32, (NSP, SEND, COLS), 1)
    out_ref[...] = jnp.where(rank < CAP, sent[:, :, 0:COLS], sent[:, :, COLS:]).astype(bf)


def squeeze(in_ref, all_ref, low_ref, high_ref, rows_ref):
    for i in range(NSP):
        x = in_ref[i].astype(f32)
        rows_ref[ROWS + CAP * i : ROWS + CAP * i + CAP, :] = x[0:CAP, :]
        rows_ref[CAP * i : CAP * i + CAP, :] = x[CAP : 2 * CAP, :]
    all_ref[...] = rows_ref[...].astype(bf)
    high_ref[...] = rows_ref[0:ROWS, :].astype(bf)
    low_ref[...] = rows_ref[ROWS:, :].astype(bf)


NEAR = ((0, 0, 0, ROWS), (0, 1, 0, 0), (3, 0, 1, ROWS), (3, 1, 1, 0), (1, 0, 2, ROWS), (1, 1, 2, 0))
FAR = ((2, 0, 0, 0), (2, 1, 1, 0))
SENDS = (
    (0, 0, 2, 0),
    (0, ROWS, 2, 1),
    (1, 0, 1, 0),
    (1, ROWS, 1, 1),
    (1, 2 * ROWS, 3, 0),
    (1, 3 * ROWS, 3, 1),
    (1, 4 * ROWS, 0, 0),
    (1, 5 * ROWS, 0, 1),
)


def accumulate(y, c, pieces, owns, others, wg_ref, wu_ref, gain_ref, g_ref, u_ref, sq_ref, fresh):
    for off, upper, n, at in pieces:
        mine, theirs = owns[n][at : at + ROWS, :], others[n][at : at + ROWS, :]
        block = lax.rem(y + off, HALF) + upper * HALF
        first = pl.multiple_of((2 * block + c) * COLS, COLS)
        second = pl.multiple_of((2 * block + 1 - c) * COLS, COLS)
        xx = jnp.concatenate([mine, theirs], axis=1)
        for w_ref, acc_ref in ((wg_ref, g_ref), (wu_ref, u_ref)):
            w = jnp.concatenate([w_ref[pl.ds(first, COLS), :], w_ref[pl.ds(second, COLS), :]], axis=0)
            part = jnp.dot(xx, w, preferred_element_type=f32)
            acc_ref[...] = part if fresh else acc_ref[...] + part
        a = mine.astype(f32) * (1.0 / gain_ref[:, pl.ds(first, COLS)])
        b = theirs.astype(f32) * (1.0 / gain_ref[:, pl.ds(second, COLS)])
        part = a * a + b * b
        sq_ref[...] = part if fresh else sq_ref[...] + part
        fresh = False


def experts_near(at_ref, every_ref, n0_ref, n1_ref, swap_ref, near_ref, wg_ref, wu_ref, gain_ref, g_ref, u_ref, sq_ref):
    owns = (every_ref, n0_ref, n1_ref)
    others = (swap_ref, near_ref.at[0 : 2 * ROWS], near_ref.at[2 * ROWS :])
    accumulate(at_ref[0], at_ref[1], NEAR, owns, others, wg_ref, wu_ref, gain_ref, g_ref, u_ref, sq_ref, True)


def experts(at_ref, f0_ref, f1_ref, far_ref, g_in, u_in, sq_in, wg_ref, wu_ref, wd_ref, gain_ref, *refs):
    outs = refs[0:4]
    g_ref, u_ref, sq_ref, h_ref = refs[4:]
    y, c = at_ref[0], at_ref[1]
    others = (far_ref.at[0:ROWS], far_ref.at[ROWS:])
    g_ref[...] = g_in[...]
    u_ref[...] = u_in[...]
    sq_ref[...] = sq_in[...]
    accumulate(y, c, FAR, (f0_ref, f1_ref), others, wg_ref, wu_ref, gain_ref, g_ref, u_ref, sq_ref, False)
    scale = lax.rsqrt(jnp.sum(sq_ref[...], axis=1, keepdims=True) / D + EPS)
    gate = g_ref[...] * scale
    up = u_ref[...] * scale
    h_ref[...] = (gate / (1.0 + jnp.exp(-gate)) * up).astype(bf)
    even = c == 0
    for ref, at, off, upper in SENDS:
        block = lax.rem(y + off, HALF) + upper * HALF
        place = pl.multiple_of(2 * block * COLS, 2 * COLS)
        res = jnp.dot(h_ref[...], wd_ref[:, pl.ds(place, 2 * COLS)], preferred_element_type=f32)
        low, high = res[:, 0:COLS], res[:, COLS:]
        outs[ref][at : at + ROWS, :] = jnp.where(even, low, high).astype(bf)
        outs[ref + 2][at : at + ROWS, :] = jnp.where(even, high, low).astype(bf)


def gather_sum(mine_ref, theirs_ref, n0_ref, n1_ref, f0_ref, f1_ref, out_ref, rows_ref):
    base = 4 * ROWS
    pad = jnp.zeros((SLOT - CAP, COLS), f32)
    for q, far_ref in enumerate((f0_ref, f1_ref)):
        at = slice(q * ROWS, (q + 1) * ROWS)
        kept = slice(base + q * ROWS, base + (q + 1) * ROWS)
        acc = mine_ref[kept, :].astype(f32) + theirs_ref[kept, :].astype(f32)
        acc = acc + n0_ref[at, :].astype(f32) + n1_ref[at, :].astype(f32)
        rows_ref[...] = acc + far_ref[...].astype(f32)
        for i in range(NSP):
            out_ref[2 * i + q] = jnp.concatenate([rows_ref[CAP * i : CAP * i + CAP, :], pad], axis=0).astype(bf)


def finish(ret_ref, back_ref, rw_ref, stream_ref, out_ref):
    weight = jnp.concatenate([rw_ref[...], jnp.zeros((6, TOK), f32)], axis=0).T
    got = jnp.dot(back_ref[...], ret_ref[...], preferred_element_type=f32)
    out = stream_ref[...] + weight[:, 0:1] * got[0:TOK, :] + weight[:, 1:2] * got[TOK:, :]
    out_ref[...] = out.astype(bf)


def shift(v, by):
    return lax.ppermute(v, Y, [(i, (i + by) % NY) for i in range(NY)])


def exchange(v, axis):
    return lax.all_to_all(v, axis, 0, 0, tiled=True)


def layer(
    queries,
    keys,
    values,
    cum_gate,
    out_weight,
    resid,
    norm_gain,
    routes,
    route_weight,
    gate_weight,
    up_weight,
    down_weight,
):
    z, x, y, c = (lax.axis_index(a) for a in ("z", "x", Y, "c"))
    sds = jax.ShapeDtypeStruct
    half = NY // 2
    low = (lax.rem(y, half) * NC + c) * COLS
    at_cols = jnp.stack([low, low + half * NC * COLS, y // half]).astype(jnp.int32)
    at = jnp.stack([z, x]).astype(jnp.int32)
    kv_send, q_send = call(
        prepare,
        (sds((NZ, 2 * HD, TOK), bf), sds((NX, HD, TOK), bf)),
        (jnp.concatenate([keys.T, values.T, queries.T], axis=0),),
    )
    q_send, at, at_cols = lax.optimization_barrier((q_send, at, at_cols))
    q = exchange(q_send, "x")
    kv_send, q = lax.optimization_barrier((kv_send, q))
    kv = exchange(kv_send, "z")
    w_raw, kv = lax.optimization_barrier((out_weight, kv))
    w_send = call(spread_weight, sds((NTP, 2 * HD, COLS), bf), (w_raw,))
    w_cols = exchange(w_send, TP)
    sent = call(
        attend,
        (sds((HD + 16, TOK), bf),) * NX,
        (at, q, kv, cum_gate),
        smem=1,
        scratch=(
            pltpu.VMEM((2 * HD, ROW), bf),
            pltpu.VMEM((NZ, TOK, ROW), f32),
            pltpu.VMEM((8, ROW), f32),
            pltpu.VMEM((HD + 16, ROW), f32),
            pltpu.VMEM((HD + 16, ROW), bf),
        ),
        limit=14,
    )
    parts = [sent[0]]
    for n in range(1, NX):
        parts.append(lax.ppermute(sent[n], "x", [(i, (i + n) % NX) for i in range(NX)]))
    pick, back_pick, resid_cols = call(
        route,
        (sds((NSP * SEND, TOK), bf), sds((2 * TOK, 2 * PADROWS), bf), sds((TOK, 2 * COLS), bf)),
        (at_cols, routes.T, resid),
        smem=1,
    )
    attended = call(merge, sds((HD, TOK), bf), tuple(parts))
    attended = lax.all_gather(attended, TP, axis=0, tiled=True)
    stream, outgoing = call(
        project,
        (sds((TOK, COLS), f32), sds((NSP, SEND, COLS), bf)),
        (at_cols, attended, w_cols, resid_cols, norm_gain.reshape(1, D), pick),
        smem=1,
    )
    arrived = exchange(outgoing, SP)
    every, lower, higher = call(
        squeeze,
        (sds((2 * ROWS, COLS), bf), sds((ROWS, COLS), bf), sds((ROWS, COLS), bf)),
        (arrived,),
        scratch=(pltpu.VMEM((2 * ROWS, COLS), f32),),
    )
    swap = [(0, 1), (1, 0)]
    owns = [every]
    for v, by in ((every, 1), (every, -1), (lower, 2), (higher, -2)):
        owns.append(shift(v, by))
    others = []
    for v in (every, jnp.concatenate(owns[1:3], axis=0), jnp.concatenate(owns[3:5], axis=0)):
        others.append(lax.ppermute(v, "c", swap))
    gain = norm_gain.reshape(1, D)
    at_yc = jnp.stack([y, c]).astype(jnp.int32)
    sums = (sds((ROWS, FFL), f32), sds((ROWS, FFL), f32), sds((ROWS, COLS), f32))
    partial = call(experts_near, sums, (at_yc, *owns[0:3], *others[0:2], gate_weight[0], up_weight[0], gain), smem=1)
    far_out, near_out = sds((2 * ROWS, COLS), bf), sds((6 * ROWS, COLS), bf)
    far_mine, near_mine, far_theirs, near_theirs = call(
        experts,
        (far_out, near_out, far_out, near_out),
        (at_yc, *owns[3:5], others[2], *partial, gate_weight[0], up_weight[0], down_weight[0], gain),
        smem=1,
        scratch=[pltpu.VMEM(v.shape, f32) for v in sums] + [pltpu.VMEM((ROWS, FFL), bf)],
    )
    far_theirs = lax.ppermute(far_theirs, "c", swap)
    near_theirs = lax.ppermute(near_theirs, "c", swap)

    def pair(a, b, first, count):
        part = slice(first * ROWS, (first + count) * ROWS)
        return (a[part].astype(f32) + b[part].astype(f32)).astype(bf)

    got = []
    for a, b, first, count, by in (
        (far_mine, far_theirs, 0, 1, 2),
        (far_mine, far_theirs, 1, 1, -2),
        (near_mine, near_theirs, 0, 2, 1),
        (near_mine, near_theirs, 2, 2, -1),
    ):
        got.append(shift(pair(a, b, first, count), by))
    back = call(
        gather_sum,
        sds((2 * NSP, SLOT, COLS), bf),
        (near_mine, near_theirs, got[2], got[3], got[0], got[1]),
        scratch=(pltpu.VMEM((ROWS, COLS), f32),),
    )
    returned = exchange(back, ("z", "x", "yh")).reshape(2 * PADROWS, COLS)
    return call(finish, sds((TOK, COLS), bf), (returned, back_pick, route_weight.T, stream))


def solution(mesh):
    grid = Mesh(mesh.devices.reshape(NZ, NX, 2, HALF, NC), ("z", "x", "yh", "yl", "c"))
    return jax.shard_map(
        layer,
        mesh=grid,
        in_specs=(
            P(SP, TP),
            P(SP, TP),
            P(SP, TP),
            P(TP, None),
            P(TP, None),
            P(SP, None),
            P(),
            P(SP, None),
            P(SP, None),
            P(SP, None, TP),
            P(SP, None, TP),
            P(SP, TP, None),
        ),
        out_specs=P(SP, TP),
        check_vma=False,
    )
```

```python
import jax
import jax.numpy as jnp
from jax import lax
from jax.experimental import pallas as pl
from jax.experimental.pallas import tpu as pltpu
from jax.sharding import Mesh, PartitionSpec as P


NZ, NX, NY, NC = 8, 4, 8, 2
NSP, NTP = NZ * NX, NY * NC
Y = ("yh", "yl")
SP, TP = ("z", "x"), ("yh", "yl", "c")
HALF = NY // 2
HD = 64
TOK = 256
D = 2048
COLS = D // NTP
ROW = NX * TOK
CAP = 20
SLOT = 24
SEND = 2 * CAP
ROWS = NSP * CAP
PADROWS = NSP * SLOT
FFL = 256
EPS = 1e-06
LOW = -1e30
bf = jnp.bfloat16
f32 = jnp.float32

INTERPRET = False


def call(body, out_shape, inputs, smem=0, scratch=(), limit=12):
    specs = [pl.BlockSpec(memory_space=pltpu.SMEM)] * smem
    specs += [pl.BlockSpec(memory_space=pltpu.VMEM)] * (len(inputs) - smem)
    many = isinstance(out_shape, (tuple, list))
    vm = pl.BlockSpec(memory_space=pltpu.VMEM)
    return pl.pallas_call(
        body,
        out_shape=out_shape,
        in_specs=specs,
        out_specs=tuple([vm] * len(out_shape)) if many else vm,
        scratch_shapes=list(scratch),
        interpret=INTERPRET,
        compiler_params=pltpu.CompilerParams(vmem_limit_bytes=limit * 1024 * 1024),
    )(*inputs)


def three(v):
    hi = v.astype(bf).astype(f32)
    rest = v - hi
    mid = rest.astype(bf).astype(f32)
    return hi, mid, rest - mid


def attend(at_ref, q_ref, kv_ref, gate_ref, out0_ref, out1_ref, out2_ref, out3_ref, qs_ref, s_ref, m_ref, acc_ref, o_ref):
    z, x = at_ref[0], at_ref[1]
    first = gate_ref[:, pl.ds(pl.multiple_of(z * ROW, ROW), TOK)][:, 0:1]
    row64 = lax.broadcasted_iota(jnp.int32, (HD, TOK), 0)
    ones = jnp.where(row64 < 3, 1.0, 0.0).astype(bf)
    for j in range(NX):
        qs_ref[0:HD, j * TOK : (j + 1) * TOK] = q_ref[j] * bf(HD**-0.5)
        qs_ref[HD : 2 * HD, j * TOK : (j + 1) * TOK] = ones

    def scores(zk):
        place = pl.multiple_of(zk * ROW + x * TOK, TOK)
        hi, mid, lo = three(first - gate_ref[:, pl.ds(place, TOK)])
        extra = jnp.where(row64 == 0, hi, jnp.where(row64 == 1, mid, jnp.where(row64 == 2, lo, 0.0)))
        both = jnp.concatenate([kv_ref[zk, 0:HD, :], extra.astype(bf)], axis=0)
        return jnp.dot(both.T, qs_ref[...], preferred_element_type=f32)

    s = scores(z)
    ki = lax.broadcasted_iota(jnp.int32, (TOK, ROW), 0) + x * TOK
    qi = lax.broadcasted_iota(jnp.int32, (TOK, ROW), 1)
    s = jnp.where(ki <= qi, s, LOW)
    s_ref[z] = s
    m_ref[...] = jnp.broadcast_to(jnp.max(s, axis=0, keepdims=True), (8, ROW))

    def look(zk, carry):
        s = scores(zk)
        s_ref[zk] = s
        m_ref[...] = jnp.maximum(m_ref[...], jnp.max(s, axis=0, keepdims=True))
        return carry

    def look_two(i, carry):
        one, two = scores(2 * i), scores(2 * i + 1)
        s_ref[2 * i] = one
        s_ref[2 * i + 1] = two
        top = jnp.max(jnp.maximum(one, two), axis=0, keepdims=True)
        m_ref[...] = jnp.maximum(m_ref[...], top)
        return carry

    lax.fori_loop(0, z // 2, look_two, 0)
    lax.fori_loop(z // 2 * 2, z, look, 0)
    m = m_ref[0:1, :]
    acc_ref[...] = jnp.zeros((HD + 16, ROW), f32)

    def weigh(zk, carry):
        p = jnp.exp(s_ref[zk] - m).astype(bf)
        v = jnp.concatenate([kv_ref[zk, HD : 2 * HD, :], jnp.ones((16, TOK), bf)], axis=0)
        acc_ref[...] += jnp.dot(v, p, preferred_element_type=f32)
        return carry

    def weigh_two(i, carry):
        zk = 2 * i
        p = jnp.exp(s_ref[pl.ds(zk, 2)].reshape(2 * TOK, ROW) - m).astype(bf)
        v = jnp.concatenate([kv_ref[zk, HD : 2 * HD, :], kv_ref[zk + 1, HD : 2 * HD, :]], axis=1)
        v = jnp.concatenate([v, jnp.ones((16, 2 * TOK), bf)], axis=0)
        acc_ref[...] += jnp.dot(v, p, preferred_element_type=f32)
        return carry

    lax.fori_loop(0, (z + 1) // 2, weigh_two, 0)
    lax.fori_loop((z + 1) // 2 * 2, z + 1, weigh, 0)
    row16 = lax.broadcasted_iota(jnp.int32, (16, ROW), 0)
    total = acc_ref[HD : HD + 1, :]
    hi, mid, lo = three(m + jnp.log(total))
    stats = jnp.where(row16 == 0, hi, jnp.where(row16 == 1, mid, jnp.where(row16 == 2, lo, 0.0))).astype(bf)
    o_ref[0:HD, :] = (acc_ref[0:HD, :] / total).astype(bf)
    o_ref[HD : HD + 16, :] = stats
    for j, out_ref in enumerate((out0_ref, out1_ref, out2_ref, out3_ref)):
        out_ref[...] = o_ref[:, pl.ds(pl.multiple_of(lax.rem(x + j, NX) * TOK, TOK), TOK)]


def merge(*refs):
    parts, out_ref = refs[0:NX], refs[NX]
    ls = []
    for i in range(NX):
        st = parts[i][HD : HD + 16, :].astype(f32)
        ls.append(st[0:1] + st[1:2] + st[2:3])
    m = ls[0]
    for v in ls[1:]:
        m = jnp.maximum(m, v)
    acc = jnp.zeros((HD, TOK), f32)
    total = jnp.zeros((1, TOK), f32)
    for i in range(NX):
        w = jnp.exp(ls[i] - m)
        total = total + w
        acc = acc + w * parts[i][0:HD, :].astype(f32)
    out_ref[...] = (acc / total).astype(bf)


def prepare(kvq_ref, kv_ref, qs_ref):
    for z in range(NZ):
        kv_ref[z] = kvq_ref[0 : 2 * HD, :]
    for x in range(NX):
        qs_ref[x] = kvq_ref[2 * HD :, :]


def spread_weight(w_ref, out_ref):
    for y in range(NY):
        for c in range(NC):
            for q in range(2):
                block = (y % HALF + q * HALF) * NC + c
                out_ref[y * NC + c, q * HD : (q + 1) * HD, :] = w_ref[:, block * COLS : (block + 1) * COLS]


def route(at_ref, routes_ref, resid_ref, pick_ref, slots_ref, cols_ref):
    for q in range(2):
        cols_ref[:, q * COLS : (q + 1) * COLS] = resid_ref[:, pl.ds(pl.multiple_of(at_ref[q], COLS), COLS)]
    e0, e1 = routes_ref[0:1, :], routes_ref[1:2, :]
    io = lax.broadcasted_iota(jnp.int32, (NSP, TOK), 0)
    h0, h1 = io == e0, io == e1
    hit = jnp.where(h0, 1.0, jnp.where(h1, 1.0, 0.0)).astype(bf)
    ia = lax.broadcasted_iota(jnp.int32, (TOK, TOK), 0)
    ib = lax.broadcasted_iota(jnp.int32, (TOK, TOK), 1)
    upper = jnp.where(ia < ib, 1.0, 0.0).astype(bf)
    before = jnp.dot(hit, upper, preferred_element_type=f32)
    r0 = jnp.sum(jnp.where(h0, before, 0.0), axis=0, keepdims=True).astype(jnp.int32)
    r1 = jnp.sum(jnp.where(h1, before, 0.0), axis=0, keepdims=True).astype(jnp.int32)
    slots_ref[...] = jnp.concatenate([2 * SLOT * e0 + r0, 2 * SLOT * e1 + r1, jnp.zeros((6, TOK), jnp.int32)], axis=0)
    s0 = e0 * SEND + r0
    s1 = e1 * SEND + r1
    ir = lax.broadcasted_iota(jnp.int32, (NSP * SEND, TOK), 0)
    hits = (ir == s0) | (ir == s1) | (ir == s0 + CAP) | (ir == s1 + CAP)
    pick_ref[...] = jnp.where(hits, 1.0, 0.0).astype(bf)


def project(at_ref, att_ref, w_ref, resid_ref, gain_ref, pick_ref, stream_ref, out_ref):
    c0 = pl.multiple_of(at_ref[0], COLS)
    c1 = pl.multiple_of(at_ref[1], COLS)
    weights = [jnp.concatenate([w_ref[t, q * HD : (q + 1) * HD, :] for t in range(NTP)], axis=0) for q in range(2)]
    w = jnp.concatenate(weights, axis=1)
    mixed = lax.dot_general(att_ref[...], w, (((0,), (0,)), ((), ())), preferred_element_type=f32)
    gain = jnp.concatenate([gain_ref[:, pl.ds(c0, COLS)], gain_ref[:, pl.ds(c1, COLS)]], axis=1)
    stream = resid_ref[...].astype(f32) + mixed
    stream_ref[...] = jnp.where(at_ref[2] == 0, stream[:, 0:COLS], stream[:, COLS:])
    scaled = (stream * gain).astype(bf)
    sent = jnp.dot(pick_ref[...], scaled, preferred_element_type=f32).reshape(NSP, SEND, 2 * COLS)
    rank = lax.broadcasted_iota(jnp.int32, (NSP, SEND, COLS), 1)
    out_ref[...] = jnp.where(rank < CAP, sent[:, :, 0:COLS], sent[:, :, COLS:]).astype(bf)


def squeeze(in_ref, all_ref, low_ref, high_ref, rows_ref):
    for i in range(NSP):
        x = in_ref[i].astype(f32)
        rows_ref[ROWS + CAP * i : ROWS + CAP * i + CAP, :] = x[0:CAP, :]
        rows_ref[CAP * i : CAP * i + CAP, :] = x[CAP : 2 * CAP, :]
    all_ref[...] = rows_ref[...].astype(bf)
    high_ref[...] = rows_ref[0:ROWS, :].astype(bf)
    low_ref[...] = rows_ref[ROWS:, :].astype(bf)


NEAR = ((0, 0, 0, ROWS), (0, 1, 0, 0), (3, 0, 1, ROWS), (3, 1, 1, 0), (1, 0, 2, ROWS), (1, 1, 2, 0))
FAR = ((2, 0, 0, 0), (2, 1, 1, 0))
SENDS = (
    (0, 0, 2, 0),
    (0, ROWS, 2, 1),
    (1, 0, 1, 0),
    (1, ROWS, 1, 1),
    (1, 2 * ROWS, 3, 0),
    (1, 3 * ROWS, 3, 1),
    (1, 4 * ROWS, 0, 0),
    (1, 5 * ROWS, 0, 1),
)


def accumulate(y, c, pieces, owns, others, wg_ref, wu_ref, gain_ref, g_ref, u_ref, sq_ref, fresh):
    for off, upper, n, at in pieces:
        mine, theirs = owns[n][at : at + ROWS, :], others[n][at : at + ROWS, :]
        block = lax.rem(y + off, HALF) + upper * HALF
        first = pl.multiple_of((2 * block + c) * COLS, COLS)
        second = pl.multiple_of((2 * block + 1 - c) * COLS, COLS)
        xx = jnp.concatenate([mine, theirs], axis=1)
        for w_ref, acc_ref in ((wg_ref, g_ref), (wu_ref, u_ref)):
            w = jnp.concatenate([w_ref[pl.ds(first, COLS), :], w_ref[pl.ds(second, COLS), :]], axis=0)
            part = jnp.dot(xx, w, preferred_element_type=f32)
            acc_ref[...] = part if fresh else acc_ref[...] + part
        a = mine.astype(f32) * (1.0 / gain_ref[:, pl.ds(first, COLS)])
        b = theirs.astype(f32) * (1.0 / gain_ref[:, pl.ds(second, COLS)])
        part = a * a + b * b
        sq_ref[...] = part if fresh else sq_ref[...] + part
        fresh = False


def experts_near(at_ref, every_ref, n0_ref, n1_ref, swap_ref, near_ref, wg_ref, wu_ref, gain_ref, g_ref, u_ref, sq_ref):
    owns = (every_ref, n0_ref, n1_ref)
    others = (swap_ref, near_ref.at[0 : 2 * ROWS], near_ref.at[2 * ROWS :])
    accumulate(at_ref[0], at_ref[1], NEAR, owns, others, wg_ref, wu_ref, gain_ref, g_ref, u_ref, sq_ref, True)


def experts(at_ref, f0_ref, f1_ref, far_ref, g_in, u_in, sq_in, wg_ref, wu_ref, wd_ref, gain_ref, *refs):
    outs = refs[0:4]
    g_ref, u_ref, sq_ref, h_ref = refs[4:]
    y, c = at_ref[0], at_ref[1]
    others = (far_ref.at[0:ROWS], far_ref.at[ROWS:])
    g_ref[...] = g_in[...]
    u_ref[...] = u_in[...]
    sq_ref[...] = sq_in[...]
    accumulate(y, c, FAR, (f0_ref, f1_ref), others, wg_ref, wu_ref, gain_ref, g_ref, u_ref, sq_ref, False)
    scale = lax.rsqrt(jnp.sum(sq_ref[...], axis=1, keepdims=True) / D + EPS)
    gate = g_ref[...] * scale
    up = u_ref[...] * scale
    h_ref[...] = (gate / (1.0 + jnp.exp(-gate)) * up).astype(bf)
    even = c == 0
    for ref, at, off, upper in SENDS:
        block = lax.rem(y + off, HALF) + upper * HALF
        place = pl.multiple_of(2 * block * COLS, 2 * COLS)
        res = jnp.dot(h_ref[...], wd_ref[:, pl.ds(place, 2 * COLS)], preferred_element_type=f32)
        low, high = res[:, 0:COLS], res[:, COLS:]
        outs[ref][at : at + ROWS, :] = jnp.where(even, low, high).astype(bf)
        outs[ref + 2][at : at + ROWS, :] = jnp.where(even, high, low).astype(bf)


def gather_sum(mine_ref, theirs_ref, n0_ref, n1_ref, f0_ref, f1_ref, out_ref, rows_ref):
    base = 4 * ROWS
    pad = jnp.zeros((SLOT - CAP, COLS), f32)
    for q, far_ref in enumerate((f0_ref, f1_ref)):
        at = slice(q * ROWS, (q + 1) * ROWS)
        kept = slice(base + q * ROWS, base + (q + 1) * ROWS)
        acc = mine_ref[kept, :].astype(f32) + theirs_ref[kept, :].astype(f32)
        acc = acc + n0_ref[at, :].astype(f32) + n1_ref[at, :].astype(f32)
        rows_ref[...] = acc + far_ref[...].astype(f32)
        for i in range(NSP):
            out_ref[2 * i + q] = jnp.concatenate([rows_ref[CAP * i : CAP * i + CAP, :], pad], axis=0).astype(bf)


def route_back(slots_ref, back_ref):
    slots = slots_ref[...].astype(f32).T
    at = lax.broadcasted_iota(jnp.int32, (TOK, 2 * PADROWS), 1).astype(f32)
    for k in range(2):
        slot = slots[:, k : k + 1]
        back_ref[k * TOK : (k + 1) * TOK, :] = jnp.where((at == slot) | (at == slot + SLOT), 1.0, 0.0).astype(bf)


def finish(ret_ref, back_ref, rw_ref, stream_ref, out_ref):
    weight = jnp.concatenate([rw_ref[...], jnp.zeros((6, TOK), f32)], axis=0).T
    got = jnp.dot(back_ref[...], ret_ref[...], preferred_element_type=f32)
    out = stream_ref[...] + weight[:, 0:1] * got[0:TOK, :] + weight[:, 1:2] * got[TOK:, :]
    out_ref[...] = out.astype(bf)


def shift(v, by):
    return lax.ppermute(v, Y, [(i, (i + by) % NY) for i in range(NY)])


def exchange(v, axis):
    return lax.all_to_all(v, axis, 0, 0, tiled=True)


def layer(
    queries,
    keys,
    values,
    cum_gate,
    out_weight,
    resid,
    norm_gain,
    routes,
    route_weight,
    gate_weight,
    up_weight,
    down_weight,
):
    z, x, y, c = (lax.axis_index(a) for a in ("z", "x", Y, "c"))
    sds = jax.ShapeDtypeStruct
    half = NY // 2
    low = (lax.rem(y, half) * NC + c) * COLS
    at_cols = jnp.stack([low, low + half * NC * COLS, y // half]).astype(jnp.int32)
    at = jnp.stack([z, x]).astype(jnp.int32)
    kv_send, q_send = call(
        prepare,
        (sds((NZ, 2 * HD, TOK), bf), sds((NX, HD, TOK), bf)),
        (jnp.concatenate([keys.T, values.T, queries.T], axis=0),),
    )
    q_send, at, at_cols = lax.optimization_barrier((q_send, at, at_cols))
    q = exchange(q_send, "x")
    kv_send, q = lax.optimization_barrier((kv_send, q))
    kv = exchange(kv_send, "z")
    w_raw, kv = lax.optimization_barrier((out_weight, kv))
    w_send = call(spread_weight, sds((NTP, 2 * HD, COLS), bf), (w_raw,))
    w_cols = exchange(w_send, TP)
    sent = call(
        attend,
        (sds((HD + 16, TOK), bf),) * NX,
        (at, q, kv, cum_gate),
        smem=1,
        scratch=(
            pltpu.VMEM((2 * HD, ROW), bf),
            pltpu.VMEM((NZ, TOK, ROW), f32),
            pltpu.VMEM((8, ROW), f32),
            pltpu.VMEM((HD + 16, ROW), f32),
            pltpu.VMEM((HD + 16, ROW), bf),
        ),
        limit=14,
    )
    parts = [sent[0]]
    for n in range(1, NX):
        parts.append(lax.ppermute(sent[n], "x", [(i, (i + n) % NX) for i in range(NX)]))
    pick, slots, resid_cols = call(
        route,
        (sds((NSP * SEND, TOK), bf), sds((8, TOK), jnp.int32), sds((TOK, 2 * COLS), bf)),
        (at_cols, routes.T, resid),
        smem=1,
    )
    attended = call(merge, sds((HD, TOK), bf), tuple(parts))
    attended = lax.all_gather(attended, TP, axis=0, tiled=True)
    stream, outgoing = call(
        project,
        (sds((TOK, COLS), f32), sds((NSP, SEND, COLS), bf)),
        (at_cols, attended, w_cols, resid_cols, norm_gain.reshape(1, D), pick),
        smem=1,
    )
    arrived = exchange(outgoing, SP)
    every, lower, higher = call(
        squeeze,
        (sds((2 * ROWS, COLS), bf), sds((ROWS, COLS), bf), sds((ROWS, COLS), bf)),
        (arrived,),
        scratch=(pltpu.VMEM((2 * ROWS, COLS), f32),),
    )
    swap = [(0, 1), (1, 0)]
    owns = [every]
    for v, by in ((every, 1), (every, -1), (lower, 2), (higher, -2)):
        owns.append(shift(v, by))
    others = []
    for v in (every, jnp.concatenate(owns[1:3], axis=0), jnp.concatenate(owns[3:5], axis=0)):
        others.append(lax.ppermute(v, "c", swap))
    gain = norm_gain.reshape(1, D)
    at_yc = jnp.stack([y, c]).astype(jnp.int32)
    sums = (sds((ROWS, FFL), f32), sds((ROWS, FFL), f32), sds((ROWS, COLS), f32))
    partial = call(experts_near, sums, (at_yc, *owns[0:3], *others[0:2], gate_weight[0], up_weight[0], gain), smem=1)
    far_out, near_out = sds((2 * ROWS, COLS), bf), sds((6 * ROWS, COLS), bf)
    far_mine, near_mine, far_theirs, near_theirs = call(
        experts,
        (far_out, near_out, far_out, near_out),
        (at_yc, *owns[3:5], others[2], *partial, gate_weight[0], up_weight[0], down_weight[0], gain),
        smem=1,
        scratch=[pltpu.VMEM(v.shape, f32) for v in sums] + [pltpu.VMEM((ROWS, FFL), bf)],
    )
    far_theirs = lax.ppermute(far_theirs, "c", swap)
    near_theirs = lax.ppermute(near_theirs, "c", swap)

    def pair(a, b, first, count):
        part = slice(first * ROWS, (first + count) * ROWS)
        return (a[part].astype(f32) + b[part].astype(f32)).astype(bf)

    got = []
    for a, b, first, count, by in (
        (far_mine, far_theirs, 0, 1, 2),
        (far_mine, far_theirs, 1, 1, -2),
        (near_mine, near_theirs, 0, 2, 1),
        (near_mine, near_theirs, 2, 2, -1),
    ):
        got.append(shift(pair(a, b, first, count), by))
    back_pick = call(route_back, sds((2 * TOK, 2 * PADROWS), bf), (slots,))
    back = call(
        gather_sum,
        sds((2 * NSP, SLOT, COLS), bf),
        (near_mine, near_theirs, got[2], got[3], got[0], got[1]),
        scratch=(pltpu.VMEM((ROWS, COLS), f32),),
    )
    returned = exchange(back, ("z", "x", "yh")).reshape(2 * PADROWS, COLS)
    return call(finish, sds((TOK, COLS), bf), (returned, back_pick, route_weight.T, stream))


def solution(mesh):
    grid = Mesh(mesh.devices.reshape(NZ, NX, 2, HALF, NC), ("z", "x", "yh", "yl", "c"))
    return jax.shard_map(
        layer,
        mesh=grid,
        in_specs=(
            P(SP, TP),
            P(SP, TP),
            P(SP, TP),
            P(TP, None),
            P(TP, None),
            P(SP, None),
            P(),
            P(SP, None),
            P(SP, None),
            P(SP, None, TP),
            P(SP, None, TP),
            P(SP, TP, None),
        ),
        out_specs=P(SP, TP),
        check_vma=False,
    )
```

```python
import jax
import jax.numpy as jnp
from jax import lax
from jax.experimental import pallas as pl
from jax.experimental.pallas import tpu as pltpu
from jax.sharding import Mesh, PartitionSpec as P


NZ, NX, NY, NC = 8, 4, 8, 2
NSP, NTP = NZ * NX, NY * NC
Y = ("yh", "yl")
SP, TP = ("z", "x"), ("yh", "yl", "c")
HALF = NY // 2
HD = 64
TOK = 256
D = 2048
COLS = D // NTP
ROW = NX * TOK
CAP = 20
SLOT = 24
SEND = 2 * CAP
ROWS = NSP * CAP
PADROWS = NSP * SLOT
FFL = 256
EPS = 1e-06
LOW = -1e30
bf = jnp.bfloat16
f32 = jnp.float32

INTERPRET = False


def call(body, out_shape, inputs, smem=0, scratch=(), limit=12):
    specs = [pl.BlockSpec(memory_space=pltpu.SMEM)] * smem
    specs += [pl.BlockSpec(memory_space=pltpu.VMEM)] * (len(inputs) - smem)
    many = isinstance(out_shape, (tuple, list))
    vm = pl.BlockSpec(memory_space=pltpu.VMEM)
    return pl.pallas_call(
        body,
        out_shape=out_shape,
        in_specs=specs,
        out_specs=tuple([vm] * len(out_shape)) if many else vm,
        scratch_shapes=list(scratch),
        interpret=INTERPRET,
        compiler_params=pltpu.CompilerParams(vmem_limit_bytes=limit * 1024 * 1024),
    )(*inputs)


def three(v):
    hi = v.astype(bf).astype(f32)
    rest = v - hi
    mid = rest.astype(bf).astype(f32)
    return hi, mid, rest - mid


def attend(at_ref, q_ref, kv_ref, gate_ref, out0_ref, out1_ref, out2_ref, out3_ref, qs_ref, s_ref, m_ref, acc_ref, o_ref):
    z, x = at_ref[0], at_ref[1]
    first = gate_ref[:, pl.ds(pl.multiple_of(z * ROW, ROW), TOK)][:, 0:1]
    row64 = lax.broadcasted_iota(jnp.int32, (HD, TOK), 0)
    ones = jnp.where(row64 < 3, 1.0, 0.0).astype(bf)
    for j in range(NX):
        qs_ref[0:HD, j * TOK : (j + 1) * TOK] = q_ref[j] * bf(HD**-0.5)
        qs_ref[HD : 2 * HD, j * TOK : (j + 1) * TOK] = ones

    def scores(zk):
        place = pl.multiple_of(zk * ROW + x * TOK, TOK)
        hi, mid, lo = three(first - gate_ref[:, pl.ds(place, TOK)])
        extra = jnp.where(row64 == 0, hi, jnp.where(row64 == 1, mid, jnp.where(row64 == 2, lo, 0.0)))
        both = jnp.concatenate([kv_ref[zk, 0:HD, :], extra.astype(bf)], axis=0)
        return jnp.dot(both.T, qs_ref[...], preferred_element_type=f32)

    s = scores(z)
    ki = lax.broadcasted_iota(jnp.int32, (TOK, ROW), 0) + x * TOK
    qi = lax.broadcasted_iota(jnp.int32, (TOK, ROW), 1)
    s = jnp.where(ki <= qi, s, LOW)
    s_ref[z] = s
    m_ref[...] = jnp.broadcast_to(jnp.max(s, axis=0, keepdims=True), (8, ROW))

    def look(zk, carry):
        s = scores(zk)
        s_ref[zk] = s
        m_ref[...] = jnp.maximum(m_ref[...], jnp.max(s, axis=0, keepdims=True))
        return carry

    def look_two(i, carry):
        one, two = scores(2 * i), scores(2 * i + 1)
        s_ref[2 * i] = one
        s_ref[2 * i + 1] = two
        top = jnp.max(jnp.maximum(one, two), axis=0, keepdims=True)
        m_ref[...] = jnp.maximum(m_ref[...], top)
        return carry

    lax.fori_loop(0, z // 2, look_two, 0)
    lax.fori_loop(z // 2 * 2, z, look, 0)
    m = m_ref[0:1, :]
    acc_ref[...] = jnp.zeros((HD + 16, ROW), f32)

    def weigh(zk, carry):
        p = jnp.exp(s_ref[zk] - m).astype(bf)
        v = jnp.concatenate([kv_ref[zk, HD : 2 * HD, :], jnp.ones((16, TOK), bf)], axis=0)
        acc_ref[...] += jnp.dot(v, p, preferred_element_type=f32)
        return carry

    def weigh_two(i, carry):
        zk = 2 * i
        p = jnp.exp(s_ref[pl.ds(zk, 2)].reshape(2 * TOK, ROW) - m).astype(bf)
        v = jnp.concatenate([kv_ref[zk, HD : 2 * HD, :], kv_ref[zk + 1, HD : 2 * HD, :]], axis=1)
        v = jnp.concatenate([v, jnp.ones((16, 2 * TOK), bf)], axis=0)
        acc_ref[...] += jnp.dot(v, p, preferred_element_type=f32)
        return carry

    lax.fori_loop(0, (z + 1) // 2, weigh_two, 0)
    lax.fori_loop((z + 1) // 2 * 2, z + 1, weigh, 0)
    row16 = lax.broadcasted_iota(jnp.int32, (16, ROW), 0)
    total = acc_ref[HD : HD + 1, :]
    hi, mid, lo = three(m + jnp.log(total))
    stats = jnp.where(row16 == 0, hi, jnp.where(row16 == 1, mid, jnp.where(row16 == 2, lo, 0.0))).astype(bf)
    o_ref[0:HD, :] = (acc_ref[0:HD, :] / total).astype(bf)
    o_ref[HD : HD + 16, :] = stats
    for j, out_ref in enumerate((out0_ref, out1_ref, out2_ref, out3_ref)):
        out_ref[...] = o_ref[:, pl.ds(pl.multiple_of(lax.rem(x + j, NX) * TOK, TOK), TOK)]


def merge(*refs):
    parts, out_ref = refs[0:NX], refs[NX]
    ls = []
    for i in range(NX):
        st = parts[i][HD : HD + 16, :].astype(f32)
        ls.append(st[0:1] + st[1:2] + st[2:3])
    m = ls[0]
    for v in ls[1:]:
        m = jnp.maximum(m, v)
    acc = jnp.zeros((HD, TOK), f32)
    total = jnp.zeros((1, TOK), f32)
    for i in range(NX):
        w = jnp.exp(ls[i] - m)
        total = total + w
        acc = acc + w * parts[i][0:HD, :].astype(f32)
    out_ref[...] = (acc / total).astype(bf)


def prepare(kvq_ref, kv_ref, qs_ref):
    for z in range(NZ):
        kv_ref[z] = kvq_ref[0 : 2 * HD, :]
    for x in range(NX):
        qs_ref[x] = kvq_ref[2 * HD :, :]


def spread_weight(w_ref, out_ref):
    for y in range(NY):
        for c in range(NC):
            for q in range(2):
                block = (y % HALF + q * HALF) * NC + c
                out_ref[y * NC + c, q * HD : (q + 1) * HD, :] = w_ref[:, block * COLS : (block + 1) * COLS]


def route(at_ref, routes_ref, resid_ref, pick_ref, slots_ref, cols_ref):
    for q in range(2):
        cols_ref[:, q * COLS : (q + 1) * COLS] = resid_ref[:, pl.ds(pl.multiple_of(at_ref[q], COLS), COLS)]
    e0, e1 = routes_ref[0:1, :], routes_ref[1:2, :]
    io = lax.broadcasted_iota(jnp.int32, (NSP, TOK), 0)
    h0, h1 = io == e0, io == e1
    hit = jnp.where(h0, 1.0, jnp.where(h1, 1.0, 0.0)).astype(bf)
    ia = lax.broadcasted_iota(jnp.int32, (TOK, TOK), 0)
    ib = lax.broadcasted_iota(jnp.int32, (TOK, TOK), 1)
    upper = jnp.where(ia < ib, 1.0, 0.0).astype(bf)
    before = jnp.dot(hit, upper, preferred_element_type=f32)
    r0 = jnp.sum(jnp.where(h0, before, 0.0), axis=0, keepdims=True).astype(jnp.int32)
    r1 = jnp.sum(jnp.where(h1, before, 0.0), axis=0, keepdims=True).astype(jnp.int32)
    slots_ref[...] = jnp.concatenate([SLOT * e0 + r0, SLOT * e1 + r1, jnp.zeros((6, TOK), jnp.int32)], axis=0)
    s0 = e0 * SEND + r0
    s1 = e1 * SEND + r1
    ir = lax.broadcasted_iota(jnp.int32, (NSP * SEND, TOK), 0)
    hits = (ir == s0) | (ir == s1) | (ir == s0 + CAP) | (ir == s1 + CAP)
    pick_ref[...] = jnp.where(hits, 1.0, 0.0).astype(bf)


def project(at_ref, att_ref, w_ref, resid_ref, gain_ref, pick_ref, stream_ref, out_ref):
    c0 = pl.multiple_of(at_ref[0], COLS)
    c1 = pl.multiple_of(at_ref[1], COLS)
    weights = [jnp.concatenate([w_ref[t, q * HD : (q + 1) * HD, :] for t in range(NTP)], axis=0) for q in range(2)]
    w = jnp.concatenate(weights, axis=1)
    mixed = lax.dot_general(att_ref[...], w, (((0,), (0,)), ((), ())), preferred_element_type=f32)
    gain = jnp.concatenate([gain_ref[:, pl.ds(c0, COLS)], gain_ref[:, pl.ds(c1, COLS)]], axis=1)
    stream = resid_ref[...].astype(f32) + mixed
    stream_ref[...] = jnp.where(at_ref[2] == 0, stream[:, 0:COLS], stream[:, COLS:])
    scaled = (stream * gain).astype(bf)
    sent = jnp.dot(pick_ref[...], scaled, preferred_element_type=f32).reshape(NSP, SEND, 2 * COLS)
    rank = lax.broadcasted_iota(jnp.int32, (NSP, SEND, COLS), 1)
    out_ref[...] = jnp.where(rank < CAP, sent[:, :, 0:COLS], sent[:, :, COLS:]).astype(bf)


def squeeze(in_ref, all_ref, low_ref, high_ref, rows_ref):
    for i in range(NSP):
        x = in_ref[i].astype(f32)
        rows_ref[ROWS + CAP * i : ROWS + CAP * i + CAP, :] = x[0:CAP, :]
        rows_ref[CAP * i : CAP * i + CAP, :] = x[CAP : 2 * CAP, :]
    all_ref[...] = rows_ref[...].astype(bf)
    high_ref[...] = rows_ref[0:ROWS, :].astype(bf)
    low_ref[...] = rows_ref[ROWS:, :].astype(bf)


NEAR = ((0, 0, 0, ROWS), (0, 1, 0, 0), (3, 0, 1, ROWS), (3, 1, 1, 0), (1, 0, 2, ROWS), (1, 1, 2, 0))
FAR = ((2, 0, 0, 0), (2, 1, 1, 0))
SENDS = (
    (0, 0, 2, 0),
    (0, ROWS, 2, 1),
    (1, 0, 1, 0),
    (1, ROWS, 1, 1),
    (1, 2 * ROWS, 3, 0),
    (1, 3 * ROWS, 3, 1),
    (1, 4 * ROWS, 0, 0),
    (1, 5 * ROWS, 0, 1),
)


def accumulate(y, c, pieces, owns, others, wg_ref, wu_ref, gain_ref, g_ref, u_ref, sq_ref, before):
    for off, upper, n, at in pieces:
        mine, theirs = owns[n][at : at + ROWS, :], others[n][at : at + ROWS, :]
        block = lax.rem(y + off, HALF) + upper * HALF
        first = pl.multiple_of((2 * block + c) * COLS, COLS)
        second = pl.multiple_of((2 * block + 1 - c) * COLS, COLS)
        xx = jnp.concatenate([mine, theirs], axis=1)
        for i, (w_ref, acc_ref) in enumerate(((wg_ref, g_ref), (wu_ref, u_ref))):
            w = jnp.concatenate([w_ref[pl.ds(first, COLS), :], w_ref[pl.ds(second, COLS), :]], axis=0)
            part = jnp.dot(xx, w, preferred_element_type=f32)
            acc_ref[...] = part if before is None else before[i][...] + part
        a = mine.astype(f32) * (1.0 / gain_ref[:, pl.ds(first, COLS)])
        b = theirs.astype(f32) * (1.0 / gain_ref[:, pl.ds(second, COLS)])
        part = a * a + b * b
        sq_ref[...] = part if before is None else before[2][...] + part
        before = (g_ref, u_ref, sq_ref)


def experts_near(at_ref, every_ref, n0_ref, n1_ref, swap_ref, near_ref, wg_ref, wu_ref, gain_ref, g_ref, u_ref, sq_ref):
    owns = (every_ref, n0_ref, n1_ref)
    others = (swap_ref, near_ref.at[0 : 2 * ROWS], near_ref.at[2 * ROWS :])
    accumulate(at_ref[0], at_ref[1], NEAR, owns, others, wg_ref, wu_ref, gain_ref, g_ref, u_ref, sq_ref, None)


def experts(at_ref, f0_ref, f1_ref, far_ref, g_in, u_in, sq_in, wg_ref, wu_ref, wd_ref, gain_ref, *refs):
    outs = refs[0:4]
    g_ref, u_ref, sq_ref, h_ref = refs[4:]
    y, c = at_ref[0], at_ref[1]
    others = (far_ref.at[0:ROWS], far_ref.at[ROWS:])
    before = (g_in, u_in, sq_in)
    accumulate(y, c, FAR, (f0_ref, f1_ref), others, wg_ref, wu_ref, gain_ref, g_ref, u_ref, sq_ref, before)
    scale = lax.rsqrt(jnp.sum(sq_ref[...], axis=1, keepdims=True) / D + EPS)
    gate = g_ref[...] * scale
    up = u_ref[...] * scale
    h_ref[...] = (gate / (1.0 + jnp.exp(-gate)) * up).astype(bf)
    even = c == 0
    for ref, at, off, upper in SENDS:
        block = lax.rem(y + off, HALF) + upper * HALF
        place = pl.multiple_of(2 * block * COLS, 2 * COLS)
        res = jnp.dot(h_ref[...], wd_ref[:, pl.ds(place, 2 * COLS)], preferred_element_type=f32)
        low, high = res[:, 0:COLS], res[:, COLS:]
        outs[ref][at : at + ROWS, :] = jnp.where(even, low, high).astype(bf)
        outs[ref + 2][at : at + ROWS, :] = jnp.where(even, high, low).astype(bf)


def gather_sum(mine_ref, theirs_ref, n0_ref, n1_ref, f0_ref, f1_ref, out_ref, rows_ref):
    base = 4 * ROWS
    pad = jnp.zeros((SLOT - CAP, COLS), f32)
    for q, far_ref in enumerate((f0_ref, f1_ref)):
        at = slice(q * ROWS, (q + 1) * ROWS)
        kept = slice(base + q * ROWS, base + (q + 1) * ROWS)
        acc = mine_ref[kept, :].astype(f32) + theirs_ref[kept, :].astype(f32)
        acc = acc + n0_ref[at, :].astype(f32) + n1_ref[at, :].astype(f32)
        rows_ref[...] = acc + far_ref[...].astype(f32)
        for i in range(NSP):
            out_ref[q * NSP + i] = jnp.concatenate([rows_ref[CAP * i : CAP * i + CAP, :], pad], axis=0).astype(bf)


def route_back(slots_ref, back_ref):
    slots = slots_ref[...].astype(f32).T
    at = lax.broadcasted_iota(jnp.int32, (TOK, 2 * PADROWS), 1).astype(f32)
    for k in range(2):
        slot = slots[:, k : k + 1]
        back_ref[k * TOK : (k + 1) * TOK, :] = jnp.where((at == slot) | (at == slot + PADROWS), 1.0, 0.0).astype(bf)


def finish(ret_ref, back_ref, rw_ref, stream_ref, out_ref):
    weight = jnp.concatenate([rw_ref[...], jnp.zeros((6, TOK), f32)], axis=0).T
    got = jnp.dot(back_ref[...], ret_ref[...], preferred_element_type=f32)
    out = stream_ref[...] + weight[:, 0:1] * got[0:TOK, :] + weight[:, 1:2] * got[TOK:, :]
    out_ref[...] = out.astype(bf)


def shift(v, by):
    return lax.ppermute(v, Y, [(i, (i + by) % NY) for i in range(NY)])


def exchange(v, axis):
    return lax.all_to_all(v, axis, 0, 0, tiled=True)


def layer(
    queries,
    keys,
    values,
    cum_gate,
    out_weight,
    resid,
    norm_gain,
    routes,
    route_weight,
    gate_weight,
    up_weight,
    down_weight,
):
    z, x, y, c = (lax.axis_index(a) for a in ("z", "x", Y, "c"))
    sds = jax.ShapeDtypeStruct
    half = NY // 2
    low = (lax.rem(y, half) * NC + c) * COLS
    at_cols = jnp.stack([low, low + half * NC * COLS, y // half]).astype(jnp.int32)
    at = jnp.stack([z, x]).astype(jnp.int32)
    kv_send, q_send = call(
        prepare,
        (sds((NZ, 2 * HD, TOK), bf), sds((NX, HD, TOK), bf)),
        (jnp.concatenate([keys.T, values.T, queries.T], axis=0),),
    )
    q_send, at, at_cols = lax.optimization_barrier((q_send, at, at_cols))
    q = exchange(q_send, "x")
    kv_send, q = lax.optimization_barrier((kv_send, q))
    kv = exchange(kv_send, "z")
    w_raw, kv = lax.optimization_barrier((out_weight, kv))
    w_send = call(spread_weight, sds((NTP, 2 * HD, COLS), bf), (w_raw,))
    w_cols = exchange(w_send, TP)
    sent = call(
        attend,
        (sds((HD + 16, TOK), bf),) * NX,
        (at, q, kv, cum_gate),
        smem=1,
        scratch=(
            pltpu.VMEM((2 * HD, ROW), bf),
            pltpu.VMEM((NZ, TOK, ROW), f32),
            pltpu.VMEM((8, ROW), f32),
            pltpu.VMEM((HD + 16, ROW), f32),
            pltpu.VMEM((HD + 16, ROW), bf),
        ),
        limit=14,
    )
    parts = [sent[0]]
    for n in range(1, NX):
        parts.append(lax.ppermute(sent[n], "x", [(i, (i + n) % NX) for i in range(NX)]))
    pick, slots, resid_cols = call(
        route,
        (sds((NSP * SEND, TOK), bf), sds((8, TOK), jnp.int32), sds((TOK, 2 * COLS), bf)),
        (at_cols, routes.T, resid),
        smem=1,
    )
    attended = call(merge, sds((HD, TOK), bf), tuple(parts))
    attended = lax.all_gather(attended, TP, axis=0, tiled=True)
    stream, outgoing = call(
        project,
        (sds((TOK, COLS), f32), sds((NSP, SEND, COLS), bf)),
        (at_cols, attended, w_cols, resid_cols, norm_gain.reshape(1, D), pick),
        smem=1,
    )
    arrived = exchange(outgoing, SP)
    every, lower, higher = call(
        squeeze,
        (sds((2 * ROWS, COLS), bf), sds((ROWS, COLS), bf), sds((ROWS, COLS), bf)),
        (arrived,),
        scratch=(pltpu.VMEM((2 * ROWS, COLS), f32),),
    )
    swap = [(0, 1), (1, 0)]
    owns = [every]
    for v, by in ((every, 1), (every, -1), (lower, 2), (higher, -2)):
        owns.append(shift(v, by))
    others = []
    for v in (every, jnp.concatenate(owns[1:3], axis=0), jnp.concatenate(owns[3:5], axis=0)):
        others.append(lax.ppermute(v, "c", swap))
    gain = norm_gain.reshape(1, D)
    at_yc = jnp.stack([y, c]).astype(jnp.int32)
    sums = (sds((ROWS, FFL), f32), sds((ROWS, FFL), f32), sds((ROWS, COLS), f32))
    partial = call(experts_near, sums, (at_yc, *owns[0:3], *others[0:2], gate_weight[0], up_weight[0], gain), smem=1)
    far_out, near_out = sds((2 * ROWS, COLS), bf), sds((6 * ROWS, COLS), bf)
    far_mine, near_mine, far_theirs, near_theirs = call(
        experts,
        (far_out, near_out, far_out, near_out),
        (at_yc, *owns[3:5], others[2], *partial, gate_weight[0], up_weight[0], down_weight[0], gain),
        smem=1,
        scratch=[pltpu.VMEM(v.shape, f32) for v in sums] + [pltpu.VMEM((ROWS, FFL), bf)],
    )
    far_theirs = lax.ppermute(far_theirs, "c", swap)
    near_theirs = lax.ppermute(near_theirs, "c", swap)

    def pair(a, b, first, count):
        part = slice(first * ROWS, (first + count) * ROWS)
        return (a[part].astype(f32) + b[part].astype(f32)).astype(bf)

    got = []
    for a, b, first, count, by in (
        (far_mine, far_theirs, 0, 1, 2),
        (far_mine, far_theirs, 1, 1, -2),
        (near_mine, near_theirs, 0, 2, 1),
        (near_mine, near_theirs, 2, 2, -1),
    ):
        got.append(shift(pair(a, b, first, count), by))
    back_pick = call(route_back, sds((2 * TOK, 2 * PADROWS), bf), (slots,))
    back = call(
        gather_sum,
        sds((2 * NSP, SLOT, COLS), bf),
        (near_mine, near_theirs, got[2], got[3], got[0], got[1]),
        scratch=(pltpu.VMEM((ROWS, COLS), f32),),
    )
    returned = exchange(back, ("yh", "z", "x")).reshape(2 * PADROWS, COLS)
    return call(finish, sds((TOK, COLS), bf), (returned, back_pick, route_weight.T, stream))


def solution(mesh):
    grid = Mesh(mesh.devices.reshape(NZ, NX, 2, HALF, NC), ("z", "x", "yh", "yl", "c"))
    return jax.shard_map(
        layer,
        mesh=grid,
        in_specs=(
            P(SP, TP),
            P(SP, TP),
            P(SP, TP),
            P(TP, None),
            P(TP, None),
            P(SP, None),
            P(),
            P(SP, None),
            P(SP, None),
            P(SP, None, TP),
            P(SP, None, TP),
            P(SP, TP, None),
        ),
        out_specs=P(SP, TP),
        check_vma=False,
    )
```
